128 devices in a mesh: sp: 32 (over z, y, core), tp: 4 (over x).
Axes of the slice: x: 4, y: 4, z: 4, core: 2. Of those that a mesh axis runs over, the one named last changes fastest.
Arguments:
- layer_input: bfloat16 [16384, 2048], P('sp'), may hold values from -6 to 6
- out_cot: bfloat16 [16384, 2048], P('sp'), may hold values from -6 to 6
- expert_ids: int32 [16384, 2], P('sp'), may hold values from 0 to 31, all different within a row; in each aligned block of 512 rows (0 to 511, 512 to 1023, ...) at most 40 rows name the same one
- route_weight: float32 [16384, 2], P('sp'), may hold values from 0.1 to 1
- w_gate: bfloat16 [32, 2048, 1024], P('sp', None, 'tp'), may hold values from -0.125 to 0.125
- w_up: bfloat16 [32, 2048, 1024], P('sp', None, 'tp'), may hold values from -0.125 to 0.125
- w_down: bfloat16 [32, 1024, 2048], P('sp', 'tp'), may hold values from -0.1875 to 0.1875
- out_proj: bfloat16 [2048, 1024], P(None, 'tp'), may hold values from -0.1875 to 0.1875
- rec_input: bfloat16 [16384, 1024], P('sp', 'tp'), may hold values from -6 to 6
- gate_input: bfloat16 [16384, 1024], P('sp', 'tp'), may hold values from -6 to 6
- prev_state: float32 [16384, 1024], P('sp', 'tp'), may hold values from -6 to 6
- decay_param: float32 [1024], replicated, may hold values from 4 to 20
- extra_decay: float32 [8, 16384], P('tp', 'sp'), may hold values from -3 to 0, as said below
- gate_a_w: bfloat16 [8, 128, 128], replicated, may hold values from -0.5 to 0.5
- gate_i_w: bfloat16 [8, 128, 128], replicated, may hold values from -0.5 to 0.5
Outputs:
- grad_gate: float32 [32, 2048, 1024], P('sp', None, 'tp')
- grad_up: float32 [32, 2048, 1024], P('sp', None, 'tp')
- grad_down: float32 [32, 1024, 2048], P('sp', 'tp')
- grad_out_proj: float32 [2048, 1024], P('sp', 'tp')
- rec_input_grad: bfloat16 [16384, 1024], P('sp', 'tp')
- gate_input_grad: bfloat16 [16384, 1024], P('sp', 'tp')
The draws below stay inside these ranges and needn't reach their ends.
Inputs may be any that keep to these rules, and one draw needn't show every extreme that they name: `expert_ids`: each row names 2 different experts; among the slots of the tokens of one sp index (aligned blocks of 512 rows) no expert is named more than 40 times, and in every draw some expert is named exactly 40 times in some block. `extra_decay`: every entry is at most -0.05 / 16384.
All inputs are finite; a program needn't handle non-finite values.
Results may differ from the reference program's by a relative error of at most 0.017.
Values may be sent and summed in bfloat16 or wider, within the bound.
No kernel may reach another device: no remote copies, remote signals or barrier semaphores. Data moves between devices by JAX's collectives and lax.ppermute only.
A program may use at most 128 MiB of HBM per device.

```python
import math
import jax
import jax.numpy as jnp
import numpy as np
from jax import lax

D = 2048
FF = 1024
RECURRENT_HEADS = 8
HEAD_DIM = 128
TOP = 2
TOK_DEV = 512
D_LRU = 1024
EXPERTS = 32
TOKENS = 16384
CAP = 40
EXP_ROWS = 1280
N_SP = 32
N_TP = 4


def draw_decay_param(key, part):
    head_key, rate_random_key = jax.random.split(jax.random.fold_in(key, 11))
    picks = jax.random.randint(head_key, (RECURRENT_HEADS,), 0, 10)
    quick = picks < 5
    unit = jax.random.uniform(rate_random_key, (RECURRENT_HEADS, HEAD_DIM), jnp.float32)
    quick_rate = 0.0025 * 4.0 ** unit
    slow_rate = 0.02 / TOKENS * 5.0 ** unit
    rate = jnp.where(quick[:, None], quick_rate, slow_rate).reshape(RECURRENT_HEADS * HEAD_DIM)
    return (-jnp.log(jnp.expm1(rate))).astype(jnp.float32)


def draw_extra_decay(key, part):
    rate_random_key, spike_random_key, placement_random_key = jax.random.split(jax.random.fold_in(key, 23), 3)
    blocks = TOKENS // TOK_DEV
    unit = jax.random.uniform(rate_random_key, (RECURRENT_HEADS, blocks), jnp.float32)
    block_rate = 0.1 / TOKENS * 10.0 ** unit
    token_wise = jnp.repeat(block_rate, TOK_DEV, axis=1)
    spots = jax.random.randint(placement_random_key, (RECURRENT_HEADS, 3), 0, TOKENS)
    retained_mask = jax.random.uniform(spike_random_key, (RECURRENT_HEADS, 3), jnp.float32, 0.5, 0.8)
    match_count = (spots[:, :, None] == jnp.arange(TOKENS, dtype=jnp.int32)[None, None, :]).astype(jnp.float32)
    spike_amount = jnp.sum(match_count * jnp.log(retained_mask)[:, :, None], axis=1)
    return (spike_amount - token_wise).astype(jnp.float32)


def raised(values, stream_key, source, target, blocks, factor):
    def block_of(position):
        return (jnp.arange(values.shape[position]) // (values.shape[position] // blocks)).reshape((-1,) + (1,) * (values.ndim - 1 - position))

    one_side = jax.random.permutation(stream_key, blocks)[block_of(target)]
    far = (block_of(target) + blocks // 2) % blocks
    return jnp.where((block_of(source) == one_side) | (block_of(source) == far), factor * values, values)


def shard_levels(stream_key, shape, pieces, low, high):
    loudness = 1.0
    for axis_at, parts in pieces:
        steps = jax.random.uniform(jax.random.fold_in(jax.random.fold_in(stream_key, 6), axis_at), (parts,), jnp.float32, low / len(pieces), high / len(pieces))
        loudness = loudness * jnp.repeat(jnp.exp(steps), shape[axis_at] // parts).reshape((-1,) + (1,) * (len(shape) - 1 - axis_at))
    return loudness


def deal_out(stream_key, own, number, rows, amount, top, reach, skew):
    ranking = jax.random.permutation(stream_key, amount)
    crowded, usual = portions_of(amount, rows * top, reach, skew, True), portions_of(amount, rows * top, reach, skew, False)
    places = jnp.arange(amount)

    def named(lengths, turn):
        used = int((lengths > 0).sum())
        fixed = max(1, used // 4)
        shifted = fixed + (places - fixed + turn * (used - fixed)) % max(1, amount - fixed)
        return jnp.zeros((amount,), jnp.int32).at[ranking[jnp.where(places < fixed, places, shifted)]].set(jnp.asarray(lengths, jnp.int32))

    lengths = jnp.where(number % 4 == 0, named(crowded, number // 4), named(usual, number - number // 4 - 1))
    mixed = jax.random.permutation(jax.random.fold_in(own, 3), amount)
    giver, sink = mixed[0:amount // 2 * 2:2], mixed[1:amount // 2 * 2:2]
    room = jnp.minimum(lengths[giver] - 1, reach - lengths[sink]) // 2
    room = jnp.where((giver == ranking[0]) | (sink == ranking[0]) | (lengths[sink] == 0), 0, jnp.maximum(room, 0))
    shifted = jax.random.randint(jax.random.fold_in(own, 4), (amount // 2,), 0, 1 << 20) % (room + 1)
    lengths = lengths.at[giver].add(-shifted).at[sink].add(shifted)
    items = jnp.searchsorted(jnp.cumsum(lengths), jnp.arange(rows * top), side="right").astype(jnp.int32)
    table = items.reshape(top, rows).T
    table = table[jax.random.permutation(jax.random.fold_in(own, 1), rows)]
    turn = jax.random.randint(jax.random.fold_in(own, 2), (rows, 1), 0, top)
    return jnp.take_along_axis(table, (jnp.arange(top)[None, :] + turn) % top, axis=1)


def portions_of(amount, total, limit, lean, full):
    loads = [(1 << 20) // math.isqrt(grade ** lean) + 1 for grade in range(1, amount + 1)]
    largest = limit if full else min(limit, max(-(-total // amount), total * loads[0] // sum(loads)))
    least = 1 if total - largest >= amount - 1 else 0
    holding, rest = [largest] + [least] * (amount - 1), total - largest - least * (amount - 1)
    while rest > 0:
        candidates = [i for i in range(1, amount) if holding[i] < largest] or [i for i in range(1, amount) if holding[i] < limit]
        pool, left = sum([loads[i] for i in candidates]), rest
        for i in candidates:
            extra = min(limit - holding[i], max(1, left * loads[i] // pool), rest)
            holding[i] = holding[i] + extra
            rest = rest - extra
    return np.array(holding)


def centred(key, dims, width, limit, cuts=(), kind=jnp.bfloat16):
    entries = width * jax.random.normal(key, dims, jnp.float32)
    if cuts:
        entries = entries * shard_levels(key, dims, cuts, -0.22, 0.18)
    return jnp.clip(entries, -limit, limit).astype(kind)


def noise_with(rng, extent, width, most, cuts, heavy, kind=jnp.bfloat16):
    entries = width * jax.random.normal(rng, extent, jnp.float32)
    if cuts:
        entries = entries * shard_levels(rng, extent, cuts, -0.22, 0.18)
    return jnp.clip(raised(entries, jax.random.fold_in(rng, 3), *heavy), -most, most).astype(kind)


def setup_inputs(seed: int = 0) -> dict:
    seeds = jax.random.split(jax.random.key(seed), 16)
    layer_input = centred(seeds[0], (TOKENS, D), 1.0, 6.0, ((0, 32),))
    out_cot = noise_with(seeds[1], (TOKENS, D), 1.0, 6.0, ((0, 32),), (0, 1, 32, 2.75))
    expert_ids_keys = jax.random.split(jax.random.fold_in(seeds[2], 1), TOKENS // TOK_DEV)
    expert_ids_turns = jax.random.permutation(jax.random.fold_in(seeds[2], 3), TOKENS // TOK_DEV)
    expert_ids = jax.vmap(lambda own, number: deal_out(jax.random.fold_in(seeds[2], 2), own, number, TOK_DEV, EXPERTS, TOP, CAP, 1))(expert_ids_keys, expert_ids_turns).reshape((TOKENS, TOP))
    route_weight = jnp.clip(0.1 + 0.9 * jax.random.uniform(seeds[3], (TOKENS, TOP), jnp.float32) ** shard_levels(seeds[3], (TOKENS, TOP), ((0, 32),), -0.2, 0.2), 0.1, 1.0)
    w_gate = centred(seeds[4], (EXPERTS, D, FF), D ** -0.5, 0.125, ((0, 32), (2, 4)))
    w_up = centred(seeds[5], (EXPERTS, D, FF), D ** -0.5, 0.125, ((0, 32), (2, 4)))
    w_down = centred(seeds[6], (EXPERTS, FF, D), FF ** -0.5, 0.1875, ((0, 32), (1, 4)))
    out_proj = centred(seeds[7], (D, D_LRU), D_LRU ** -0.5, 0.1875, ((1, 4),))
    rec_input = centred(seeds[8], (TOKENS, D_LRU), 1.0, 6.0, ((0, 32), (1, 4)))
    gate_input = centred(seeds[9], (TOKENS, D_LRU), 1.0, 6.0, ((0, 32), (1, 4)))
    prev_state = centred(seeds[10], (TOKENS, D_LRU), 1.0, 6.0, ((0, 32), (1, 4)), jnp.float32)
    decay_param = draw_decay_param(jax.random.fold_in(seeds[15], 71), 0)
    extra_decay = draw_extra_decay(jax.random.fold_in(seeds[15], 71), 0)
    gate_a_w = centred(seeds[13], (RECURRENT_HEADS, HEAD_DIM, HEAD_DIM), HEAD_DIM ** -0.5, 0.5)
    gate_i_w = centred(seeds[14], (RECURRENT_HEADS, HEAD_DIM, HEAD_DIM), HEAD_DIM ** -0.5, 0.5)
    return {"layer_input": layer_input, "out_cot": out_cot, "expert_ids": expert_ids, "route_weight": route_weight, "w_gate": w_gate, "w_up": w_up, "w_down": w_down, "out_proj": out_proj, "rec_input": rec_input, "gate_input": gate_input, "prev_state": prev_state, "decay_param": decay_param, "extra_decay": extra_decay, "gate_a_w": gate_a_w, "gate_i_w": gate_i_w}


gelu_scale = 0.7978845608028654
gelu_cubic = 0.044715
decay_factor = 8.0

def gelu_pair(values_in):
    inner = gelu_scale * (values_in + gelu_cubic * values_in * values_in * values_in)
    bend = jnp.tanh(inner)
    active = 0.5 * values_in * (1.0 + bend)
    slope = 0.5 * (1.0 + bend) + 0.5 * values_in * (1.0 - bend * bend) * gelu_scale * (1.0 + 3.0 * gelu_cubic * values_in * values_in)
    return (active, slope)

def head_product(row_block, weights, backward):
    blocks = row_block.astype(jnp.float32).reshape(row_block.shape[0], RECURRENT_HEADS, HEAD_DIM)
    wide = weights.astype(jnp.float32)
    if backward:
        result = jnp.einsum('nhe,hde->nhd', blocks, wide)
    else:
        result = jnp.einsum('nhd,hde->nhe', blocks, wide)
    return result.reshape(row_block.shape[0], RECURRENT_HEADS * HEAD_DIM)

def chain_link(earlier, later):
    return (earlier[0] * later[0], later[0] * earlier[1] + later[1])

def expert_backward(operands):
    row_block, cot_block, gate_w, up_w, down_w = operands
    gate_pre = jnp.dot(row_block, gate_w, preferred_element_type=jnp.float32)
    up_pre = jnp.dot(row_block, up_w, preferred_element_type=jnp.float32)
    sigma = jax.nn.sigmoid(gate_pre)
    swish = gate_pre * sigma
    hidden = (swish * up_pre).astype(jnp.bfloat16)
    hidden_cot = jnp.dot(cot_block, down_w.T, preferred_element_type=jnp.float32)
    grad_down = jnp.dot(hidden.T, cot_block, preferred_element_type=jnp.float32)
    gate_cot = (hidden_cot * up_pre * sigma * (1.0 + gate_pre * (1.0 - sigma))).astype(jnp.bfloat16)
    up_cot = (hidden_cot * swish).astype(jnp.bfloat16)
    grad_gate = jnp.dot(row_block.T, gate_cot, preferred_element_type=jnp.float32)
    grad_up = jnp.dot(row_block.T, up_cot, preferred_element_type=jnp.float32)
    part_width = FF // N_TP
    gate_groups = gate_cot.astype(jnp.float32).reshape(EXP_ROWS, N_TP, part_width)
    up_groups = up_cot.astype(jnp.float32).reshape(EXP_ROWS, N_TP, part_width)
    gate_wide = gate_w.astype(jnp.float32).reshape(D, N_TP, part_width)
    up_wide = up_w.astype(jnp.float32).reshape(D, N_TP, part_width)
    terms = jnp.einsum('rgf,dgf->grd', gate_groups, gate_wide) + jnp.einsum('rgf,dgf->grd', up_groups, up_wide)
    rounded = lax.optimization_barrier(terms.astype(jnp.bfloat16))
    row_cot = lax.optimization_barrier(jnp.sum(rounded.astype(jnp.float32), axis=0)).astype(jnp.bfloat16)
    return (grad_gate, grad_up, grad_down, row_cot)

def reference(layer_input, out_cot, expert_ids, route_weight, w_gate, w_up, w_down, out_proj, rec_input, gate_input, prev_state, decay_param, extra_decay, gate_a_w, gate_i_w):
    slot_total = TOKENS * TOP
    device_ids = expert_ids.reshape(N_SP, TOK_DEV * TOP)
    onehot = (device_ids[:, :, None] == jnp.arange(EXPERTS, dtype=jnp.int32)[None, None, :]).astype(jnp.int32)
    earlier_count = lax.optimization_barrier(jnp.sum((jnp.cumsum(onehot, axis=1) - onehot) * onehot, axis=2)).astype(jnp.int32)
    source_index = jnp.arange(N_SP, dtype=jnp.int32)[:, None]
    places = (source_index * CAP + earlier_count).reshape(slot_total).astype(jnp.int32)
    flat_ids = expert_ids.reshape(slot_total).astype(jnp.int32)
    token_index = jnp.arange(slot_total, dtype=jnp.int32) // TOP
    weighted = (route_weight[:, :, None] * out_cot[:, None, :].astype(jnp.float32)).astype(jnp.bfloat16).reshape(slot_total, D)
    row_buffer = jnp.zeros((EXPERTS, EXP_ROWS, D), jnp.bfloat16).at[flat_ids, places].set(layer_input[token_index])
    cot_buffer = jnp.zeros((EXPERTS, EXP_ROWS, D), jnp.bfloat16).at[flat_ids, places].set(weighted)
    grad_gate, grad_up, grad_down, back_buffer = lax.map(expert_backward, (row_buffer, cot_buffer, w_gate, w_up, w_down))
    slot_cot = back_buffer[flat_ids, places].astype(jnp.float32).reshape(TOKENS, TOP, D)
    layer_cot = (out_cot.astype(jnp.float32) + lax.optimization_barrier(jnp.sum(slot_cot, axis=1))).astype(jnp.bfloat16)
    mix_cot = jnp.dot(layer_cot, out_proj, preferred_element_type=jnp.float32)
    rgate = jax.nn.sigmoid(head_product(rec_input, gate_a_w, False))
    igate = jax.nn.sigmoid(head_product(rec_input, gate_i_w, False))
    rate_scale = decay_factor * jax.nn.softplus(-decay_param)
    log_decay = -rate_scale[None, :] * rgate + jnp.repeat(extra_decay.T, HEAD_DIM, axis=1)
    decay = jnp.exp(log_decay)
    scale = jnp.sqrt(-jnp.expm1(2.0 * log_decay))
    values_in = rec_input.astype(jnp.float32)
    state = decay * prev_state + scale * igate * values_in
    gate_act, gate_slope = gelu_pair(gate_input.astype(jnp.float32))
    rec_output = (state * gate_act).astype(jnp.bfloat16)
    grad_out_proj = jnp.dot(layer_cot.T, rec_output, preferred_element_type=jnp.float32)
    next_decay = jnp.concatenate([decay[1:], jnp.zeros((1, D_LRU), jnp.float32)], axis=0)
    drive = mix_cot * gate_act
    _, state_cot = lax.associative_scan(chain_link, (next_decay, drive), reverse=True)
    gate_input_grad = (mix_cot * state * gate_slope).astype(jnp.bfloat16)
    log_cot = state_cot * (decay * prev_state - decay * decay / scale * igate * values_in)
    a_pre_cot = (log_cot * -rate_scale[None, :] * rgate * (1.0 - rgate)).astype(jnp.bfloat16)
    i_pre_cot = (state_cot * scale * values_in * igate * (1.0 - igate)).astype(jnp.bfloat16)
    rec_input_grad = (state_cot * scale * igate + head_product(a_pre_cot, gate_a_w, True) + head_product(i_pre_cot, gate_i_w, True)).astype(jnp.bfloat16)
    return (grad_gate, grad_up, grad_down, grad_out_proj, rec_input_grad, gate_input_grad)
```

```python
import functools
import jax
import jax.numpy as jnp
from jax import lax
from jax.experimental import pallas as pl
from jax.experimental.pallas import tpu as pltpu
from jax.sharding import Mesh, PartitionSpec as P

F32 = jnp.float32
BF16 = jnp.bfloat16
gelu_scale = 0.7978845608028654
gelu_cubic = 0.044715
decay_factor = 8.0


def params(limit_mib=48, **extra):
    return pltpu.CompilerParams(vmem_limit_bytes=limit_mib * 1024 * 1024, **extra)


def cost(flops, moved):
    return pl.CostEstimate(flops=flops, bytes_accessed=moved, transcendentals=0)


def whole(shape):
    return pl.BlockSpec(shape, lambda *_: (0,) * len(shape))


SMEM = pl.BlockSpec(memory_space=pltpu.SMEM)


def dot(a, b, dims=((1,), (0,))):
    return lax.dot_general(a, b, (dims, ((), ())), preferred_element_type=F32)


def sigmoid(v):
    return 1.0 / (1.0 + jnp.exp(-v))


def minus_expm1(v):
    series = 1.0 + v / 8.0
    for order in range(7, 1, -1):
        series = 1.0 + v / order * series
    return jnp.where(v > -0.5, -v * series, 1.0 - jnp.exp(v))


def early_kernel(
    where_ref, ids, rec, gate_in, prev, rates, extra, map_a, map_i,
    out_rec, out_act, out_b, out_ca, out_ci, out_cs, out_decay, out_seg, out_exp, out_block, out_sel,
    *, capacity, experts,
):
    tokens, channels = rec.shape
    heads = channels // 128
    first = where_ref[0] * heads
    for h in range(heads):
        cols = slice(h * 128, (h + 1) * 128)
        values_bf = rec[:, cols]
        x = values_bf.astype(F32)
        ra = sigmoid(dot(values_bf, map_a[first + h]))
        ig = sigmoid(dot(values_bf, map_i[first + h]))
        rate = rates[pl.ds(first + h, 1), :]
        log_decay = -rate * ra + extra[:, h : h + 1]
        decay = jnp.exp(log_decay)
        scale = jnp.sqrt(minus_expm1(2.0 * log_decay))
        before = prev[:, cols]
        state = decay * before + scale * ig * x
        g = gate_in[:, cols].astype(F32)
        bend = jnp.tanh(gelu_scale * (g + gelu_cubic * g * g * g))
        act = 0.5 * g * (1.0 + bend)
        slope = 0.5 * (1.0 + bend) + 0.5 * g * (1.0 - bend * bend) * gelu_scale * (
            1.0 + 3.0 * gelu_cubic * g * g
        )
        out_rec[:, cols] = (state * act).astype(BF16)
        out_act[:, cols] = act
        out_b[:, cols] = state * slope
        out_ca[:, cols] = (decay * before - decay * decay / scale * ig * x) * -rate * ra * (1.0 - ra)
        out_ci[:, cols] = scale * x * ig * (1.0 - ig)
        out_cs[:, cols] = scale * ig
        out_decay[h] = decay
    length = tokens // 8
    for h in range(heads):
        cols = slice(h * 128, (h + 1) * 128)
        product = jnp.ones((8, 128), F32)
        for i in range(length - 1, -1, -1):
            out_seg[h, pl.ds(i, 8, stride=length), :] = product
            product = product * out_decay[h, pl.ds(i, 8, stride=length), :]
        carry = jnp.ones((1, 128), F32)
        for k in range(7, -1, -1):
            rows = slice(k * length, (k + 1) * length)
            out_exp[rows, cols] = out_seg[h, rows, :] * carry
            carry = carry * product[k : k + 1, :]
        out_block[:, cols] = jnp.broadcast_to(carry, (8, 128))
    lane = lax.broadcasted_iota(jnp.int32, (tokens, 128), 1)
    first_id = ids[:, 0:1]
    second_id = ids[:, 1:2]
    one = (lane == first_id).astype(F32)
    two = (lane == second_id).astype(F32)
    lower = lax.broadcasted_iota(jnp.int32, (tokens, tokens), 0) > lax.broadcasted_iota(
        jnp.int32, (tokens, tokens), 1
    )
    rank = dot(lower.astype(F32).astype(BF16), (one + two).astype(BF16))
    place_one = first_id * capacity + jnp.sum(rank * one, axis=1, keepdims=True).astype(jnp.int32)
    place_two = second_id * capacity + jnp.sum(rank * two, axis=1, keepdims=True).astype(jnp.int32)
    slots = experts * capacity
    for at in range(0, slots, 256):
        slot = lax.broadcasted_iota(jnp.int32, (tokens, 256), 1) + at
        hit = (slot == place_one) | (slot == place_two)
        out_sel[:, at : at + 256] = jnp.where(hit, 1.0, 0.0).astype(BF16)


def early(position, ids, rec, gate_in, prev, rates, extra, map_a, map_i, capacity, experts):
    tokens, channels = rec.shape
    wide = jax.ShapeDtypeStruct((tokens, channels), F32)
    heads = jax.ShapeDtypeStruct((channels // 128, tokens, 128), F32)
    outs = (
        jax.ShapeDtypeStruct((tokens, channels), BF16),
        wide, wide, wide, wide, wide, heads, heads, wide,
        jax.ShapeDtypeStruct((8, channels), F32),
        jax.ShapeDtypeStruct((tokens, experts * capacity), BF16),
    )
    args = (position, ids, rec, gate_in, prev, rates, extra, map_a, map_i)
    return pl.pallas_call(
        functools.partial(early_kernel, capacity=capacity, experts=experts),
        out_shape=outs,
        in_specs=[SMEM] + [whole(a.shape) for a in args[1:]],
        out_specs=[whole(o.shape) for o in outs],
        compiler_params=params(),
        cost_estimate=cost(3 * 10**9, 8 * 2**20),
        name="early",
    )(*args)


def build_kernel(ids, weight, source, cot, rec, out, rank_ref, weight_ref, *, capacity, group):
    experts, tokens = rank_ref.shape
    width = source.shape[1]

    @pl.when(pl.program_id(0) == 0)
    def _():
        name = lax.broadcasted_iota(jnp.int32, (experts, tokens), 0)
        one = jnp.where(name == ids[0:1, :], 1.0, 0.0)
        two = jnp.where(name == ids[1:2, :], 1.0, 0.0)
        both = one + two
        upper = lax.broadcasted_iota(jnp.int32, (tokens, tokens), 0) < lax.broadcasted_iota(
            jnp.int32, (tokens, tokens), 1
        )
        rank = dot(both.astype(BF16), upper.astype(F32).astype(BF16))
        rank_ref[...] = jnp.where(both > 0.0, rank, -1.0)
        weight_ref[...] = one * weight[0:1, :] + two * weight[1:2, :]

    first = pl.program_id(0) * group
    place = lax.broadcasted_iota(jnp.int32, (capacity, tokens), 0).astype(F32)
    picks, weights = [], []
    for e in range(group):
        hit = place == rank_ref[pl.ds(first + e, 1), :]
        picks.append(jnp.where(hit, 1.0, 0.0))
        weights.append(
            jnp.sum(jnp.where(hit, weight_ref[pl.ds(first + e, 1), :], 0.0), axis=1, keepdims=True)
        )
    pick = jnp.concatenate(picks, axis=0).astype(BF16)
    by = jnp.concatenate(weights, axis=0)
    out[:, :width] = dot(pick, source[...]).astype(BF16)
    out[:, width : 2 * width] = (dot(pick, cot[...]) * by).astype(BF16)
    out[:, 2 * width :] = dot(pick, rec[...]).astype(BF16)


def build(ids, weight, source, cot, rec, capacity, experts, group=4):
    tokens, width = source.shape
    total = 2 * width + rec.shape[1]
    args = (ids, weight, source, cot, rec)
    return pl.pallas_call(
        functools.partial(build_kernel, capacity=capacity, group=group),
        out_shape=jax.ShapeDtypeStruct((experts * capacity, total), BF16),
        grid=(experts // group,),
        in_specs=[whole(a.shape) for a in args],
        out_specs=pl.BlockSpec((group * capacity, total), lambda i: (i, 0)),
        scratch_shapes=[pltpu.VMEM((experts, tokens), F32), pltpu.VMEM((experts, tokens), F32)],
        compiler_params=params(),
        cost_estimate=cost(6 * 10**9, 20 * 2**20),
        name="build",
    )(*args)


def weights_kernel(where_ref, w_gate, w_up, own, left, right, far, out_gate, out_up):
    at = where_ref[0]
    for step, piece in ((0, own), (3, left), (1, right), (2, far)):
        group = lax.rem(at + step, 4)
        out_gate[group] = dot(w_gate[...], piece[...], ((0,), (0,))).astype(BF16)
        out_up[group] = dot(w_up[...], piece[...], ((0,), (0,))).astype(BF16)


def folded_weights(position, w_gate, w_up, pieces):
    hidden, width = w_gate.shape[1], pieces[0].shape[1]
    args = (position, w_gate, w_up, *pieces)
    out = jax.ShapeDtypeStruct((4, hidden, width), BF16)
    return pl.pallas_call(
        weights_kernel,
        out_shape=(out, out),
        in_specs=[SMEM] + [whole(a.shape) for a in args[1:]],
        out_specs=[whole(out.shape)] * 2,
        compiler_params=params(),
        cost_estimate=cost(4 * 10**9, 7 * 2**20),
        name="folded",
    )(*args)


def expert_kernel(got_rows, got_cot, w_gate, w_up, w_down, fold_gate, fold_up, out_hidden, out_gate, out_up, out_mix):
    gate_pre = dot(got_rows[...], w_gate[...])
    up_pre = dot(got_rows[...], w_up[...])
    hidden_cot = dot(got_cot[...], w_down[...], ((1,), (1,)))
    sigma = sigmoid(gate_pre)
    swish = gate_pre * sigma
    out_hidden[...] = (swish * up_pre).astype(BF16)
    gate_cot = (hidden_cot * up_pre * sigma * (1.0 + gate_pre * (1.0 - sigma))).astype(BF16)
    up_cot = (hidden_cot * swish).astype(BF16)
    out_gate[...] = gate_cot
    out_up[...] = up_cot
    for c in range(4):
        out_mix[c] = (dot(gate_cot, fold_gate[c]) + dot(up_cot, fold_up[c])).astype(BF16)


def expert(got, w_gate, w_up, w_down, fold_gate, fold_up, steps=4):
    rows = got.shape[0]
    width, hidden = w_gate.shape
    block = rows // steps
    part = fold_gate.shape[2]
    narrow = jax.ShapeDtypeStruct((rows, hidden), BF16)
    mine = pl.BlockSpec((block, hidden), lambda i: (i, 0))
    return pl.pallas_call(
        expert_kernel,
        out_shape=(narrow, narrow, narrow, jax.ShapeDtypeStruct((4, rows, part), BF16)),
        grid=(steps,),
        in_specs=[
            pl.BlockSpec((block, width), lambda i: (i, 0)),
            pl.BlockSpec((block, width), lambda i: (i, 1)),
            *(whole(a.shape) for a in (w_gate, w_up, w_down, fold_gate, fold_up)),
        ],
        out_specs=[mine, mine, mine, pl.BlockSpec((4, block, part), lambda i: (0, i, 0))],
        compiler_params=params(),
        cost_estimate=cost(7 * 10**9, 18 * 2**20),
        name="expert",
    )(got, got, w_gate, w_up, w_down, fold_gate, fold_up)


def grads_kernel(got_rows, got_cot, hidden, gate_cot, up_cot, out_gate, out_up, out_down):
    out_gate[0] = dot(got_rows[...], gate_cot[...], ((0,), (0,)))
    out_up[0] = dot(got_rows[...], up_cot[...], ((0,), (0,)))
    out_down[0] = dot(hidden[...], got_cot[...], ((0,), (0,)))


def grads(got, hidden, gate_cot, up_cot, width, steps=4):
    rows, units = hidden.shape
    block = width // steps
    tall = pl.BlockSpec((1, block, units), lambda i: (0, i, 0))
    return pl.pallas_call(
        grads_kernel,
        out_shape=(
            jax.ShapeDtypeStruct((1, width, units), F32),
            jax.ShapeDtypeStruct((1, width, units), F32),
            jax.ShapeDtypeStruct((1, units, width), F32),
        ),
        grid=(steps,),
        in_specs=[
            pl.BlockSpec((rows, block), lambda i: (0, i)),
            pl.BlockSpec((rows, block), lambda i: (0, i + steps)),
            *(whole(a.shape) for a in (hidden, gate_cot, up_cot)),
        ],
        out_specs=[tall, tall, pl.BlockSpec((1, units, block), lambda i: (0, 0, i))],
        compiler_params=params(),
        cost_estimate=cost(4 * 10**9, 17 * 2**20),
        name="grads",
    )(got, got, hidden, gate_cot, up_cot)


def proj_kernel(where_ref, gate_cot, up_cot, w_gate, w_up, local, own, left, right, far, out):
    at = where_ref[0]
    core = where_ref[1]
    for step, piece in ((0, own), (3, left), (1, right), (2, far)):
        group = lax.rem(at + step, 4)
        push_gate = dot(gate_cot[...], piece[...], ((0,), (0,))).astype(BF16)
        push_up = dot(up_cot[...], piece[...], ((0,), (0,))).astype(BF16)
        term = dot(w_gate[...], push_gate) + dot(w_up[...], push_up)
        if step == 0:
            term = term + local[...]
        term = term.astype(BF16)
        lines = out.shape[3]
        for s in range(2 * out.shape[2]):
            slot = lax.rem(s % 2 + core, 2)
            out[slot, group, s // 2] = term[s * lines : (s + 1) * lines, :]


def proj(position, gate_cot, up_cot, w_gate, w_up, local, pieces, lines):
    width, part = w_gate.shape[0], pieces[0].shape[1]
    args = (position, gate_cot, up_cot, w_gate, w_up, local, *pieces)
    out = jax.ShapeDtypeStruct((2, 4, width // lines // 2, lines, part), BF16)
    return pl.pallas_call(
        proj_kernel,
        out_shape=out,
        in_specs=[SMEM] + [whole(a.shape) for a in args[1:]],
        out_specs=whole(out.shape),
        compiler_params=params(),
        cost_estimate=cost(4 * 10**9, 14 * 2**20),
        name="proj",
    )(*args)


def scan_kernel(back, sel, base, act, b, decay, seg, block, out_grad, out_local, out_pair, drive, part):
    tokens, channels = base.shape
    length = tokens // 8
    mix = base[...]
    total = back[0].astype(F32) + back[1].astype(F32) + back[2].astype(F32) + back[3].astype(F32)
    mix = mix + dot(sel[...], total.astype(BF16))
    out_grad[...] = (mix * b[...]).astype(BF16)
    push = mix * act[...]
    for h in range(channels // 128):
        cols = slice(h * 128, (h + 1) * 128)
        drive[h] = push[:, cols]
        value = drive[h, pl.ds(length - 1, 8, stride=length), :]
        part[h, pl.ds(length - 1, 8, stride=length), :] = value
        for i in range(length - 2, -1, -1):
            value = (
                drive[h, pl.ds(i, 8, stride=length), :]
                + decay[h, pl.ds(i + 1, 8, stride=length), :] * value
            )
            part[h, pl.ds(i, 8, stride=length), :] = value
        lead = decay[h, pl.ds(0, 8, stride=length), :]
        inner = seg[h, pl.ds(0, 8, stride=length), :]
        carry = jnp.zeros((1, 128), F32)
        for k in range(7, -1, -1):
            rows = slice(k * length, (k + 1) * length)
            out_local[rows, cols] = part[h, rows, :] + seg[h, rows, :] * carry
            one = slice(k, k + 1)
            carry = lead[one, :] * (value[one, :] + inner[one, :] * carry)
        out_pair[:, cols] = jnp.concatenate([carry, block[0:1, cols]], axis=0)


def scanned(back, sel, base, act, b, decay, seg, block):
    tokens, channels = base.shape
    args = (back, sel, base, act, b, decay, seg, block)
    outs = (
        jax.ShapeDtypeStruct((tokens, channels), BF16),
        jax.ShapeDtypeStruct((tokens, channels), F32),
        jax.ShapeDtypeStruct((2, channels), F32),
    )
    return pl.pallas_call(
        scan_kernel,
        out_shape=outs,
        in_specs=[whole(a.shape) for a in args],
        out_specs=[whole(o.shape) for o in outs],
        scratch_shapes=[pltpu.VMEM(decay.shape, F32), pltpu.VMEM(decay.shape, F32)],
        compiler_params=params(),
        cost_estimate=cost(4 * 10**8, 8 * 2**20),
        name="scanned",
    )(*args)


def final_kernel(where_ref, pairs, local, exp, ca, ci, cs, map_a, map_i, out):
    channels = local.shape[1]
    heads = channels // 128
    first = where_ref[0] * heads
    me = where_ref[2]
    carry = jnp.zeros((1, channels), F32)
    for s in range(pairs.shape[0] - 1, 0, -1):
        carry = jnp.where(me < s, pairs[s, 0:1, :] + pairs[s, 1:2, :] * carry, carry)
    for h in range(heads):
        cols = slice(h * 128, (h + 1) * 128)
        cot = local[:, cols] + exp[:, cols] * carry[:, cols]
        a_cot = (cot * ca[:, cols]).astype(BF16)
        i_cot = (cot * ci[:, cols]).astype(BF16)
        total = (
            cot * cs[:, cols]
            + dot(a_cot, map_a[first + h], ((1,), (1,)))
            + dot(i_cot, map_i[first + h], ((1,), (1,)))
        )
        out[:, cols] = total.astype(BF16)


def final(position, pairs, local, exp, ca, ci, cs, map_a, map_i):
    args = (position, pairs, local, exp, ca, ci, cs, map_a, map_i)
    return pl.pallas_call(
        final_kernel,
        out_shape=jax.ShapeDtypeStruct(local.shape, BF16),
        in_specs=[SMEM] + [whole(a.shape) for a in args[1:]],
        out_specs=whole(local.shape),
        compiler_params=params(),
        cost_estimate=cost(10**8, 4 * 2**20),
        name="final",
    )(*args)


def shifted(piece, by):
    return lax.ppermute(piece, "tp", [(i, (i + by) % 4) for i in range(4)])


def ring_gather(own):
    half = own.shape[0] // 2
    left, right = shifted(own, 1), shifted(own, -1)
    far = jnp.concatenate([shifted(left[:half], 1), shifted(right[half:], -1)], axis=0)
    return own, left, right, far


def per_device(
    layer_input, out_cot, expert_ids, route_weight, w_gate, w_up, w_down, out_proj,
    rec_input, gate_input, prev_state, decay_param, extra_decay, gate_a_w, gate_i_w,
):
    sources = lax.axis_size("sq") * lax.axis_size("core")
    tp = lax.axis_index("tp")
    core = lax.axis_index("core")
    sp = lax.axis_index("sq") * 2 + core
    position = jnp.stack([tp, core, sp]).astype(jnp.int32)
    w_gate, w_up, w_down = w_gate[0], w_up[0], w_down[0]
    tokens, width = layer_input.shape
    capacity = 5 * tokens * expert_ids.shape[1] // (4 * sources)
    rates = (decay_factor * jax.nn.softplus(-decay_param)).reshape(-1, gate_a_w.shape[1])
    rec_output, act, b, ca, ci, cs, decay, seg, exp, block, sel = early(
        position, expert_ids, rec_input, gate_input, prev_state, rates, extra_decay.T,
        gate_a_w, gate_i_w, capacity, sources,
    )
    send = build(
        expert_ids.T, route_weight.T, layer_input, out_cot, rec_output, capacity, sources
    )
    got = lax.all_to_all(
        send.reshape(sources, capacity, -1), ("sq", "core"), 0, 0, tiled=True
    ).reshape(sources * capacity, -1)
    fold_gate, fold_up = folded_weights(position, w_gate, w_up, ring_gather(out_proj))
    base = jnp.dot(out_cot, out_proj, preferred_element_type=F32)
    local_proj = lax.dot_general(
        out_cot, rec_output, (((0,), (0,)), ((), ())), preferred_element_type=F32
    )
    hidden, gate_cot, up_cot, mix = expert(got, w_gate, w_up, w_down, fold_gate, fold_up)
    back = lax.all_to_all(
        mix.reshape(4 * sources, capacity, -1), ("tp", "sq", "core"), 0, 0, tiled=True
    ).reshape(mix.shape)
    grad_gate, grad_up, grad_down = grads(got, hidden, gate_cot, up_cot, width)
    pieces = ring_gather(got[:, 2 * width :])
    lines = width // sources
    parts = proj(position, gate_cot, up_cot, w_gate, w_up, local_proj, pieces, lines)
    other = lax.ppermute(parts[1], "core", [(0, 1), (1, 0)])
    chip = (parts[0].astype(F32) + other.astype(F32)).astype(BF16)
    arrived = lax.all_to_all(
        chip.reshape(4 * chip.shape[1], lines, -1), ("tp", "sq"), 0, 0, tiled=True
    )
    grad_out_proj = arrived.astype(F32).sum(axis=0)
    gate_input_grad, local, pair = scanned(back, sel, base, act, b, decay, seg, block)
    pairs = lax.all_to_all(
        jnp.broadcast_to(pair[None], (sources, *pair.shape)), ("sq", "core"), 0, 0, tiled=True
    )
    rec_input_grad = final(position, pairs, local, exp, ca, ci, cs, gate_a_w, gate_i_w)
    return (grad_gate, grad_up, grad_down, grad_out_proj, rec_input_grad, gate_input_grad)


def solution(mesh):
    sp, tp = mesh.devices.shape
    inner = Mesh(mesh.devices.reshape(sp // 2, 2, tp), ("sq", "core", "tp"))
    sp = ("sq", "core")
    in_specs = (
        P(sp, None),
        P(sp, None),
        P(sp, None),
        P(sp, None),
        P(sp, None, "tp"),
        P(sp, None, "tp"),
        P(sp, "tp", None),
        P(None, "tp"),
        P(sp, "tp"),
        P(sp, "tp"),
        P(sp, "tp"),
        P(),
        P("tp", sp),
        P(),
        P(),
    )
    out_specs = (
        P(sp, None, "tp"),
        P(sp, None, "tp"),
        P(sp, "tp", None),
        P(sp, "tp"),
        P(sp, "tp"),
        P(sp, "tp"),
    )
    return jax.shard_map(
        per_device, mesh=inner, in_specs=in_specs, out_specs=out_specs, check_vma=False
    )
```

```python
import functools
import jax
import jax.numpy as jnp
from jax import lax
from jax.experimental import pallas as pl
from jax.experimental.pallas import tpu as pltpu
from jax.sharding import Mesh, PartitionSpec as P


F32 = jnp.float32
BF16 = jnp.bfloat16
gelu_scale = 0.7978845608028654
gelu_cubic = 0.044715
decay_factor = 8.0
ring_steps = (0, 3, 1, 2)


def params(limit_mib=48, **extra):
    return pltpu.CompilerParams(vmem_limit_bytes=limit_mib * 1024 * 1024, **extra)


def cost(flops, moved):
    return pl.CostEstimate(flops=flops, bytes_accessed=moved, transcendentals=0)


def whole(shape):
    return pl.BlockSpec(shape, lambda *_: (0,) * len(shape), pipeline_mode=pl.Buffered(1))


SMEM = pl.BlockSpec(memory_space=pltpu.SMEM)


def made(shape, dtype):
    return pltpu.HBM(shape, dtype)


def kept(arrays):
    return [pltpu.with_memory_space_constraint(a, pltpu.HBM) for a in arrays]


def dot(a, b, dims=((1,), (0,))):
    return lax.dot_general(a, b, (dims, ((), ())), preferred_element_type=F32)


def sigmoid(v):
    return 1.0 / (1.0 + jnp.exp(-v))


def minus_expm1(v):
    series = 1.0 + v / 8.0
    for order in range(7, 1, -1):
        series = 1.0 + v / order * series
    return jnp.where(v > -0.5, -v * series, 1.0 - jnp.exp(v))


def early_kernel(
    where_ref, ids, rec, gate_in, prev, rates, extra, map_a, map_i,
    out_rec, out_act, out_b, out_ca, out_ci, out_cs, out_decay, out_seg, out_exp, out_block, out_sel,
    *, capacity, experts,
):
    tokens, channels = rec.shape
    heads = channels // 128
    first = where_ref[0] * heads
    for h in range(heads):
        cols = slice(h * 128, (h + 1) * 128)
        values_bf = rec[:, cols]
        x = values_bf.astype(F32)
        ra = sigmoid(dot(values_bf, map_a[first + h]))
        ig = sigmoid(dot(values_bf, map_i[first + h]))
        rate = rates[pl.ds(first + h, 1), :]
        log_decay = -rate * ra + extra[:, h : h + 1]
        decay = jnp.exp(log_decay)
        scale = jnp.sqrt(minus_expm1(2.0 * log_decay))
        before = prev[:, cols]
        state = decay * before + scale * ig * x
        g = gate_in[:, cols].astype(F32)
        bend = jnp.tanh(gelu_scale * (g + gelu_cubic * g * g * g))
        act = 0.5 * g * (1.0 + bend)
        slope = 0.5 * (1.0 + bend) + 0.5 * g * (1.0 - bend * bend) * gelu_scale * (
            1.0 + 3.0 * gelu_cubic * g * g
        )
        out_rec[:, cols] = (state * act).astype(BF16)
        out_act[:, cols] = act
        out_b[:, cols] = state * slope
        out_ca[:, cols] = (decay * before - decay * decay / scale * ig * x) * -rate * ra * (1.0 - ra)
        out_ci[:, cols] = scale * x * ig * (1.0 - ig)
        out_cs[:, cols] = scale * ig
        out_decay[h] = decay
    length = tokens // 8
    for h in range(heads):
        cols = slice(h * 128, (h + 1) * 128)
        product = jnp.ones((8, 128), F32)
        for i in range(length - 1, -1, -1):
            out_seg[h, pl.ds(i, 8, stride=length), :] = product
            product = product * out_decay[h, pl.ds(i, 8, stride=length), :]
        carry = jnp.ones((1, 128), F32)
        for k in range(7, -1, -1):
            rows = slice(k * length, (k + 1) * length)
            out_exp[rows, cols] = out_seg[h, rows, :] * carry
            carry = carry * product[k : k + 1, :]
        out_block[:, cols] = jnp.broadcast_to(carry, (8, 128))
    lane = lax.broadcasted_iota(jnp.int32, (tokens, 128), 1)
    first_id = ids[:, 0:1]
    second_id = ids[:, 1:2]
    one = (lane == first_id).astype(F32)
    two = (lane == second_id).astype(F32)
    lower = lax.broadcasted_iota(jnp.int32, (tokens, tokens), 0) > lax.broadcasted_iota(
        jnp.int32, (tokens, tokens), 1
    )
    rank = dot(lower.astype(F32).astype(BF16), (one + two).astype(BF16))
    place_one = first_id * capacity + jnp.sum(rank * one, axis=1, keepdims=True).astype(jnp.int32)
    place_two = second_id * capacity + jnp.sum(rank * two, axis=1, keepdims=True).astype(jnp.int32)
    slots = experts * capacity
    for at in range(0, slots, 256):
        slot = lax.broadcasted_iota(jnp.int32, (tokens, 256), 1) + at
        hit = (slot == place_one) | (slot == place_two)
        out_sel[:, at : at + 256] = jnp.where(hit, 1.0, 0.0).astype(BF16)


def early(position, ids, rec, gate_in, prev, rates, extra, map_a, map_i, capacity, experts):
    tokens, channels = rec.shape
    wide = made((tokens, channels), F32)
    heads = made((channels // 128, tokens, 128), F32)
    outs = (
        made((tokens, channels), BF16),
        wide, wide, wide, wide, wide, heads, heads, wide,
        made((8, channels), F32),
        made((tokens, experts * capacity), BF16),
    )
    args = (position, ids, rec, gate_in, prev, rates, extra, map_a, map_i)
    return pl.pallas_call(
        functools.partial(early_kernel, capacity=capacity, experts=experts),
        out_shape=outs,
        in_specs=[SMEM] + [whole(a.shape) for a in args[1:]],
        out_specs=[whole(o.shape) for o in outs],
        compiler_params=params(14),
        cost_estimate=cost(3 * 10**9, 8 * 2**20),
        name="early",
    )(args[0], *kept(args[1:]))


def build_kernel(where_ref, ids, weight, *refs, capacity, group, weighted):
    sources, out, rank_ref, weight_ref = refs[:-3], refs[-3], refs[-2], refs[-1]
    experts, tokens = rank_ref.shape

    @pl.when(pl.program_id(0) == 0)
    def _():
        name = lax.broadcasted_iota(jnp.int32, (experts, tokens), 0)
        one = jnp.where(name == ids[0:1, :], 1.0, 0.0)
        two = jnp.where(name == ids[1:2, :], 1.0, 0.0)
        both = one + two
        upper = lax.broadcasted_iota(jnp.int32, (tokens, tokens), 0) < lax.broadcasted_iota(
            jnp.int32, (tokens, tokens), 1
        )
        rank = dot(both.astype(BF16), upper.astype(F32).astype(BF16))
        rank_ref[...] = jnp.where(both > 0.0, rank, -1.0)
        weight_ref[...] = one * weight[0:1, :] + two * weight[1:2, :]

    first = pl.program_id(0) * group
    place = lax.broadcasted_iota(jnp.int32, (capacity, tokens), 0).astype(F32)
    picks, weights = [], []
    for e in range(group):
        hit = place == rank_ref[pl.ds(first + e, 1), :]
        picks.append(jnp.where(hit, 1.0, 0.0))
        weights.append(
            jnp.sum(jnp.where(hit, weight_ref[pl.ds(first + e, 1), :], 0.0), axis=1, keepdims=True)
        )
    pick = jnp.concatenate(picks, axis=0).astype(BF16)
    by = jnp.concatenate(weights, axis=0)
    at = 0
    for source, scaled in zip(sources, weighted):
        rows = dot(pick, source[...])
        if scaled:
            rows = rows * by
        out[:, at : at + source.shape[1]] = rows.astype(BF16)
        at += source.shape[1]


def build(position, ids, weight, parts, capacity, experts, group=4):
    tokens = ids.shape[1]
    total = sum(width for _, width, _, _ in parts)
    specs = [pl.BlockSpec(ids.shape, lambda i, where: (0, 0))] * 2
    for _, width, column, _ in parts:
        specs.append(pl.BlockSpec((tokens, width), functools.partial(column_block, column)))
    return pl.pallas_call(
        functools.partial(
            build_kernel, capacity=capacity, group=group, weighted=tuple(p[3] for p in parts)
        ),
        out_shape=made((experts * capacity, total), BF16),
        grid_spec=pltpu.PrefetchScalarGridSpec(
            num_scalar_prefetch=1,
            grid=(experts // group,),
            in_specs=specs,
            out_specs=pl.BlockSpec((group * capacity, total), lambda i, where: (i, 0)),
            scratch_shapes=[pltpu.VMEM((experts, tokens), F32), pltpu.VMEM((experts, tokens), F32)],
        ),
        compiler_params=params(14),
        cost_estimate=cost(1400000 * total, 5000 * total),
    )(position, *kept([ids, weight, *(p[0] for p in parts)]))


def column_block(column, i, where):
    return (0, where[0] if column is None else column)


def weights_kernel(where_ref, w_gate, w_up, *refs):
    pieces, out_gate, out_up = refs[:-2], refs[-2], refs[-1]
    at = where_ref[0]
    for n, step in enumerate(ring_steps):
        group = lax.rem(at + step, 4)
        top, bottom = pieces[2 * n], pieces[2 * n + 1]
        half = top.shape[0]
        for weights, out in ((w_gate, out_gate), (w_up, out_up)):
            out[group] = (
                dot(weights[:half, :], top[...], ((0,), (0,)))
                + dot(weights[half:, :], bottom[...], ((0,), (0,)))
            ).astype(BF16)


def folded_weights(position, w_gate, w_up, pieces):
    hidden, width = w_gate.shape[1], pieces[0].shape[1]
    args = (position, w_gate, w_up, *pieces)
    out = made((4, hidden, width), BF16)
    return pl.pallas_call(
        weights_kernel,
        out_shape=(out, out),
        in_specs=[SMEM] + [whole(a.shape) for a in args[1:]],
        out_specs=[whole(out.shape)] * 2,
        compiler_params=params(16),
        cost_estimate=cost(4 * 10**9, 7 * 2**20),
        name="folded",
    )(position, *kept([w_gate, w_up]), *pieces)


def expert_kernel(where_ref, got_rows, got_cot, *refs, row_part, cot_part):
    pieces = refs[:8]
    w_gate, w_up, w_down, fold_gate, fold_up, out_hidden, out_gate, out_up, out_mix = refs[8:]
    at = where_ref[0]
    upper = pl.program_id(0) < pl.num_programs(0) // 2
    rows, cots = got_rows[...], got_cot[...]
    gate_pre = dot(rows, w_gate[4 * row_part :, :])
    up_pre = dot(rows, w_up[4 * row_part :, :])
    hidden_cot = dot(cots, w_down[:, 4 * cot_part :], ((1,), (1,)))
    for n, step in enumerate(ring_steps):
        group = lax.rem(at + step, 4)
        piece = jnp.where(upper, pieces[2 * n][...], pieces[2 * n + 1][...])
        lines = pl.ds(pl.multiple_of(group * row_part, row_part), row_part)
        columns = pl.ds(pl.multiple_of(group * cot_part, 128), cot_part)
        gate_pre = gate_pre + dot(piece[:, :row_part], w_gate[lines, :])
        up_pre = up_pre + dot(piece[:, :row_part], w_up[lines, :])
        hidden_cot = hidden_cot + dot(piece[:, row_part:], w_down[:, columns], ((1,), (1,)))
    sigma = sigmoid(gate_pre)
    swish = gate_pre * sigma
    out_hidden[...] = (swish * up_pre).astype(BF16)
    gate_cot = (hidden_cot * up_pre * sigma * (1.0 + gate_pre * (1.0 - sigma))).astype(BF16)
    up_cot = (hidden_cot * swish).astype(BF16)
    out_gate[...] = gate_cot
    out_up[...] = up_cot
    for c in range(4):
        out_mix[c] = (dot(gate_cot, fold_gate[c]) + dot(up_cot, fold_up[c])).astype(BF16)


def expert(position, got, pieces, w_gate, w_up, w_down, fold_gate, fold_up, row_part, cot_part, steps=4):
    rows = got.shape[0]
    width, hidden = w_gate.shape
    block = rows // steps
    part = fold_gate.shape[2]
    half = steps // 2
    row_rest, cot_rest = width - 4 * row_part, width - 4 * cot_part
    narrow = made((rows, hidden), BF16)
    mine = pl.BlockSpec((block, hidden), lambda i: (i, 0))
    top = pl.BlockSpec((block, row_part + cot_part), lambda i: (jnp.minimum(i, half - 1), 0))
    bottom = pl.BlockSpec((block, row_part + cot_part), lambda i: (jnp.maximum(i - half, 0), 0))
    return pl.pallas_call(
        functools.partial(expert_kernel, row_part=row_part, cot_part=cot_part),
        out_shape=(narrow, narrow, narrow, made((4, rows, part), BF16)),
        grid=(steps,),
        in_specs=[
            SMEM,
            pl.BlockSpec((block, row_rest), lambda i: (i, 0)),
            pl.BlockSpec((block, cot_rest), lambda i: (i, row_rest // cot_rest)),
            *([top, bottom] * 4),
            *(whole(a.shape) for a in (w_gate, w_up, w_down, fold_gate, fold_up)),
        ],
        out_specs=[mine, mine, mine, pl.BlockSpec((4, block, part), lambda i: (0, i, 0))],
        compiler_params=params(30),
        cost_estimate=cost(7 * 10**9, 18 * 2**20),
        name="expert",
    )(position, *kept([got, got]), *pieces, *kept([w_gate, w_up, w_down, fold_gate, fold_up]))


def grads_kernel(where_ref, got_rows, got_cot, *refs, row_part, cot_part):
    pieces = refs[:8]
    hidden, gate_cot, up_cot, out_gate, out_up, out_down = refs[8:]
    at = where_ref[0]
    first = ((0,), (0,))
    rows = got_rows[...]
    out_gate[0, 4 * row_part :, :] = dot(rows, gate_cot[...], first)
    out_up[0, 4 * row_part :, :] = dot(rows, up_cot[...], first)
    out_down[0, :, 4 * cot_part :] = dot(hidden[...], got_cot[...], first)
    for n, step in enumerate(ring_steps):
        group = lax.rem(at + step, 4)
        top, bottom = pieces[2 * n], pieces[2 * n + 1]
        half = top.shape[0]
        lines = pl.ds(pl.multiple_of(group * row_part, row_part), row_part)
        columns = pl.ds(pl.multiple_of(group * cot_part, 128), cot_part)
        for cot, out in ((gate_cot, out_gate), (up_cot, out_up)):
            out[0, lines, :] = dot(top[:, :row_part], cot[:half, :], first) + dot(
                bottom[:, :row_part], cot[half:, :], first
            )
        out_down[0, :, columns] = dot(hidden[:half, :], top[:, row_part:], first) + dot(
            hidden[half:, :], bottom[:, row_part:], first
        )


def grads(position, got, pieces, hidden, gate_cot, up_cot, width, row_part, cot_part):
    rows, units = hidden.shape
    row_rest, cot_rest = width - 4 * row_part, width - 4 * cot_part
    outs = (
        made((1, width, units), F32),
        made((1, width, units), F32),
        made((1, units, width), F32),
    )
    tail = (*pieces, hidden, gate_cot, up_cot)
    return pl.pallas_call(
        functools.partial(grads_kernel, row_part=row_part, cot_part=cot_part),
        out_shape=outs,
        grid=(1,),
        in_specs=[
            SMEM,
            pl.BlockSpec((rows, row_rest), lambda i: (0, 0), pipeline_mode=pl.Buffered(1)),
            pl.BlockSpec(
                (rows, cot_rest), lambda i: (0, row_rest // cot_rest), pipeline_mode=pl.Buffered(1)
            ),
            *(whole(a.shape) for a in tail),
        ],
        out_specs=[whole(o.shape) for o in outs],
        compiler_params=params(30),
        cost_estimate=cost(4 * 10**9, 17 * 2**20),
        name="grads",
    )(position, *kept([got, got]), *pieces, *kept(tail[len(pieces) :]))


def proj_kernel(where_ref, gate_cot, up_cot, w_gate, w_up, local, *refs):
    pieces, out = refs[:-1], refs[-1]
    at = where_ref[0]
    core = where_ref[1]
    first = ((0,), (0,))
    for n, step in enumerate(ring_steps):
        group = lax.rem(at + step, 4)
        top, bottom = pieces[2 * n], pieces[2 * n + 1]
        half = top.shape[0]
        push_gate, push_up = (
            (dot(cot[:half, :], top[...], first) + dot(cot[half:, :], bottom[...], first)).astype(BF16)
            for cot in (gate_cot, up_cot)
        )
        term = dot(w_gate[...], push_gate) + dot(w_up[...], push_up)
        if step == 0:
            term = term + local[...]
        term = term.astype(BF16)
        lines = out.shape[3]
        for s in range(2 * out.shape[2]):
            slot = lax.rem(s % 2 + core, 2)
            out[slot, group, s // 2] = term[s * lines : (s + 1) * lines, :]


def proj(position, gate_cot, up_cot, w_gate, w_up, local, pieces, lines):
    width, part = w_gate.shape[0], pieces[0].shape[1]
    args = (position, gate_cot, up_cot, w_gate, w_up, local, *pieces)
    out = made((2, 4, width // lines // 2, lines, part), BF16)
    return pl.pallas_call(
        proj_kernel,
        out_shape=out,
        in_specs=[SMEM] + [whole(a.shape) for a in args[1:]],
        out_specs=whole(out.shape),
        compiler_params=params(22),
        cost_estimate=cost(4 * 10**9, 14 * 2**20),
        name="proj",
    )(position, *kept(args[1:6]), *pieces)


def scan_kernel(back, sel, base, act, b, decay, seg, block, out_grad, out_local, out_pair, drive, part):
    tokens, channels = base.shape
    length = tokens // 8
    mix = base[...]
    total = back[0].astype(F32) + back[1].astype(F32) + back[2].astype(F32) + back[3].astype(F32)
    mix = mix + dot(sel[...], total.astype(BF16))
    out_grad[...] = (mix * b[...]).astype(BF16)
    push = mix * act[...]
    for h in range(channels // 128):
        cols = slice(h * 128, (h + 1) * 128)
        drive[h] = push[:, cols]
        value = drive[h, pl.ds(length - 1, 8, stride=length), :]
        part[h, pl.ds(length - 1, 8, stride=length), :] = value
        for i in range(length - 2, -1, -1):
            value = (
                drive[h, pl.ds(i, 8, stride=length), :]
                + decay[h, pl.ds(i + 1, 8, stride=length), :] * value
            )
            part[h, pl.ds(i, 8, stride=length), :] = value
        lead = decay[h, pl.ds(0, 8, stride=length), :]
        inner = seg[h, pl.ds(0, 8, stride=length), :]
        carry = jnp.zeros((1, 128), F32)
        for k in range(7, -1, -1):
            rows = slice(k * length, (k + 1) * length)
            out_local[rows, cols] = part[h, rows, :] + seg[h, rows, :] * carry
            one = slice(k, k + 1)
            carry = lead[one, :] * (value[one, :] + inner[one, :] * carry)
        out_pair[:, cols] = jnp.concatenate([carry, block[0:1, cols]], axis=0)


def scanned(back, sel, base, act, b, decay, seg, block):
    tokens, channels = base.shape
    args = (back, sel, base, act, b, decay, seg, block)
    outs = (
        made((tokens, channels), BF16),
        made((tokens, channels), F32),
        made((2, channels), F32),
    )
    return pl.pallas_call(
        scan_kernel,
        out_shape=outs,
        in_specs=[whole(a.shape) for a in args],
        out_specs=[whole(o.shape) for o in outs],
        scratch_shapes=[pltpu.VMEM(decay.shape, F32), pltpu.VMEM(decay.shape, F32)],
        compiler_params=params(14),
        cost_estimate=cost(4 * 10**8, 8 * 2**20),
        name="scanned",
    )(back, *kept(args[1:]))


def final_kernel(where_ref, carry, local, exp, ca, ci, cs, map_a, map_i, out):
    channels = local.shape[1]
    heads = channels // 128
    first = where_ref[0] * heads
    for h in range(heads):
        cols = slice(h * 128, (h + 1) * 128)
        cot = local[:, cols] + exp[:, cols] * carry[0:1, cols]
        a_cot = (cot * ca[:, cols]).astype(BF16)
        i_cot = (cot * ci[:, cols]).astype(BF16)
        total = (
            cot * cs[:, cols]
            + dot(a_cot, map_a[first + h], ((1,), (1,)))
            + dot(i_cot, map_i[first + h], ((1,), (1,)))
        )
        out[:, cols] = total.astype(BF16)


def final(position, carry, local, exp, ca, ci, cs, map_a, map_i):
    args = (position, carry, local, exp, ca, ci, cs, map_a, map_i)
    return pl.pallas_call(
        final_kernel,
        out_shape=made(local.shape, BF16),
        in_specs=[SMEM] + [whole(a.shape) for a in args[1:]],
        out_specs=whole(local.shape),
        compiler_params=params(8),
        cost_estimate=cost(10**8, 4 * 2**20),
        name="final",
    )(position, carry, *kept(args[2:]))


def shifted(piece, by):
    return lax.ppermute(piece, "tp", [(i, (i + by) % 4) for i in range(4)])


def ring_gather(top, bottom):
    left_top, right_bottom = shifted(top, 1), shifted(bottom, -1)
    left_bottom, right_top = shifted(bottom, 1), shifted(top, -1)
    far_top, far_bottom = shifted(left_top, 1), shifted(right_bottom, -1)
    return top, bottom, left_top, left_bottom, right_top, right_bottom, far_top, far_bottom


def later(pair, by, length):
    return lax.ppermute(pair, ("sq", "core"), [(i, i - by) for i in range(by, length)])


def joined(near, far):
    return jnp.stack([near[0] + near[1] * far[0], near[1] * far[1]])


def carried(pair, length):
    one, two, three, four = (later(pair, by, length) for by in (1, 2, 3, 4))
    pair = joined(joined(one, two), joined(three, four))
    one, two, three = (later(pair, by, length) for by in (4, 8, 12))
    pair = joined(joined(pair, one), joined(two, three))
    return joined(pair, later(pair, 16, length))


def per_device(
    layer_input, out_cot, expert_ids, route_weight, w_gate, w_up, w_down, out_proj,
    rec_input, gate_input, prev_state, decay_param, extra_decay, gate_a_w, gate_i_w,
):
    sources = lax.axis_size("sq") * lax.axis_size("core")
    tp = lax.axis_index("tp")
    core = lax.axis_index("core")
    sp_axes = ("sq", "core")
    position = jnp.stack([tp, core]).astype(jnp.int32)
    w_gate, w_up, w_down = w_gate[0], w_up[0], w_down[0]
    tokens, width = layer_input.shape
    capacity = 5 * tokens * expert_ids.shape[1] // (4 * sources)
    slots = sources * capacity
    row_part, cot_part = width // 8, 3 * width // 16
    row_rest, cot_rest = width - 4 * row_part, width - 4 * cot_part
    ids, weight = expert_ids.T, route_weight.T

    def exchanged(rows):
        return lax.all_to_all(
            rows.reshape(sources, capacity, -1), sp_axes, 0, 0, tiled=True
        ).reshape(rows.shape)

    spread = build(
        position, ids, weight,
        [(layer_input, row_part, None, False), (out_cot, cot_part, None, True)],
        capacity, sources,
    )
    spread = exchanged(spread)
    half = out_proj.shape[0] // 2
    projections = ring_gather(out_proj[:half], out_proj[half:])
    fold_gate, fold_up = folded_weights(position, w_gate, w_up, projections)
    rates = (decay_factor * jax.nn.softplus(-decay_param)).reshape(-1, gate_a_w.shape[1])
    rec_output, act, b, ca, ci, cs, decay, seg, exp, block, sel = early(
        position, expert_ids, rec_input, gate_input, prev_state, rates, extra_decay.T,
        gate_a_w, gate_i_w, capacity, sources,
    )
    direct = build(
        position, ids, weight,
        [
            (layer_input, row_rest, 4 * row_part // row_rest, False),
            (out_cot, cot_rest, 4 * cot_part // cot_rest, True),
            (rec_output, rec_output.shape[1], 0, False),
        ],
        capacity, sources,
    )
    got = exchanged(direct)
    pieces = ring_gather(spread[: slots // 2], spread[slots // 2 :])
    base = jnp.dot(out_cot, out_proj, preferred_element_type=F32)
    local_proj = lax.dot_general(
        out_cot, rec_output, (((0,), (0,)), ((), ())), preferred_element_type=F32
    )
    hidden, gate_cot, up_cot, mix = expert(
        position, got, pieces, w_gate, w_up, w_down, fold_gate, fold_up, row_part, cot_part
    )
    back = lax.all_to_all(
        mix.reshape(4 * sources, capacity, -1), ("tp", *sp_axes), 0, 0, tiled=True
    ).reshape(mix.shape)
    grad_gate, grad_up, grad_down = grads(
        position, got, pieces, hidden, gate_cot, up_cot, width, row_part, cot_part
    )
    start = row_rest + cot_rest
    recs = ring_gather(got[: slots // 2, start:], got[slots // 2 :, start:])
    lines = width // sources
    parts = proj(position, gate_cot, up_cot, w_gate, w_up, local_proj, recs, lines)
    other = lax.ppermute(parts[1], "core", [(0, 1), (1, 0)])
    chip = (parts[0].astype(F32) + other.astype(F32)).astype(BF16)
    arrived = lax.all_to_all(
        chip.reshape(4 * chip.shape[1], lines, -1), ("tp", "sq"), 0, 0, tiled=True
    )
    grad_out_proj = arrived.astype(F32).sum(axis=0)
    gate_input_grad, local, pair = scanned(back, sel, base, act, b, decay, seg, block)
    carry = carried(pair, sources)
    rec_input_grad = final(position, carry, local, exp, ca, ci, cs, gate_a_w, gate_i_w)
    return (grad_gate, grad_up, grad_down, grad_out_proj, rec_input_grad, gate_input_grad)


def solution(mesh):
    sp, tp = mesh.devices.shape
    inner = Mesh(mesh.devices.reshape(sp // 2, 2, tp), ("sq", "core", "tp"))
    sp = ("sq", "core")
    in_specs = (
        P(sp, None),
        P(sp, None),
        P(sp, None),
        P(sp, None),
        P(sp, None, "tp"),
        P(sp, None, "tp"),
        P(sp, "tp", None),
        P(None, "tp"),
        P(sp, "tp"),
        P(sp, "tp"),
        P(sp, "tp"),
        P(),
        P("tp", sp),
        P(),
        P(),
    )
    out_specs = (
        P(sp, None, "tp"),
        P(sp, None, "tp"),
        P(sp, "tp", None),
        P(sp, "tp"),
        P(sp, "tp"),
        P(sp, "tp"),
    )
    return jax.shard_map(
        per_device, mesh=inner, in_specs=in_specs, out_specs=out_specs, check_vma=False
    )
```

```python
import functools
import jax
import jax.numpy as jnp
from jax import lax
from jax.experimental import pallas as pl
from jax.experimental.pallas import tpu as pltpu
from jax.sharding import Mesh, PartitionSpec as P


F32 = jnp.float32
BF16 = jnp.bfloat16
gelu_scale = 0.7978845608028654
gelu_cubic = 0.044715
decay_factor = 8.0
ring_steps = (0, 3, 1, 2)


def params(limit_mib=48, **extra):
    return pltpu.CompilerParams(vmem_limit_bytes=limit_mib * 1024 * 1024, **extra)


def cost(flops, moved):
    return pl.CostEstimate(flops=flops, bytes_accessed=moved, transcendentals=0)


def whole(shape):
    return pl.BlockSpec(shape, lambda *_: (0,) * len(shape), pipeline_mode=pl.Buffered(1))


SMEM = pl.BlockSpec(memory_space=pltpu.SMEM)


def made(shape, dtype):
    return pltpu.HBM(shape, dtype)


def kept(arrays):
    return [pltpu.with_memory_space_constraint(a, pltpu.HBM) for a in arrays]


def dot(a, b, dims=((1,), (0,))):
    return lax.dot_general(a, b, (dims, ((), ())), preferred_element_type=F32)


def sigmoid(v):
    return 1.0 / (1.0 + jnp.exp(-v))


def minus_expm1(v):
    series = 1.0 + v / 8.0
    for order in range(7, 1, -1):
        series = 1.0 + v / order * series
    return jnp.where(v > -0.5, -v * series, 1.0 - jnp.exp(v))


def early_kernel(
    where_ref, ids, rec, gate_in, prev, rates, extra, map_a, map_i,
    out_rec, out_act, out_b, out_ca, out_ci, out_cs, out_decay, out_seg, out_exp, out_block, out_sel,
    *, capacity, experts,
):
    tokens, channels = rec.shape
    heads = channels // 128
    first = where_ref[0] * heads
    for h in range(heads):
        cols = slice(h * 128, (h + 1) * 128)
        values_bf = rec[:, cols]
        x = values_bf.astype(F32)
        ra = sigmoid(dot(values_bf, map_a[first + h]))
        ig = sigmoid(dot(values_bf, map_i[first + h]))
        rate = rates[pl.ds(first + h, 1), :]
        log_decay = -rate * ra + extra[:, h : h + 1]
        decay = jnp.exp(log_decay)
        scale = jnp.sqrt(minus_expm1(2.0 * log_decay))
        before = prev[:, cols]
        state = decay * before + scale * ig * x
        g = gate_in[:, cols].astype(F32)
        bend = jnp.tanh(gelu_scale * (g + gelu_cubic * g * g * g))
        act = 0.5 * g * (1.0 + bend)
        slope = 0.5 * (1.0 + bend) + 0.5 * g * (1.0 - bend * bend) * gelu_scale * (
            1.0 + 3.0 * gelu_cubic * g * g
        )
        out_rec[:, cols] = (state * act).astype(BF16)
        out_act[:, cols] = act
        out_b[:, cols] = state * slope
        out_ca[:, cols] = (decay * before - decay * decay / scale * ig * x) * -rate * ra * (1.0 - ra)
        out_ci[:, cols] = scale * x * ig * (1.0 - ig)
        out_cs[:, cols] = scale * ig
        out_decay[h] = decay
    length = tokens // 8
    for h in range(heads):
        cols = slice(h * 128, (h + 1) * 128)
        product = jnp.ones((8, 128), F32)
        for i in range(length - 1, -1, -1):
            out_seg[h, pl.ds(i, 8, stride=length), :] = product
            product = product * out_decay[h, pl.ds(i, 8, stride=length), :]
        carry = jnp.ones((1, 128), F32)
        for k in range(7, -1, -1):
            rows = slice(k * length, (k + 1) * length)
            out_exp[rows, cols] = out_seg[h, rows, :] * carry
            carry = carry * product[k : k + 1, :]
        out_block[:, cols] = jnp.broadcast_to(carry, (8, 128))
    lane = lax.broadcasted_iota(jnp.int32, (tokens, 128), 1)
    first_id = ids[:, 0:1]
    second_id = ids[:, 1:2]
    one = (lane == first_id).astype(F32)
    two = (lane == second_id).astype(F32)
    lower = lax.broadcasted_iota(jnp.int32, (tokens, tokens), 0) > lax.broadcasted_iota(
        jnp.int32, (tokens, tokens), 1
    )
    rank = dot(lower.astype(F32).astype(BF16), (one + two).astype(BF16))
    place_one = first_id * capacity + jnp.sum(rank * one, axis=1, keepdims=True).astype(jnp.int32)
    place_two = second_id * capacity + jnp.sum(rank * two, axis=1, keepdims=True).astype(jnp.int32)
    slots = experts * capacity
    for at in range(0, slots, 256):
        slot = lax.broadcasted_iota(jnp.int32, (tokens, 256), 1) + at
        hit = (slot == place_one) | (slot == place_two)
        out_sel[:, at : at + 256] = jnp.where(hit, 1.0, 0.0).astype(BF16)


def early(position, ids, rec, gate_in, prev, rates, extra, map_a, map_i, capacity, experts):
    tokens, channels = rec.shape
    wide = made((tokens, channels), F32)
    heads = made((channels // 128, tokens, 128), F32)
    outs = (
        made((tokens, channels), BF16),
        wide, wide, wide, wide, wide, heads, heads, wide,
        made((8, channels), F32),
        made((tokens, experts * capacity), BF16),
    )
    args = (position, ids, rec, gate_in, prev, rates, extra, map_a, map_i)
    return pl.pallas_call(
        functools.partial(early_kernel, capacity=capacity, experts=experts),
        out_shape=outs,
        in_specs=[SMEM] + [whole(a.shape) for a in args[1:]],
        out_specs=[whole(o.shape) for o in outs],
        compiler_params=params(14),
        cost_estimate=cost(3 * 10**9, 8 * 2**20),
        name="early",
    )(args[0], *kept(args[1:]))


def build_kernel(where_ref, ids, weight, *refs, capacity, group, weighted):
    sources, out, rank_ref, weight_ref = refs[:-3], refs[-3], refs[-2], refs[-1]
    experts, tokens = rank_ref.shape

    @pl.when(pl.program_id(0) == 0)
    def _():
        name = lax.broadcasted_iota(jnp.int32, (experts, tokens), 0)
        one = jnp.where(name == ids[0:1, :], 1.0, 0.0)
        two = jnp.where(name == ids[1:2, :], 1.0, 0.0)
        both = one + two
        upper = lax.broadcasted_iota(jnp.int32, (tokens, tokens), 0) < lax.broadcasted_iota(
            jnp.int32, (tokens, tokens), 1
        )
        rank = dot(both.astype(BF16), upper.astype(F32).astype(BF16))
        rank_ref[...] = jnp.where(both > 0.0, rank, -1.0)
        weight_ref[...] = one * weight[0:1, :] + two * weight[1:2, :]

    first = pl.program_id(0) * group
    place = lax.broadcasted_iota(jnp.int32, (capacity, tokens), 0).astype(F32)
    picks, weights = [], []
    for e in range(group):
        hit = place == rank_ref[pl.ds(first + e, 1), :]
        picks.append(jnp.where(hit, 1.0, 0.0))
        weights.append(
            jnp.sum(jnp.where(hit, weight_ref[pl.ds(first + e, 1), :], 0.0), axis=1, keepdims=True)
        )
    pick = jnp.concatenate(picks, axis=0).astype(BF16)
    by = jnp.concatenate(weights, axis=0)
    at = 0
    for source, scaled in zip(sources, weighted):
        rows = dot(pick, source[...])
        if scaled:
            rows = rows * by
        out[:, at : at + source.shape[1]] = rows.astype(BF16)
        at += source.shape[1]


def build(position, ids, weight, parts, capacity, experts, group=8):
    tokens = ids.shape[1]
    total = sum(width for _, width, _, _ in parts)
    specs = [pl.BlockSpec(ids.shape, lambda i, where: (0, 0))] * 2
    for _, width, column, _ in parts:
        specs.append(pl.BlockSpec((tokens, width), functools.partial(column_block, column)))
    return pl.pallas_call(
        functools.partial(
            build_kernel, capacity=capacity, group=group, weighted=tuple(p[3] for p in parts)
        ),
        out_shape=made((experts * capacity, total), BF16),
        grid_spec=pltpu.PrefetchScalarGridSpec(
            num_scalar_prefetch=1,
            grid=(experts // group,),
            in_specs=specs,
            out_specs=pl.BlockSpec((group * capacity, total), lambda i, where: (i, 0)),
            scratch_shapes=[pltpu.VMEM((experts, tokens), F32), pltpu.VMEM((experts, tokens), F32)],
        ),
        compiler_params=params(14),
        cost_estimate=cost(1400000 * total, 5000 * total),
    )(position, *kept([ids, weight, *(p[0] for p in parts)]))


def column_block(column, i, where):
    return (0, where[0] if column is None else column)


def weights_kernel(
    where_ref, w_gate, w_up, w_down, own, left, right, far_top, far_bottom,
    out_gate_up, out_down, out_gate, out_up, *, row_part, cot_part,
):
    at = where_ref[0]
    width, units = w_gate.shape
    half = width // 2
    first = ((0,), (0,))
    for weights, out in ((w_gate, out_gate), (w_up, out_up)):
        for step, piece in ((0, own), (3, left), (1, right)):
            out[lax.rem(at + step, 4)] = dot(weights[...], piece[...], first).astype(BF16)
        out[lax.rem(at + 2, 4)] = (
            dot(weights[:half, :], far_top[...], first)
            + dot(weights[half:, :], far_bottom[...], first)
        ).astype(BF16)
    rest = width - 4 * row_part
    out_gate_up[:rest, :units] = w_gate[4 * row_part :, :]
    out_gate_up[:rest, units:] = w_up[4 * row_part :, :]
    cot_rest = width - 4 * cot_part
    out_down[:cot_rest, :] = w_down[:, 4 * cot_part :].T
    for n, step in enumerate(ring_steps):
        group = lax.rem(at + step, 4)
        lines = pl.ds(pl.multiple_of(group * row_part, row_part), row_part)
        columns = pl.ds(pl.multiple_of(group * cot_part, 128), cot_part)
        to = slice(rest + n * row_part, rest + (n + 1) * row_part)
        out_gate_up[to, :units] = w_gate[lines, :]
        out_gate_up[to, units:] = w_up[lines, :]
        to = slice(cot_rest + n * cot_part, cot_rest + (n + 1) * cot_part)
        out_down[to, :] = w_down[:, columns].T


def folded_weights(position, w_gate, w_up, w_down, pieces, row_part, cot_part):
    width, units = w_gate.shape
    args = (position, w_gate, w_up, w_down, *pieces)
    fold = made((4, units, pieces[0].shape[1]), BF16)
    outs = (
        made((width, 2 * units), BF16),
        made((width, units), BF16),
        fold,
        fold,
    )
    return pl.pallas_call(
        functools.partial(weights_kernel, row_part=row_part, cot_part=cot_part),
        out_shape=outs,
        in_specs=[SMEM] + [whole(a.shape) for a in args[1:]],
        out_specs=[whole(o.shape) for o in outs],
        compiler_params=params(24),
        cost_estimate=cost(4 * 10**9, 7 * 2**20),
        name="folded",
    )(position, *kept([w_gate, w_up, w_down]), *pieces)


def expert_kernel(got_rows, got_cot, *refs, row_part):
    pieces = refs[:8]
    gate_up, down, fold_gate, fold_up, out_hidden, out_gate, out_up, out_mix = refs[8:]
    units = down.shape[1]
    upper = pl.program_id(0) < pl.num_programs(0) // 2
    parts = [jnp.where(upper, pieces[2 * n][...], pieces[2 * n + 1][...]) for n in range(4)]
    rows = jnp.concatenate([got_rows[...], *(p[:, :row_part] for p in parts)], axis=1)
    cots = jnp.concatenate([got_cot[...], *(p[:, row_part:] for p in parts)], axis=1)
    both = dot(rows, gate_up[...])
    gate_pre, up_pre = both[:, :units], both[:, units:]
    hidden_cot = dot(cots, down[...])
    sigma = sigmoid(gate_pre)
    swish = gate_pre * sigma
    out_hidden[...] = (swish * up_pre).astype(BF16)
    gate_cot = (hidden_cot * up_pre * sigma * (1.0 + gate_pre * (1.0 - sigma))).astype(BF16)
    up_cot = (hidden_cot * swish).astype(BF16)
    out_gate[...] = gate_cot
    out_up[...] = up_cot
    for c in range(4):
        out_mix[c] = (dot(gate_cot, fold_gate[c]) + dot(up_cot, fold_up[c])).astype(BF16)


def expert(got, pieces, gate_up, down, fold_gate, fold_up, row_part, cot_part, steps=4):
    rows = got.shape[0]
    width, hidden = down.shape
    block = rows // steps
    part = fold_gate.shape[2]
    half = steps // 2
    row_rest, cot_rest = width - 4 * row_part, width - 4 * cot_part
    narrow = made((rows, hidden), BF16)
    mine = pl.BlockSpec((block, hidden), lambda i: (i, 0))
    top = pl.BlockSpec((block, row_part + cot_part), lambda i: (jnp.minimum(i, half - 1), 0))
    bottom = pl.BlockSpec((block, row_part + cot_part), lambda i: (jnp.maximum(i - half, 0), 0))
    return pl.pallas_call(
        functools.partial(expert_kernel, row_part=row_part),
        out_shape=(narrow, narrow, narrow, made((4, rows, part), BF16)),
        grid=(steps,),
        in_specs=[
            pl.BlockSpec((block, row_rest), lambda i: (i, 0)),
            pl.BlockSpec((block, cot_rest), lambda i: (i, row_rest // cot_rest)),
            *([top, bottom] * 4),
            *(whole(a.shape) for a in (gate_up, down, fold_gate, fold_up)),
        ],
        out_specs=[mine, mine, mine, pl.BlockSpec((4, block, part), lambda i: (0, i, 0))],
        compiler_params=params(26),
        cost_estimate=cost(7 * 10**9, 18 * 2**20),
        name="expert",
    )(*kept([got, got]), *pieces, *kept([gate_up, down, fold_gate, fold_up]))


def grads_kernel(where_ref, got_rows, got_cot, *refs, row_part, cot_part):
    pieces = refs[:8]
    hidden, gate_cot, up_cot, out_gate, out_up, out_down = refs[8:]
    at = where_ref[0]
    first = ((0,), (0,))
    rows = got_rows[...]
    out_gate[0, 4 * row_part :, :] = dot(rows, gate_cot[...], first)
    out_up[0, 4 * row_part :, :] = dot(rows, up_cot[...], first)
    out_down[0, :, 4 * cot_part :] = dot(hidden[...], got_cot[...], first)
    for n, step in enumerate(ring_steps):
        group = lax.rem(at + step, 4)
        top, bottom = pieces[2 * n], pieces[2 * n + 1]
        half = top.shape[0]
        lines = pl.ds(pl.multiple_of(group * row_part, row_part), row_part)
        columns = pl.ds(pl.multiple_of(group * cot_part, 128), cot_part)
        for cot, out in ((gate_cot, out_gate), (up_cot, out_up)):
            out[0, lines, :] = dot(top[:, :row_part], cot[:half, :], first) + dot(
                bottom[:, :row_part], cot[half:, :], first
            )
        out_down[0, :, columns] = dot(hidden[:half, :], top[:, row_part:], first) + dot(
            hidden[half:, :], bottom[:, row_part:], first
        )


def grads(position, got, pieces, hidden, gate_cot, up_cot, width, row_part, cot_part):
    rows, units = hidden.shape
    row_rest, cot_rest = width - 4 * row_part, width - 4 * cot_part
    outs = (
        made((1, width, units), F32),
        made((1, width, units), F32),
        made((1, units, width), F32),
    )
    tail = (*pieces, hidden, gate_cot, up_cot)
    return pl.pallas_call(
        functools.partial(grads_kernel, row_part=row_part, cot_part=cot_part),
        out_shape=outs,
        grid=(1,),
        in_specs=[
            SMEM,
            pl.BlockSpec((rows, row_rest), lambda i: (0, 0), pipeline_mode=pl.Buffered(1)),
            pl.BlockSpec(
                (rows, cot_rest), lambda i: (0, row_rest // cot_rest), pipeline_mode=pl.Buffered(1)
            ),
            *(whole(a.shape) for a in tail),
        ],
        out_specs=[whole(o.shape) for o in outs],
        compiler_params=params(30),
        cost_estimate=cost(4 * 10**9, 17 * 2**20),
        name="grads",
    )(position, *kept([got, got]), *pieces, *kept(tail[len(pieces) :]))


def proj_kernel(where_ref, gate_cot, up_cot, w_gate, w_up, local, *refs):
    pieces, out = refs[:-1], refs[-1]
    at = where_ref[0]
    core = where_ref[1]
    first = ((0,), (0,))
    for n, step in enumerate(ring_steps):
        group = lax.rem(at + step, 4)
        top, bottom = pieces[2 * n], pieces[2 * n + 1]
        half = top.shape[0]
        push_gate, push_up = (
            (dot(cot[:half, :], top[...], first) + dot(cot[half:, :], bottom[...], first)).astype(BF16)
            for cot in (gate_cot, up_cot)
        )
        term = dot(w_gate[...], push_gate) + dot(w_up[...], push_up)
        if step == 0:
            term = term + local[...]
        term = term.astype(BF16)
        lines = out.shape[3]
        for s in range(2 * out.shape[2]):
            slot = lax.rem(s % 2 + core, 2)
            out[slot, group, s // 2] = term[s * lines : (s + 1) * lines, :]


def proj(position, gate_cot, up_cot, w_gate, w_up, local, pieces, lines):
    width, part = w_gate.shape[0], pieces[0].shape[1]
    args = (position, gate_cot, up_cot, w_gate, w_up, local, *pieces)
    out = made((2, 4, width // lines // 2, lines, part), BF16)
    return pl.pallas_call(
        proj_kernel,
        out_shape=out,
        in_specs=[SMEM] + [whole(a.shape) for a in args[1:]],
        out_specs=whole(out.shape),
        compiler_params=params(22),
        cost_estimate=cost(4 * 10**9, 14 * 2**20),
        name="proj",
    )(position, *kept(args[1:6]), *pieces)


def scan_kernel(back, sel, base, act, b, decay, seg, block, out_grad, out_local, out_pair, drive, part):
    tokens, channels = base.shape
    length = tokens // 8
    mix = base[...]
    total = back[0].astype(F32) + back[1].astype(F32) + back[2].astype(F32) + back[3].astype(F32)
    mix = mix + dot(sel[...], total.astype(BF16))
    out_grad[...] = (mix * b[...]).astype(BF16)
    push = mix * act[...]
    for h in range(channels // 128):
        cols = slice(h * 128, (h + 1) * 128)
        drive[h] = push[:, cols]
        value = drive[h, pl.ds(length - 1, 8, stride=length), :]
        part[h, pl.ds(length - 1, 8, stride=length), :] = value
        for i in range(length - 2, -1, -1):
            value = (
                drive[h, pl.ds(i, 8, stride=length), :]
                + decay[h, pl.ds(i + 1, 8, stride=length), :] * value
            )
            part[h, pl.ds(i, 8, stride=length), :] = value
        lead = decay[h, pl.ds(0, 8, stride=length), :]
        inner = seg[h, pl.ds(0, 8, stride=length), :]
        carry = jnp.zeros((1, 128), F32)
        for k in range(7, -1, -1):
            rows = slice(k * length, (k + 1) * length)
            out_local[rows, cols] = part[h, rows, :] + seg[h, rows, :] * carry
            one = slice(k, k + 1)
            carry = lead[one, :] * (value[one, :] + inner[one, :] * carry)
        out_pair[:, cols] = jnp.concatenate([carry, block[0:1, cols]], axis=0)


def scanned(back, sel, base, act, b, decay, seg, block):
    tokens, channels = base.shape
    args = (back, sel, base, act, b, decay, seg, block)
    outs = (
        made((tokens, channels), BF16),
        made((tokens, channels), F32),
        made((2, channels), F32),
    )
    return pl.pallas_call(
        scan_kernel,
        out_shape=outs,
        in_specs=[whole(a.shape) for a in args],
        out_specs=[whole(o.shape) for o in outs],
        scratch_shapes=[pltpu.VMEM(decay.shape, F32), pltpu.VMEM(decay.shape, F32)],
        compiler_params=params(14),
        cost_estimate=cost(4 * 10**8, 8 * 2**20),
        name="scanned",
    )(back, *kept(args[1:]))


def final_kernel(where_ref, carry, local, exp, ca, ci, cs, map_a, map_i, out):
    channels = local.shape[1]
    heads = channels // 128
    first = where_ref[0] * heads
    for h in range(heads):
        cols = slice(h * 128, (h + 1) * 128)
        cot = local[:, cols] + exp[:, cols] * carry[0:1, cols]
        a_cot = (cot * ca[:, cols]).astype(BF16)
        i_cot = (cot * ci[:, cols]).astype(BF16)
        total = (
            cot * cs[:, cols]
            + dot(a_cot, map_a[first + h], ((1,), (1,)))
            + dot(i_cot, map_i[first + h], ((1,), (1,)))
        )
        out[:, cols] = total.astype(BF16)


def final(position, carry, local, exp, ca, ci, cs, map_a, map_i):
    args = (position, carry, local, exp, ca, ci, cs, map_a, map_i)
    return pl.pallas_call(
        final_kernel,
        out_shape=made(local.shape, BF16),
        in_specs=[SMEM] + [whole(a.shape) for a in args[1:]],
        out_specs=whole(local.shape),
        compiler_params=params(8),
        cost_estimate=cost(10**8, 4 * 2**20),
        name="final",
    )(position, carry, *kept(args[2:]))


def shifted(piece, by):
    return lax.ppermute(piece, "tp", [(i, (i + by) % 4) for i in range(4)])


def ring_gather(top, bottom):
    left_top, right_bottom = shifted(top, 1), shifted(bottom, -1)
    left_bottom, right_top = shifted(bottom, 1), shifted(top, -1)
    far_top, far_bottom = shifted(left_top, 1), shifted(right_bottom, -1)
    return top, bottom, left_top, left_bottom, right_top, right_bottom, far_top, far_bottom


def whole_ring_gather(own):
    half = own.shape[0] // 2
    left, right = shifted(own, 1), shifted(own, -1)
    far_top, far_bottom = shifted(left[:half], 1), shifted(right[half:], -1)
    return own, left, right, far_top, far_bottom


def later(pair, by, length):
    return lax.ppermute(pair, ("sq", "core"), [(i, i - by) for i in range(by, length)])


def joined(near, far):
    return jnp.stack([near[0] + near[1] * far[0], near[1] * far[1]])


def carried(pair, length):
    one, two, three, four = (later(pair, by, length) for by in (1, 2, 3, 4))
    pair = joined(joined(one, two), joined(three, four))
    one, two, three = (later(pair, by, length) for by in (4, 8, 12))
    pair = joined(joined(pair, one), joined(two, three))
    return joined(pair, later(pair, 16, length))


def per_device(
    layer_input, out_cot, expert_ids, route_weight, w_gate, w_up, w_down, out_proj,
    rec_input, gate_input, prev_state, decay_param, extra_decay, gate_a_w, gate_i_w,
):
    sources = lax.axis_size("sq") * lax.axis_size("core")
    tp = lax.axis_index("tp")
    core = lax.axis_index("core")
    sp_axes = ("sq", "core")
    position = jnp.stack([tp, core]).astype(jnp.int32)
    w_gate, w_up, w_down = w_gate[0], w_up[0], w_down[0]
    tokens, width = layer_input.shape
    capacity = 5 * tokens * expert_ids.shape[1] // (4 * sources)
    slots = sources * capacity
    row_part, cot_part = width // 8, 3 * width // 16
    row_rest, cot_rest = width - 4 * row_part, width - 4 * cot_part
    ids, weight = expert_ids.T, route_weight.T

    def exchanged(rows):
        return lax.all_to_all(
            rows.reshape(sources, capacity, -1), sp_axes, 0, 0, tiled=True
        ).reshape(rows.shape)

    spread = build(
        position, ids, weight,
        [(layer_input, row_part, None, False), (out_cot, cot_part, None, True)],
        capacity, sources,
    )
    spread = exchanged(spread)
    projections = whole_ring_gather(out_proj)
    gate_up, down, fold_gate, fold_up = folded_weights(
        position, w_gate, w_up, w_down, projections, row_part, cot_part
    )
    rates = (decay_factor * jax.nn.softplus(-decay_param)).reshape(-1, gate_a_w.shape[1])
    rec_output, act, b, ca, ci, cs, decay, seg, exp, block, sel = early(
        position, expert_ids, rec_input, gate_input, prev_state, rates, extra_decay.T,
        gate_a_w, gate_i_w, capacity, sources,
    )
    direct = build(
        position, ids, weight,
        [
            (layer_input, row_rest, 4 * row_part // row_rest, False),
            (out_cot, cot_rest, 4 * cot_part // cot_rest, True),
            (rec_output, rec_output.shape[1], 0, False),
        ],
        capacity, sources,
    )
    got = exchanged(direct)
    pieces = ring_gather(spread[: slots // 2], spread[slots // 2 :])
    base = jnp.dot(out_cot, out_proj, preferred_element_type=F32)
    local_proj = lax.dot_general(
        out_cot, rec_output, (((0,), (0,)), ((), ())), preferred_element_type=F32
    )
    hidden, gate_cot, up_cot, mix = expert(
        got, pieces, gate_up, down, fold_gate, fold_up, row_part, cot_part
    )
    back = lax.all_to_all(
        mix.reshape(4 * sources, capacity, -1), ("tp", *sp_axes), 0, 0, tiled=True
    ).reshape(mix.shape)
    grad_gate, grad_up, grad_down = grads(
        position, got, pieces, hidden, gate_cot, up_cot, width, row_part, cot_part
    )
    start = row_rest + cot_rest
    recs = ring_gather(got[: slots // 2, start:], got[slots // 2 :, start:])
    lines = width // sources
    parts = proj(position, gate_cot, up_cot, w_gate, w_up, local_proj, recs, lines)
    other = lax.ppermute(parts[1], "core", [(0, 1), (1, 0)])
    chip = (parts[0].astype(F32) + other.astype(F32)).astype(BF16)
    arrived = lax.all_to_all(
        chip.reshape(4 * chip.shape[1], lines, -1), ("tp", "sq"), 0, 0, tiled=True
    )
    grad_out_proj = arrived.astype(F32).sum(axis=0)
    gate_input_grad, local, pair = scanned(back, sel, base, act, b, decay, seg, block)
    carry = carried(pair, sources)
    rec_input_grad = final(position, carry, local, exp, ca, ci, cs, gate_a_w, gate_i_w)
    return (grad_gate, grad_up, grad_down, grad_out_proj, rec_input_grad, gate_input_grad)


def solution(mesh):
    sp, tp = mesh.devices.shape
    inner = Mesh(mesh.devices.reshape(sp // 2, 2, tp), ("sq", "core", "tp"))
    sp = ("sq", "core")
    in_specs = (
        P(sp, None),
        P(sp, None),
        P(sp, None),
        P(sp, None),
        P(sp, None, "tp"),
        P(sp, None, "tp"),
        P(sp, "tp", None),
        P(None, "tp"),
        P(sp, "tp"),
        P(sp, "tp"),
        P(sp, "tp"),
        P(),
        P("tp", sp),
        P(),
        P(),
    )
    out_specs = (
        P(sp, None, "tp"),
        P(sp, None, "tp"),
        P(sp, "tp", None),
        P(sp, "tp"),
        P(sp, "tp"),
        P(sp, "tp"),
    )
    return jax.shard_map(
        per_device, mesh=inner, in_specs=in_specs, out_specs=out_specs, check_vma=False
    )
```

```python
import functools
import jax
import jax.numpy as jnp
from jax import lax
from jax.experimental import pallas as pl
from jax.experimental.pallas import tpu as pltpu
from jax.sharding import Mesh, PartitionSpec as P


F32 = jnp.float32
BF16 = jnp.bfloat16
gelu_scale = 0.7978845608028654
gelu_cubic = 0.044715
decay_factor = 8.0
ring_steps = (0, 3, 1, 2)


def params(limit_mib=48, **extra):
    return pltpu.CompilerParams(vmem_limit_bytes=limit_mib * 1024 * 1024, **extra)


def cost(flops, moved):
    return pl.CostEstimate(flops=flops, bytes_accessed=moved, transcendentals=0)


def whole(shape):
    return pl.BlockSpec(shape, lambda *_: (0,) * len(shape), pipeline_mode=pl.Buffered(1))


SMEM = pl.BlockSpec(memory_space=pltpu.SMEM)


def made(shape, dtype):
    return pltpu.HBM(shape, dtype)


def kept(arrays):
    return [pltpu.with_memory_space_constraint(a, pltpu.HBM) for a in arrays]


def dot(a, b, dims=((1,), (0,))):
    return lax.dot_general(a, b, (dims, ((), ())), preferred_element_type=F32)


def sigmoid(v):
    return 1.0 / (1.0 + jnp.exp(-v))


def minus_expm1(v):
    series = 1.0 + v / 8.0
    for order in range(7, 1, -1):
        series = 1.0 + v / order * series
    return jnp.where(v > -0.5, -v * series, 1.0 - jnp.exp(v))


def early_kernel(
    where_ref, ids, rec, gate_in, prev, rates, extra, map_a, map_i,
    out_rec, out_act, out_b, out_ca, out_ci, out_cs, out_decay, out_seg, out_exp, out_block, out_sel,
    *, capacity, experts,
):
    tokens, channels = rec.shape
    heads = channels // 128
    first = where_ref[0] * heads
    for h in range(heads):
        cols = slice(h * 128, (h + 1) * 128)
        values_bf = rec[:, cols]
        x = values_bf.astype(F32)
        ra = sigmoid(dot(values_bf, map_a[first + h]))
        ig = sigmoid(dot(values_bf, map_i[first + h]))
        rate = rates[pl.ds(first + h, 1), :]
        log_decay = -rate * ra + extra[:, h : h + 1]
        decay = jnp.exp(log_decay)
        scale = jnp.sqrt(minus_expm1(2.0 * log_decay))
        before = prev[:, cols]
        state = decay * before + scale * ig * x
        g = gate_in[:, cols].astype(F32)
        bend = jnp.tanh(gelu_scale * (g + gelu_cubic * g * g * g))
        act = 0.5 * g * (1.0 + bend)
        slope = 0.5 * (1.0 + bend) + 0.5 * g * (1.0 - bend * bend) * gelu_scale * (
            1.0 + 3.0 * gelu_cubic * g * g
        )
        out_rec[:, cols] = (state * act).astype(BF16)
        out_act[:, cols] = act
        out_b[:, cols] = state * slope
        out_ca[:, cols] = (decay * before - decay * decay / scale * ig * x) * -rate * ra * (1.0 - ra)
        out_ci[:, cols] = scale * x * ig * (1.0 - ig)
        out_cs[:, cols] = scale * ig
        out_decay[h] = decay
    length = tokens // 8
    for h in range(heads):
        cols = slice(h * 128, (h + 1) * 128)
        product = jnp.ones((8, 128), F32)
        for i in range(length - 1, -1, -1):
            out_seg[h, pl.ds(i, 8, stride=length), :] = product
            product = product * out_decay[h, pl.ds(i, 8, stride=length), :]
        carry = jnp.ones((1, 128), F32)
        for k in range(7, -1, -1):
            rows = slice(k * length, (k + 1) * length)
            out_exp[rows, cols] = out_seg[h, rows, :] * carry
            carry = carry * product[k : k + 1, :]
        out_block[:, cols] = jnp.broadcast_to(carry, (8, 128))
    lane = lax.broadcasted_iota(jnp.int32, (tokens, 128), 1)
    first_id = ids[:, 0:1]
    second_id = ids[:, 1:2]
    one = (lane == first_id).astype(F32)
    two = (lane == second_id).astype(F32)
    lower = lax.broadcasted_iota(jnp.int32, (tokens, tokens), 0) > lax.broadcasted_iota(
        jnp.int32, (tokens, tokens), 1
    )
    rank = dot(lower.astype(F32).astype(BF16), (one + two).astype(BF16))
    place_one = first_id * capacity + jnp.sum(rank * one, axis=1, keepdims=True).astype(jnp.int32)
    place_two = second_id * capacity + jnp.sum(rank * two, axis=1, keepdims=True).astype(jnp.int32)
    slots = experts * capacity
    for at in range(0, slots, 256):
        slot = lax.broadcasted_iota(jnp.int32, (tokens, 256), 1) + at
        hit = (slot == place_one) | (slot == place_two)
        out_sel[:, at : at + 256] = jnp.where(hit, 1.0, 0.0).astype(BF16)


def early(position, ids, rec, gate_in, prev, rates, extra, map_a, map_i, capacity, experts):
    tokens, channels = rec.shape
    wide = made((tokens, channels), F32)
    heads = made((channels // 128, tokens, 128), F32)
    outs = (
        made((tokens, channels), BF16),
        wide, wide, wide, wide, wide, heads, heads, wide,
        made((8, channels), F32),
        made((tokens, experts * capacity), BF16),
    )
    args = (position, ids, rec, gate_in, prev, rates, extra, map_a, map_i)
    return pl.pallas_call(
        functools.partial(early_kernel, capacity=capacity, experts=experts),
        out_shape=outs,
        in_specs=[SMEM] + [whole(a.shape) for a in args[1:]],
        out_specs=[whole(o.shape) for o in outs],
        compiler_params=params(14),
        cost_estimate=cost(3 * 10**9, 8 * 2**20),
        name="early",
    )(args[0], *kept(args[1:]))


def build_kernel(where_ref, ids, weight, *refs, capacity, group, weighted):
    sources, out, rank_ref, weight_ref = refs[:-3], refs[-3], refs[-2], refs[-1]
    experts, tokens = rank_ref.shape

    @pl.when(pl.program_id(0) == 0)
    def _():
        name = lax.broadcasted_iota(jnp.int32, (experts, tokens), 0)
        one = jnp.where(name == ids[0:1, :], 1.0, 0.0)
        two = jnp.where(name == ids[1:2, :], 1.0, 0.0)
        both = one + two
        upper = lax.broadcasted_iota(jnp.int32, (tokens, tokens), 0) < lax.broadcasted_iota(
            jnp.int32, (tokens, tokens), 1
        )
        rank = dot(both.astype(BF16), upper.astype(F32).astype(BF16))
        rank_ref[...] = jnp.where(both > 0.0, rank, -1.0)
        weight_ref[...] = one * weight[0:1, :] + two * weight[1:2, :]

    first = pl.program_id(0) * group
    place = lax.broadcasted_iota(jnp.int32, (capacity, tokens), 0).astype(F32)
    picks, weights = [], []
    for e in range(group):
        hit = place == rank_ref[pl.ds(first + e, 1), :]
        picks.append(jnp.where(hit, 1.0, 0.0))
        weights.append(
            jnp.sum(jnp.where(hit, weight_ref[pl.ds(first + e, 1), :], 0.0), axis=1, keepdims=True)
        )
    pick = jnp.concatenate(picks, axis=0).astype(BF16)
    by = jnp.concatenate(weights, axis=0)
    at = 0
    for source, scaled in zip(sources, weighted):
        rows = dot(pick, source[...])
        if scaled:
            rows = rows * by
        out[:, at : at + source.shape[1]] = rows.astype(BF16)
        at += source.shape[1]


def build(position, ids, weight, parts, capacity, experts, group=8):
    tokens = ids.shape[1]
    total = sum(width for _, width, _, _ in parts)
    specs = [pl.BlockSpec(ids.shape, lambda i, where: (0, 0))] * 2
    for _, width, column, _ in parts:
        specs.append(pl.BlockSpec((tokens, width), functools.partial(column_block, column)))
    return pl.pallas_call(
        functools.partial(
            build_kernel, capacity=capacity, group=group, weighted=tuple(p[3] for p in parts)
        ),
        out_shape=made((experts * capacity, total), BF16),
        grid_spec=pltpu.PrefetchScalarGridSpec(
            num_scalar_prefetch=1,
            grid=(experts // group,),
            in_specs=specs,
            out_specs=pl.BlockSpec((group * capacity, total), lambda i, where: (i, 0)),
            scratch_shapes=[pltpu.VMEM((experts, tokens), F32), pltpu.VMEM((experts, tokens), F32)],
        ),
        compiler_params=params(14),
        cost_estimate=cost(1400000 * total, 5000 * total),
    )(position, *kept([ids, weight, *(p[0] for p in parts)]))


def column_block(column, i, where):
    return (0, where[0] if column is None else column)


def weights_kernel(
    where_ref, w_gate, w_up, w_down, own, left, right, far_top, far_bottom,
    out_gate_up, out_down, out_gate, out_up, *, row_part, cot_part,
):
    at = where_ref[0]
    width, units = w_gate.shape
    half = width // 2
    first = ((0,), (0,))
    for weights, out in ((w_gate, out_gate), (w_up, out_up)):
        for step, piece in ((0, own), (3, left), (1, right)):
            out[lax.rem(at + step, 4)] = dot(weights[...], piece[...], first).astype(BF16)
        out[lax.rem(at + 2, 4)] = (
            dot(weights[:half, :], far_top[...], first)
            + dot(weights[half:, :], far_bottom[...], first)
        ).astype(BF16)
    rest = width - 4 * row_part
    out_gate_up[:rest, :units] = w_gate[4 * row_part :, :]
    out_gate_up[:rest, units:] = w_up[4 * row_part :, :]
    cot_rest = width - 4 * cot_part
    out_down[:cot_rest, :] = w_down[:, 4 * cot_part :].T
    for n, step in enumerate(ring_steps):
        group = lax.rem(at + step, 4)
        lines = pl.ds(pl.multiple_of(group * row_part, row_part), row_part)
        columns = pl.ds(pl.multiple_of(group * cot_part, 128), cot_part)
        to = slice(rest + n * row_part, rest + (n + 1) * row_part)
        out_gate_up[to, :units] = w_gate[lines, :]
        out_gate_up[to, units:] = w_up[lines, :]
        to = slice(cot_rest + n * cot_part, cot_rest + (n + 1) * cot_part)
        out_down[to, :] = w_down[:, columns].T


def folded_weights(position, w_gate, w_up, w_down, pieces, row_part, cot_part):
    width, units = w_gate.shape
    args = (position, w_gate, w_up, w_down, *pieces)
    fold = made((4, units, pieces[0].shape[1]), BF16)
    outs = (
        made((width, 2 * units), BF16),
        made((width, units), BF16),
        fold,
        fold,
    )
    return pl.pallas_call(
        functools.partial(weights_kernel, row_part=row_part, cot_part=cot_part),
        out_shape=outs,
        in_specs=[SMEM] + [whole(a.shape) for a in args[1:]],
        out_specs=[whole(o.shape) for o in outs],
        compiler_params=params(24),
        cost_estimate=cost(4 * 10**9, 7 * 2**20),
        name="folded",
    )(position, *kept([w_gate, w_up, w_down]), *pieces)


def expert_kernel(got_rows, got_cot, *refs, row_part):
    pieces = refs[:8]
    gate_up, down, fold_gate, fold_up, out_hidden, out_gate, out_up, out_mix = refs[8:]
    units = down.shape[1]
    upper = pl.program_id(0) < pl.num_programs(0) // 2
    parts = [jnp.where(upper, pieces[2 * n][...], pieces[2 * n + 1][...]) for n in range(4)]
    rows = jnp.concatenate([got_rows[...], *(p[:, :row_part] for p in parts)], axis=1)
    cots = jnp.concatenate([got_cot[...], *(p[:, row_part:] for p in parts)], axis=1)
    both = dot(rows, gate_up[...])
    gate_pre, up_pre = both[:, :units], both[:, units:]
    hidden_cot = dot(cots, down[...])
    sigma = sigmoid(gate_pre)
    swish = gate_pre * sigma
    out_hidden[...] = (swish * up_pre).astype(BF16)
    gate_cot = (hidden_cot * up_pre * sigma * (1.0 + gate_pre * (1.0 - sigma))).astype(BF16)
    up_cot = (hidden_cot * swish).astype(BF16)
    out_gate[...] = gate_cot
    out_up[...] = up_cot
    for c in range(4):
        out_mix[c] = (dot(gate_cot, fold_gate[c]) + dot(up_cot, fold_up[c])).astype(BF16)


def expert(got, pieces, gate_up, down, fold_gate, fold_up, row_part, cot_part, steps=4):
    rows = got.shape[0]
    width, hidden = down.shape
    block = rows // steps
    part = fold_gate.shape[2]
    half = steps // 2
    row_rest, cot_rest = width - 4 * row_part, width - 4 * cot_part
    narrow = made((rows, hidden), BF16)
    mine = pl.BlockSpec((block, hidden), lambda i: (i, 0))
    top = pl.BlockSpec((block, row_part + cot_part), lambda i: (jnp.minimum(i, half - 1), 0))
    bottom = pl.BlockSpec((block, row_part + cot_part), lambda i: (jnp.maximum(i - half, 0), 0))
    return pl.pallas_call(
        functools.partial(expert_kernel, row_part=row_part),
        out_shape=(narrow, narrow, narrow, made((4, rows, part), BF16)),
        grid=(steps,),
        in_specs=[
            pl.BlockSpec((block, row_rest), lambda i: (i, 0)),
            pl.BlockSpec((block, cot_rest), lambda i: (i, row_rest // cot_rest)),
            *([top, bottom] * 4),
            *(whole(a.shape) for a in (gate_up, down, fold_gate, fold_up)),
        ],
        out_specs=[mine, mine, mine, pl.BlockSpec((4, block, part), lambda i: (0, i, 0))],
        compiler_params=params(26),
        cost_estimate=cost(7 * 10**9, 18 * 2**20),
        name="expert",
    )(*kept([got, got]), *pieces, *kept([gate_up, down, fold_gate, fold_up]))


def grads_kernel(where_ref, got_rows, got_cot, *refs, row_part, cot_part):
    pieces = refs[:8]
    hidden, gate_cot, up_cot, out_gate, out_up, out_down = refs[8:]
    at = where_ref[0]
    first = ((0,), (0,))
    rows = got_rows[...]
    out_gate[0, 4 * row_part :, :] = dot(rows, gate_cot[...], first)
    out_up[0, 4 * row_part :, :] = dot(rows, up_cot[...], first)
    out_down[0, :, 4 * cot_part :] = dot(hidden[...], got_cot[...], first)
    for n, step in enumerate(ring_steps):
        group = lax.rem(at + step, 4)
        top, bottom = pieces[2 * n], pieces[2 * n + 1]
        half = top.shape[0]
        lines = pl.ds(pl.multiple_of(group * row_part, row_part), row_part)
        columns = pl.ds(pl.multiple_of(group * cot_part, 128), cot_part)
        for cot, out in ((gate_cot, out_gate), (up_cot, out_up)):
            out[0, lines, :] = dot(top[:, :row_part], cot[:half, :], first) + dot(
                bottom[:, :row_part], cot[half:, :], first
            )
        out_down[0, :, columns] = dot(hidden[:half, :], top[:, row_part:], first) + dot(
            hidden[half:, :], bottom[:, row_part:], first
        )


def grads(position, got, pieces, hidden, gate_cot, up_cot, width, row_part, cot_part):
    rows, units = hidden.shape
    row_rest, cot_rest = width - 4 * row_part, width - 4 * cot_part
    outs = (
        made((1, width, units), F32),
        made((1, width, units), F32),
        made((1, units, width), F32),
    )
    tail = (*pieces, hidden, gate_cot, up_cot)
    return pl.pallas_call(
        functools.partial(grads_kernel, row_part=row_part, cot_part=cot_part),
        out_shape=outs,
        grid=(1,),
        in_specs=[
            SMEM,
            pl.BlockSpec((rows, row_rest), lambda i: (0, 0), pipeline_mode=pl.Buffered(1)),
            pl.BlockSpec(
                (rows, cot_rest), lambda i: (0, row_rest // cot_rest), pipeline_mode=pl.Buffered(1)
            ),
            *(whole(a.shape) for a in tail),
        ],
        out_specs=[whole(o.shape) for o in outs],
        compiler_params=params(30),
        cost_estimate=cost(4 * 10**9, 17 * 2**20),
        name="grads",
    )(position, *kept([got, got]), *pieces, *kept(tail[len(pieces) :]))


def proj_kernel(where_ref, gate_cot, up_cot, w_gate, w_up, local, *refs):
    pieces, out = refs[:-1], refs[-1]
    at = where_ref[0]
    core = where_ref[1]
    first = ((0,), (0,))
    for n, step in enumerate(ring_steps):
        group = lax.rem(at + step, 4)
        top, bottom = pieces[2 * n], pieces[2 * n + 1]
        half = top.shape[0]
        push_gate, push_up = (
            (dot(cot[:half, :], top[...], first) + dot(cot[half:, :], bottom[...], first)).astype(BF16)
            for cot in (gate_cot, up_cot)
        )
        term = dot(w_gate[...], push_gate) + dot(w_up[...], push_up)
        if step == 0:
            term = term + local[...]
        term = term.astype(BF16)
        lines = out.shape[3]
        for s in range(2 * out.shape[2]):
            slot = lax.rem(s % 2 + core, 2)
            out[slot, group, s // 2] = term[s * lines : (s + 1) * lines, :]


def proj(position, gate_cot, up_cot, w_gate, w_up, local, pieces, lines):
    width, part = w_gate.shape[0], pieces[0].shape[1]
    args = (position, gate_cot, up_cot, w_gate, w_up, local, *pieces)
    out = made((2, 4, width // lines // 2, lines, part), BF16)
    return pl.pallas_call(
        proj_kernel,
        out_shape=out,
        in_specs=[SMEM] + [whole(a.shape) for a in args[1:]],
        out_specs=whole(out.shape),
        compiler_params=params(22),
        cost_estimate=cost(4 * 10**9, 14 * 2**20),
        name="proj",
    )(position, *kept(args[1:6]), *pieces)


def scan_kernel(back, sel, base, act, b, decay, seg, block, out_grad, out_local, out_pair, drive, part):
    tokens, channels = base.shape
    length = tokens // 8
    mix = base[...]
    total = back[0].astype(F32) + back[1].astype(F32) + back[2].astype(F32) + back[3].astype(F32)
    mix = mix + dot(sel[...], total.astype(BF16))
    out_grad[...] = (mix * b[...]).astype(BF16)
    push = mix * act[...]
    for h in range(channels // 128):
        cols = slice(h * 128, (h + 1) * 128)
        drive[h] = push[:, cols]
        value = drive[h, pl.ds(length - 1, 8, stride=length), :]
        part[h, pl.ds(length - 1, 8, stride=length), :] = value
        for i in range(length - 2, -1, -1):
            value = (
                drive[h, pl.ds(i, 8, stride=length), :]
                + decay[h, pl.ds(i + 1, 8, stride=length), :] * value
            )
            part[h, pl.ds(i, 8, stride=length), :] = value
        lead = decay[h, pl.ds(0, 8, stride=length), :]
        inner = seg[h, pl.ds(0, 8, stride=length), :]
        carry = jnp.zeros((1, 128), F32)
        for k in range(7, -1, -1):
            rows = slice(k * length, (k + 1) * length)
            out_local[rows, cols] = part[h, rows, :] + seg[h, rows, :] * carry
            one = slice(k, k + 1)
            carry = lead[one, :] * (value[one, :] + inner[one, :] * carry)
        out_pair[:, cols] = jnp.concatenate([carry, block[0:1, cols]], axis=0)


def scanned(back, sel, base, act, b, decay, seg, block):
    tokens, channels = base.shape
    args = (back, sel, base, act, b, decay, seg, block)
    outs = (
        made((tokens, channels), BF16),
        made((tokens, channels), F32),
        made((2, channels), F32),
    )
    return pl.pallas_call(
        scan_kernel,
        out_shape=outs,
        in_specs=[whole(a.shape) for a in args],
        out_specs=[whole(o.shape) for o in outs],
        scratch_shapes=[pltpu.VMEM(decay.shape, F32), pltpu.VMEM(decay.shape, F32)],
        compiler_params=params(14),
        cost_estimate=cost(4 * 10**8, 8 * 2**20),
        name="scanned",
    )(back, *kept(args[1:]))


def final_kernel(where_ref, *refs):
    carry = refs[:-8]
    local, exp, ca, ci, cs, map_a, map_i, out = refs[-8:]
    channels = local.shape[1]
    heads = channels // 128
    first = where_ref[0] * heads
    total = jnp.zeros((1, channels), F32)
    for pair in reversed(carry):
        total = pair[0:1, :] + pair[1:2, :] * total
    for h in range(heads):
        cols = slice(h * 128, (h + 1) * 128)
        cot = local[:, cols] + exp[:, cols] * total[:, cols]
        a_cot = (cot * ca[:, cols]).astype(BF16)
        i_cot = (cot * ci[:, cols]).astype(BF16)
        result = (
            cot * cs[:, cols]
            + dot(a_cot, map_a[first + h], ((1,), (1,)))
            + dot(i_cot, map_i[first + h], ((1,), (1,)))
        )
        out[:, cols] = result.astype(BF16)


def final(position, carry, local, exp, ca, ci, cs, map_a, map_i):
    args = (position, *carry, local, exp, ca, ci, cs, map_a, map_i)
    return pl.pallas_call(
        final_kernel,
        out_shape=made(local.shape, BF16),
        in_specs=[SMEM] + [whole(a.shape) for a in args[1:]],
        out_specs=whole(local.shape),
        compiler_params=params(8),
        cost_estimate=cost(10**8, 4 * 2**20),
        name="final",
    )(position, *carry, *kept(args[1 + len(carry) :]))


def shifted(piece, by):
    return lax.ppermute(piece, "tp", [(i, (i + by) % 4) for i in range(4)])


def ring_gather(top, bottom):
    left_top, right_bottom = shifted(top, 1), shifted(bottom, -1)
    left_bottom, right_top = shifted(bottom, 1), shifted(top, -1)
    far_top, far_bottom = shifted(left_top, 1), shifted(right_bottom, -1)
    return top, bottom, left_top, left_bottom, right_top, right_bottom, far_top, far_bottom


def whole_ring_gather(own):
    half = own.shape[0] // 2
    left, right = shifted(own, 1), shifted(own, -1)
    far_top, far_bottom = shifted(left[:half], 1), shifted(right[half:], -1)
    return own, left, right, far_top, far_bottom


def later(pair, by, length):
    return lax.ppermute(pair, ("sq", "core"), [(i, i - by) for i in range(by, length)])


def joined(near, far):
    return jnp.stack([near[0] + near[1] * far[0], near[1] * far[1]])


def carried(pair, length):
    one, two, three, four = (later(pair, by, length) for by in (1, 2, 3, 4))
    near = joined(joined(one, two), joined(three, four))
    return [near, *(later(near, by, length) for by in range(4, length, 4))]


def per_device(
    layer_input, out_cot, expert_ids, route_weight, w_gate, w_up, w_down, out_proj,
    rec_input, gate_input, prev_state, decay_param, extra_decay, gate_a_w, gate_i_w,
):
    sources = lax.axis_size("sq") * lax.axis_size("core")
    tp = lax.axis_index("tp")
    core = lax.axis_index("core")
    sp_axes = ("sq", "core")
    position = jnp.stack([tp, core]).astype(jnp.int32)
    w_gate, w_up, w_down = w_gate[0], w_up[0], w_down[0]
    tokens, width = layer_input.shape
    capacity = 5 * tokens * expert_ids.shape[1] // (4 * sources)
    slots = sources * capacity
    row_part, cot_part = width // 8, 3 * width // 16
    row_rest, cot_rest = width - 4 * row_part, width - 4 * cot_part
    ids, weight = expert_ids.T, route_weight.T

    def exchanged(rows):
        return lax.all_to_all(
            rows.reshape(sources, capacity, -1), sp_axes, 0, 0, tiled=True
        ).reshape(rows.shape)

    spread = build(
        position, ids, weight,
        [(layer_input, row_part, None, False), (out_cot, cot_part, None, True)],
        capacity, sources,
    )
    spread = exchanged(spread)
    projections = whole_ring_gather(out_proj)
    gate_up, down, fold_gate, fold_up = folded_weights(
        position, w_gate, w_up, w_down, projections, row_part, cot_part
    )
    rates = (decay_factor * jax.nn.softplus(-decay_param)).reshape(-1, gate_a_w.shape[1])
    rec_output, act, b, ca, ci, cs, decay, seg, exp, block, sel = early(
        position, expert_ids, rec_input, gate_input, prev_state, rates, extra_decay.T,
        gate_a_w, gate_i_w, capacity, sources,
    )
    direct = build(
        position, ids, weight,
        [
            (layer_input, row_rest, 4 * row_part // row_rest, False),
            (out_cot, cot_rest, 4 * cot_part // cot_rest, True),
            (rec_output, rec_output.shape[1], 0, False),
        ],
        capacity, sources,
    )
    got = exchanged(direct)
    pieces = ring_gather(spread[: slots // 2], spread[slots // 2 :])
    base = jnp.dot(out_cot, out_proj, preferred_element_type=F32)
    local_proj = lax.dot_general(
        out_cot, rec_output, (((0,), (0,)), ((), ())), preferred_element_type=F32
    )
    hidden, gate_cot, up_cot, mix = expert(
        got, pieces, gate_up, down, fold_gate, fold_up, row_part, cot_part
    )
    back = lax.all_to_all(
        mix.reshape(4 * sources, capacity, -1), ("tp", *sp_axes), 0, 0, tiled=True
    ).reshape(mix.shape)
    grad_gate, grad_up, grad_down = grads(
        position, got, pieces, hidden, gate_cot, up_cot, width, row_part, cot_part
    )
    start = row_rest + cot_rest
    recs = ring_gather(got[: slots // 2, start:], got[slots // 2 :, start:])
    lines = width // sources
    parts = proj(position, gate_cot, up_cot, w_gate, w_up, local_proj, recs, lines)
    other = lax.ppermute(parts[1], "core", [(0, 1), (1, 0)])
    chip = (parts[0].astype(F32) + other.astype(F32)).astype(BF16)
    arrived = lax.all_to_all(
        chip.reshape(4 * chip.shape[1], lines, -1), ("tp", "sq"), 0, 0, tiled=True
    )
    grad_out_proj = arrived.astype(F32).sum(axis=0)
    gate_input_grad, local, pair = scanned(back, sel, base, act, b, decay, seg, block)
    carry = carried(pair, sources)
    rec_input_grad = final(position, carry, local, exp, ca, ci, cs, gate_a_w, gate_i_w)
    return (grad_gate, grad_up, grad_down, grad_out_proj, rec_input_grad, gate_input_grad)


def solution(mesh):
    sp, tp = mesh.devices.shape
    inner = Mesh(mesh.devices.reshape(sp // 2, 2, tp), ("sq", "core", "tp"))
    sp = ("sq", "core")
    in_specs = (
        P(sp, None),
        P(sp, None),
        P(sp, None),
        P(sp, None),
        P(sp, None, "tp"),
        P(sp, None, "tp"),
        P(sp, "tp", None),
        P(None, "tp"),
        P(sp, "tp"),
        P(sp, "tp"),
        P(sp, "tp"),
        P(),
        P("tp", sp),
        P(),
        P(),
    )
    out_specs = (
        P(sp, None, "tp"),
        P(sp, None, "tp"),
        P(sp, "tp", None),
        P(sp, "tp"),
        P(sp, "tp"),
        P(sp, "tp"),
    )
    return jax.shard_map(
        per_device, mesh=inner, in_specs=in_specs, out_specs=out_specs, check_vma=False
    )
```

```python
import functools
import jax
import jax.numpy as jnp
from jax import lax
from jax.experimental import pallas as pl
from jax.experimental.pallas import tpu as pltpu
from jax.sharding import Mesh, PartitionSpec as P


F32 = jnp.float32
BF16 = jnp.bfloat16
gelu_scale = 0.7978845608028654
gelu_cubic = 0.044715
decay_factor = 8.0
ring_steps = (0, 3, 1, 2)


def params(limit_mib=48, **extra):
    return pltpu.CompilerParams(vmem_limit_bytes=limit_mib * 1024 * 1024, **extra)


def cost(flops, moved):
    return pl.CostEstimate(flops=flops, bytes_accessed=moved, transcendentals=0)


def whole(shape):
    return pl.BlockSpec(shape, lambda *_: (0,) * len(shape), pipeline_mode=pl.Buffered(1))


SMEM = pl.BlockSpec(memory_space=pltpu.SMEM)


def made(shape, dtype):
    return pltpu.HBM(shape, dtype)


def kept(arrays):
    return [pltpu.with_memory_space_constraint(a, pltpu.HBM) for a in arrays]


def dot(a, b, dims=((1,), (0,))):
    return lax.dot_general(a, b, (dims, ((), ())), preferred_element_type=F32)


def sigmoid(v):
    return 1.0 / (1.0 + jnp.exp(-v))


def minus_expm1(v):
    series = 1.0 + v / 8.0
    for order in range(7, 1, -1):
        series = 1.0 + v / order * series
    return jnp.where(v > -0.5, -v * series, 1.0 - jnp.exp(v))


def early_kernel(
    where_ref, ids, rec, gate_in, prev, rates, extra, map_a, map_i,
    out_rec, out_act, out_b, out_ca, out_ci, out_cs, out_decay, out_seg, out_exp, out_block, out_sel,
    *, capacity, experts,
):
    tokens, channels = rec.shape
    heads = channels // 128
    first = where_ref[0] * heads

    def block_of_tokens(i, _):
        rows = pl.ds(pl.multiple_of(i * 128, 128), 128)
        for h in range(heads):
            cols = slice(h * 128, (h + 1) * 128)
            values_bf = rec[rows, cols]
            x = values_bf.astype(F32)
            ra = sigmoid(dot(values_bf, map_a[first + h]))
            ig = sigmoid(dot(values_bf, map_i[first + h]))
            rate = rates[pl.ds(first + h, 1), :]
            log_decay = -rate * ra + extra[rows, h : h + 1]
            decay = jnp.exp(log_decay)
            scale = jnp.sqrt(minus_expm1(2.0 * log_decay))
            before = prev[rows, cols]
            state = decay * before + scale * ig * x
            g = gate_in[rows, cols].astype(F32)
            bend = jnp.tanh(gelu_scale * (g + gelu_cubic * g * g * g))
            act = 0.5 * g * (1.0 + bend)
            slope = 0.5 * (1.0 + bend) + 0.5 * g * (1.0 - bend * bend) * gelu_scale * (
                1.0 + 3.0 * gelu_cubic * g * g
            )
            out_rec[rows, cols] = (state * act).astype(BF16)
            out_act[rows, cols] = act
            out_b[rows, cols] = state * slope
            out_ca[rows, cols] = (decay * before - decay * decay / scale * ig * x) * -rate * ra * (1.0 - ra)
            out_ci[rows, cols] = scale * x * ig * (1.0 - ig)
            out_cs[rows, cols] = scale * ig
            out_decay[h, rows, :] = decay
        return 0

    lax.fori_loop(0, tokens // 128, block_of_tokens, 0)
    length = tokens // 8
    for h in range(heads):
        cols = slice(h * 128, (h + 1) * 128)
        product = jnp.ones((8, 128), F32)
        for i in range(length - 1, -1, -1):
            out_seg[h, pl.ds(i, 8, stride=length), :] = product
            product = product * out_decay[h, pl.ds(i, 8, stride=length), :]
        carry = jnp.ones((1, 128), F32)
        for k in range(7, -1, -1):
            rows = slice(k * length, (k + 1) * length)
            out_exp[rows, cols] = out_seg[h, rows, :] * carry
            carry = carry * product[k : k + 1, :]
        out_block[:, cols] = jnp.broadcast_to(carry, (8, 128))
    lane = lax.broadcasted_iota(jnp.int32, (tokens, 128), 1)
    first_id = ids[:, 0:1]
    second_id = ids[:, 1:2]
    one = (lane == first_id).astype(F32)
    two = (lane == second_id).astype(F32)
    lower = lax.broadcasted_iota(jnp.int32, (tokens, tokens), 0) > lax.broadcasted_iota(
        jnp.int32, (tokens, tokens), 1
    )
    rank = dot(lower.astype(F32).astype(BF16), (one + two).astype(BF16))
    place_one = first_id * capacity + jnp.sum(rank * one, axis=1, keepdims=True).astype(jnp.int32)
    place_two = second_id * capacity + jnp.sum(rank * two, axis=1, keepdims=True).astype(jnp.int32)
    slots = experts * capacity
    for at in range(0, slots, 256):
        slot = lax.broadcasted_iota(jnp.int32, (tokens, 256), 1) + at
        hit = (slot == place_one) | (slot == place_two)
        out_sel[:, at : at + 256] = jnp.where(hit, 1.0, 0.0).astype(BF16)


def early(position, ids, rec, gate_in, prev, rates, extra, map_a, map_i, capacity, experts):
    tokens, channels = rec.shape
    wide = made((tokens, channels), F32)
    heads = made((channels // 128, tokens, 128), F32)
    outs = (
        made((tokens, channels), BF16),
        wide, wide, wide, wide, wide, heads, heads, wide,
        made((8, channels), F32),
        made((tokens, experts * capacity), BF16),
    )
    args = (position, ids, rec, gate_in, prev, rates, extra, map_a, map_i)
    return pl.pallas_call(
        functools.partial(early_kernel, capacity=capacity, experts=experts),
        out_shape=outs,
        in_specs=[SMEM] + [whole(a.shape) for a in args[1:]],
        out_specs=[whole(o.shape) for o in outs],
        compiler_params=params(14),
        cost_estimate=cost(3 * 10**9, 8 * 2**20),
        name="early",
    )(args[0], *kept(args[1:]))


def build_kernel(where_ref, ids, weight, *refs, capacity, group, weighted):
    sources, out, rank_ref, weight_ref = refs[:-3], refs[-3], refs[-2], refs[-1]
    experts, tokens = rank_ref.shape

    @pl.when(pl.program_id(0) == 0)
    def _():
        name = lax.broadcasted_iota(jnp.int32, (experts, tokens), 0)
        one = jnp.where(name == ids[0:1, :], 1.0, 0.0)
        two = jnp.where(name == ids[1:2, :], 1.0, 0.0)
        both = one + two
        upper = lax.broadcasted_iota(jnp.int32, (tokens, tokens), 0) < lax.broadcasted_iota(
            jnp.int32, (tokens, tokens), 1
        )
        rank = dot(both.astype(BF16), upper.astype(F32).astype(BF16))
        rank_ref[...] = jnp.where(both > 0.0, rank, -1.0)
        weight_ref[...] = one * weight[0:1, :] + two * weight[1:2, :]

    first = pl.program_id(0) * group
    place = lax.broadcasted_iota(jnp.int32, (capacity, tokens), 0).astype(F32)
    picks, weights = [], []
    for e in range(group):
        hit = place == rank_ref[pl.ds(first + e, 1), :]
        picks.append(jnp.where(hit, 1.0, 0.0))
        weights.append(
            jnp.sum(jnp.where(hit, weight_ref[pl.ds(first + e, 1), :], 0.0), axis=1, keepdims=True)
        )
    pick = jnp.concatenate(picks, axis=0).astype(BF16)
    by = jnp.concatenate(weights, axis=0)
    at = 0
    for source, scaled in zip(sources, weighted):
        rows = dot(pick, source[...])
        if scaled:
            rows = rows * by
        out[:, at : at + source.shape[1]] = rows.astype(BF16)
        at += source.shape[1]


def build(position, ids, weight, parts, capacity, experts, group=8):
    tokens = ids.shape[1]
    total = sum(width for _, width, _, _ in parts)
    specs = [pl.BlockSpec(ids.shape, lambda i, where: (0, 0))] * 2
    for _, width, column, _ in parts:
        specs.append(pl.BlockSpec((tokens, width), functools.partial(column_block, column)))
    return pl.pallas_call(
        functools.partial(
            build_kernel, capacity=capacity, group=group, weighted=tuple(p[3] for p in parts)
        ),
        out_shape=made((experts * capacity, total), BF16),
        grid_spec=pltpu.PrefetchScalarGridSpec(
            num_scalar_prefetch=1,
            grid=(experts // group,),
            in_specs=specs,
            out_specs=pl.BlockSpec((group * capacity, total), lambda i, where: (i, 0)),
            scratch_shapes=[pltpu.VMEM((experts, tokens), F32), pltpu.VMEM((experts, tokens), F32)],
        ),
        compiler_params=params(14),
        cost_estimate=cost(1400000 * total, 5000 * total),
    )(position, *kept([ids, weight, *(p[0] for p in parts)]))


def column_block(column, i, where):
    return (0, where[0] if column is None else column)


def weights_kernel(
    where_ref, w_gate, w_up, w_down, whole_own, *refs, row_part, cot_part,
):
    pieces = refs[:8]
    out_gate_up, out_down, out_gate, out_up = refs[8:]
    at, core = where_ref[0], where_ref[1]
    width, units = w_gate.shape
    half = width // 2
    first = ((0,), (0,))
    mine = pl.multiple_of(core * half, half)
    other = pl.multiple_of(half - core * half, half)
    for weights, out in ((w_gate, out_gate), (w_up, out_up)):
        out[at] = dot(weights[...], whole_own[...], first).astype(BF16)
        for step, n in ((3, 0), (1, 1)):
            out[lax.rem(at + step, 4)] = (
                dot(weights[pl.ds(mine, half), :], pieces[n][...], first)
                + dot(weights[pl.ds(other, half), :], pieces[4 + n][...], first)
            ).astype(BF16)
        quarter = half // 2
        out[lax.rem(at + 2, 4)] = sum(
            dot(weights[pl.ds(start + n * quarter, quarter), :], pieces[side + 2 + n][...], first)
            for start, side in ((mine, 0), (other, 4))
            for n in range(2)
        ).astype(BF16)
    rest = width - 4 * row_part
    out_gate_up[:rest, :units] = w_gate[4 * row_part :, :]
    out_gate_up[:rest, units:] = w_up[4 * row_part :, :]
    cot_rest = width - 4 * cot_part
    out_down[:cot_rest, :] = w_down[:, 4 * cot_part :].T
    for n, step in enumerate((2, 0, 3, 1)):
        group = lax.rem(at + step, 4)
        lines = pl.ds(pl.multiple_of(group * row_part, row_part), row_part)
        columns = pl.ds(pl.multiple_of(group * cot_part, 128), cot_part)
        to = slice(rest + n * row_part, rest + (n + 1) * row_part)
        out_gate_up[to, :units] = w_gate[lines, :]
        out_gate_up[to, units:] = w_up[lines, :]
        to = slice(cot_rest + n * cot_part, cot_rest + (n + 1) * cot_part)
        out_down[to, :] = w_down[:, columns].T


def folded_weights(position, w_gate, w_up, w_down, own, pieces, row_part, cot_part):
    width, units = w_gate.shape
    args = (position, w_gate, w_up, w_down, own, *pieces)
    fold = made((4, units, own.shape[1]), BF16)
    outs = (made((width, 2 * units), BF16), made((width, units), BF16), fold, fold)
    return pl.pallas_call(
        functools.partial(weights_kernel, row_part=row_part, cot_part=cot_part),
        out_shape=outs,
        in_specs=[SMEM] + [whole(a.shape) for a in args[1:]],
        out_specs=[whole(o.shape) for o in outs],
        compiler_params=params(24),
        cost_estimate=cost(4 * 10**9, 7 * 2**20),
        name="folded",
    )(position, *kept([w_gate, w_up, w_down, own]), *pieces)


def ahead_kernel(gate_up, down, *refs, row_part, row_from, cot_from):
    pieces, out = refs[:-1], refs[-1]
    half = pieces[0].shape[0]
    wide = gate_up.shape[1]
    for n in range(2):
        lines = slice(n * half, (n + 1) * half)
        rows = jnp.concatenate([p[:, :row_part] for p in pieces[n::2]], axis=1)
        cots = jnp.concatenate([p[:, row_part:] for p in pieces[n::2]], axis=1)
        out[lines, :wide] = dot(rows, gate_up[row_from:, :])
        out[lines, wide:] = dot(cots, down[cot_from:, :])


def ahead(pieces, gate_up, down, row_part, cot_part):
    width = gate_up.shape[0]
    out = made((2 * pieces[0].shape[0], gate_up.shape[1] + down.shape[1]), F32)
    args = (gate_up, down, *pieces)
    return pl.pallas_call(
        functools.partial(
            ahead_kernel,
            row_part=row_part,
            row_from=width - 3 * row_part,
            cot_from=width - 3 * cot_part,
        ),
        out_shape=out,
        in_specs=[whole(a.shape) for a in args],
        out_specs=whole(out.shape),
        compiler_params=params(20),
        cost_estimate=cost(2 * 10**9, 12 * 2**20),
        name="ahead",
    )(*kept([gate_up, down]), *pieces)


def expert_kernel(
    got_rows, got_cot, far_top, far_bottom, before, gate_up, down, fold_gate, fold_up,
    out_hidden, out_gate, out_up, out_mix, *, row_part,
):
    units = down.shape[1]
    upper = pl.program_id(0) < pl.num_programs(0) // 2
    far = jnp.where(upper, far_top[...], far_bottom[...])
    rows = jnp.concatenate([got_rows[...], far[:, :row_part]], axis=1)
    cots = jnp.concatenate([got_cot[...], far[:, row_part:]], axis=1)
    both = dot(rows, gate_up[...]) + before[:, : 2 * units]
    gate_pre, up_pre = both[:, :units], both[:, units:]
    hidden_cot = dot(cots, down[...]) + before[:, 2 * units :]
    sigma = sigmoid(gate_pre)
    swish = gate_pre * sigma
    out_hidden[...] = (swish * up_pre).astype(BF16)
    gate_cot = (hidden_cot * up_pre * sigma * (1.0 + gate_pre * (1.0 - sigma))).astype(BF16)
    up_cot = (hidden_cot * swish).astype(BF16)
    out_gate[...] = gate_cot
    out_up[...] = up_cot
    for c in range(4):
        out_mix[c] = (dot(gate_cot, fold_gate[c]) + dot(up_cot, fold_up[c])).astype(BF16)


def first_rows(array, count):
    return pl.BlockSpec(
        (count, array.shape[1]), lambda i: (0, 0), pipeline_mode=pl.Buffered(1)
    )


def expert(got, far, before, gate_up, down, fold_gate, fold_up, row_part, cot_part, steps=4):
    rows = got.shape[0]
    width, hidden = down.shape
    block = rows // steps
    part = fold_gate.shape[2]
    half = steps // 2
    row_rest, cot_rest = width - 4 * row_part, width - 4 * cot_part
    narrow = made((rows, hidden), BF16)
    mine = pl.BlockSpec((block, hidden), lambda i: (i, 0))
    return pl.pallas_call(
        functools.partial(expert_kernel, row_part=row_part),
        out_shape=(narrow, narrow, narrow, made((4, rows, part), BF16)),
        grid=(steps,),
        in_specs=[
            pl.BlockSpec((block, row_rest), lambda i: (i, 0)),
            pl.BlockSpec((block, cot_rest), lambda i: (i, row_rest // cot_rest)),
            pl.BlockSpec((block, row_part + cot_part), lambda i: (jnp.minimum(i, half - 1), 0)),
            pl.BlockSpec((block, row_part + cot_part), lambda i: (jnp.maximum(i - half, 0), 0)),
            pl.BlockSpec((block, before.shape[1]), lambda i: (i, 0)),
            first_rows(gate_up, row_rest + row_part),
            first_rows(down, cot_rest + cot_part),
            whole(fold_gate.shape),
            whole(fold_up.shape),
        ],
        out_specs=[mine, mine, mine, pl.BlockSpec((4, block, part), lambda i: (0, i, 0))],
        compiler_params=params(26),
        cost_estimate=cost(5 * 10**9, 16 * 2**20),
        name="expert",
    )(*kept([got, got]), *far, *kept([before, gate_up, down, fold_gate, fold_up]))


def grads_kernel(where_ref, got_rows, got_cot, *refs, row_part, cot_part):
    pieces = refs[:8]
    hidden, gate_cot, up_cot, out_gate, out_up, out_down = refs[8:]
    at = where_ref[0]
    first = ((0,), (0,))
    rows = got_rows[...]
    out_gate[0, 4 * row_part :, :] = dot(rows, gate_cot[...], first)
    out_up[0, 4 * row_part :, :] = dot(rows, up_cot[...], first)
    out_down[0, :, 4 * cot_part :] = dot(hidden[...], got_cot[...], first)
    for n, step in enumerate(ring_steps):
        group = lax.rem(at + step, 4)
        top, bottom = pieces[2 * n], pieces[2 * n + 1]
        half = top.shape[0]
        lines = pl.ds(pl.multiple_of(group * row_part, row_part), row_part)
        columns = pl.ds(pl.multiple_of(group * cot_part, 128), cot_part)
        for cot, out in ((gate_cot, out_gate), (up_cot, out_up)):
            out[0, lines, :] = dot(top[:, :row_part], cot[:half, :], first) + dot(
                bottom[:, :row_part], cot[half:, :], first
            )
        out_down[0, :, columns] = dot(hidden[:half, :], top[:, row_part:], first) + dot(
            hidden[half:, :], bottom[:, row_part:], first
        )


def grads(position, got, pieces, hidden, gate_cot, up_cot, width, row_part, cot_part):
    rows, units = hidden.shape
    row_rest, cot_rest = width - 4 * row_part, width - 4 * cot_part
    outs = (
        made((1, width, units), F32),
        made((1, width, units), F32),
        made((1, units, width), F32),
    )
    tail = (*pieces, hidden, gate_cot, up_cot)
    return pl.pallas_call(
        functools.partial(grads_kernel, row_part=row_part, cot_part=cot_part),
        out_shape=outs,
        grid=(1,),
        in_specs=[
            SMEM,
            pl.BlockSpec((rows, row_rest), lambda i: (0, 0), pipeline_mode=pl.Buffered(1)),
            pl.BlockSpec(
                (rows, cot_rest), lambda i: (0, row_rest // cot_rest), pipeline_mode=pl.Buffered(1)
            ),
            *(whole(a.shape) for a in tail),
        ],
        out_specs=[whole(o.shape) for o in outs],
        compiler_params=params(30),
        cost_estimate=cost(4 * 10**9, 17 * 2**20),
        name="grads",
    )(position, *kept([got, got]), *pieces, *kept(tail[len(pieces) :]))


def proj_kernel(where_ref, gate_cot, up_cot, w_gate, w_up, local, *refs):
    pieces, out = refs[:-1], refs[-1]
    at = where_ref[0]
    core = where_ref[1]
    first = ((0,), (0,))
    for n, step in enumerate(ring_steps):
        group = lax.rem(at + step, 4)
        top, bottom = pieces[2 * n], pieces[2 * n + 1]
        half = top.shape[0]
        push_gate, push_up = (
            (dot(cot[:half, :], top[...], first) + dot(cot[half:, :], bottom[...], first)).astype(BF16)
            for cot in (gate_cot, up_cot)
        )
        term = dot(w_gate[...], push_gate) + dot(w_up[...], push_up)
        if step == 0:
            term = term + local[...]
        term = term.astype(BF16)
        lines = out.shape[3]
        for s in range(2 * out.shape[2]):
            slot = lax.rem(s % 2 + core, 2)
            out[slot, group, s // 2] = term[s * lines : (s + 1) * lines, :]


def proj(position, gate_cot, up_cot, w_gate, w_up, local, pieces, lines):
    width, part = w_gate.shape[0], pieces[0].shape[1]
    args = (position, gate_cot, up_cot, w_gate, w_up, local, *pieces)
    out = made((2, 4, width // lines // 2, lines, part), BF16)
    return pl.pallas_call(
        proj_kernel,
        out_shape=out,
        in_specs=[SMEM] + [whole(a.shape) for a in args[1:]],
        out_specs=whole(out.shape),
        compiler_params=params(22),
        cost_estimate=cost(4 * 10**9, 14 * 2**20),
        name="proj",
    )(position, *kept(args[1:6]), *pieces)


def scan_kernel(back, sel, base, act, b, decay, seg, block, out_grad, out_local, out_pair, drive, part):
    tokens, channels = base.shape
    length = tokens // 8
    mix = base[...]
    total = back[0].astype(F32) + back[1].astype(F32) + back[2].astype(F32) + back[3].astype(F32)
    mix = mix + dot(sel[...], total.astype(BF16))
    out_grad[...] = (mix * b[...]).astype(BF16)
    push = mix * act[...]
    for h in range(channels // 128):
        cols = slice(h * 128, (h + 1) * 128)
        drive[h] = push[:, cols]
        value = drive[h, pl.ds(length - 1, 8, stride=length), :]
        part[h, pl.ds(length - 1, 8, stride=length), :] = value
        for i in range(length - 2, -1, -1):
            value = (
                drive[h, pl.ds(i, 8, stride=length), :]
                + decay[h, pl.ds(i + 1, 8, stride=length), :] * value
            )
            part[h, pl.ds(i, 8, stride=length), :] = value
        lead = decay[h, pl.ds(0, 8, stride=length), :]
        inner = seg[h, pl.ds(0, 8, stride=length), :]
        carry = jnp.zeros((1, 128), F32)
        for k in range(7, -1, -1):
            rows = slice(k * length, (k + 1) * length)
            out_local[rows, cols] = part[h, rows, :] + seg[h, rows, :] * carry
            one = slice(k, k + 1)
            carry = lead[one, :] * (value[one, :] + inner[one, :] * carry)
        pair = jnp.concatenate([carry, block[0:1, cols]], axis=0)
        out_pair[:, :, cols] = jnp.broadcast_to(pair[None], (out_pair.shape[0], *pair.shape))


def scanned(back, sel, base, act, b, decay, seg, block, sources):
    tokens, channels = base.shape
    args = (back, sel, base, act, b, decay, seg, block)
    outs = (
        made((tokens, channels), BF16),
        made((tokens, channels), F32),
        made((sources, 2, channels), F32),
    )
    return pl.pallas_call(
        scan_kernel,
        out_shape=outs,
        in_specs=[whole(a.shape) for a in args],
        out_specs=[whole(o.shape) for o in outs],
        scratch_shapes=[pltpu.VMEM(decay.shape, F32), pltpu.VMEM(decay.shape, F32)],
        compiler_params=params(14),
        cost_estimate=cost(4 * 10**8, 8 * 2**20),
        name="scanned",
    )(back, *kept(args[1:]))


def final_kernel(where_ref, pairs, local, exp, ca, ci, cs, map_a, map_i, out):
    channels = local.shape[1]
    heads = channels // 128
    first = where_ref[0] * heads
    total = jnp.zeros((1, channels), F32)
    me = where_ref[2]
    for s in range(pairs.shape[0] - 1, 0, -1):
        total = jnp.where(me < s, pairs[s, 0:1, :] + pairs[s, 1:2, :] * total, total)
    for h in range(heads):
        cols = slice(h * 128, (h + 1) * 128)
        cot = local[:, cols] + exp[:, cols] * total[:, cols]
        a_cot = (cot * ca[:, cols]).astype(BF16)
        i_cot = (cot * ci[:, cols]).astype(BF16)
        result = (
            cot * cs[:, cols]
            + dot(a_cot, map_a[first + h], ((1,), (1,)))
            + dot(i_cot, map_i[first + h], ((1,), (1,)))
        )
        out[:, cols] = result.astype(BF16)


def final(position, pairs, local, exp, ca, ci, cs, map_a, map_i):
    args = (position, pairs, local, exp, ca, ci, cs, map_a, map_i)
    return pl.pallas_call(
        final_kernel,
        out_shape=made(local.shape, BF16),
        in_specs=[SMEM] + [whole(a.shape) for a in args[1:]],
        out_specs=whole(local.shape),
        compiler_params=params(8),
        cost_estimate=cost(10**8, 4 * 2**20),
        name="final",
    )(position, pairs, *kept(args[2:]))


def shifted(piece, by):
    return lax.ppermute(piece, "tp", [(i, (i + by) % 4) for i in range(4)])


def ring_gather(top, bottom):
    left_top, right_bottom = shifted(top, 1), shifted(bottom, -1)
    left_bottom, right_top = shifted(bottom, 1), shifted(top, -1)
    far_top, far_bottom = shifted(left_top, 1), shifted(right_bottom, -1)
    return top, bottom, left_top, left_bottom, right_top, right_bottom, far_top, far_bottom


def shared_ring_gather(own, core):
    half = own.shape[0] // 2
    mine = lax.dynamic_slice_in_dim(own, core * half, half, 0)
    left, right = shifted(mine, 1), shifted(mine, -1)
    quarter = half // 2
    far_top, far_bottom = shifted(left[:quarter], 1), shifted(right[quarter:], -1)
    pieces = (left, right, far_top, far_bottom)
    others = tuple(lax.ppermute(p, "core", [(0, 1), (1, 0)]) for p in pieces)
    return pieces + others


def per_device(
    layer_input, out_cot, expert_ids, route_weight, w_gate, w_up, w_down, out_proj,
    rec_input, gate_input, prev_state, decay_param, extra_decay, gate_a_w, gate_i_w,
):
    sources = lax.axis_size("sq") * lax.axis_size("core")
    tp = lax.axis_index("tp")
    core = lax.axis_index("core")
    sp_axes = ("sq", "core")
    sp = lax.axis_index("sq") * 2 + core
    position = jnp.stack([tp, core, sp]).astype(jnp.int32)
    w_gate, w_up, w_down = w_gate[0], w_up[0], w_down[0]
    tokens, width = layer_input.shape
    capacity = 5 * tokens * expert_ids.shape[1] // (4 * sources)
    slots = sources * capacity
    row_part, cot_part = width // 8, 3 * width // 16
    row_rest, cot_rest = width - 4 * row_part, width - 4 * cot_part
    ids, weight = expert_ids.T, route_weight.T

    def exchanged(rows):
        return lax.all_to_all(
            rows.reshape(sources, capacity, -1), sp_axes, 0, 0, tiled=True
        ).reshape(rows.shape)

    spread = build(
        position, ids, weight,
        [(layer_input, row_part, None, False), (out_cot, cot_part, None, True)],
        capacity, sources,
    )
    spread = exchanged(spread)
    projections = shared_ring_gather(out_proj, core)
    gate_up, down, fold_gate, fold_up = folded_weights(
        position, w_gate, w_up, w_down, out_proj, projections, row_part, cot_part
    )
    rates = (decay_factor * jax.nn.softplus(-decay_param)).reshape(-1, gate_a_w.shape[1])
    rec_output, act, b, ca, ci, cs, decay, seg, exp, block, sel = early(
        position, expert_ids, rec_input, gate_input, prev_state, rates, extra_decay.T,
        gate_a_w, gate_i_w, capacity, sources,
    )
    direct = build(
        position, ids, weight,
        [
            (layer_input, row_rest, 4 * row_part // row_rest, False),
            (out_cot, cot_rest, 4 * cot_part // cot_rest, True),
            (rec_output, rec_output.shape[1], 0, False),
        ],
        capacity, sources,
    )
    got = exchanged(direct)
    pieces = ring_gather(spread[: slots // 2], spread[slots // 2 :])
    base = jnp.dot(out_cot, out_proj, preferred_element_type=F32)
    local_proj = lax.dot_general(
        out_cot, rec_output, (((0,), (0,)), ((), ())), preferred_element_type=F32
    )
    before = ahead(pieces[:6], gate_up, down, row_part, cot_part)
    hidden, gate_cot, up_cot, mix = expert(
        got, pieces[6:], before, gate_up, down, fold_gate, fold_up, row_part, cot_part
    )
    back = lax.all_to_all(
        mix.reshape(4 * sources, capacity, -1), ("tp", *sp_axes), 0, 0, tiled=True
    ).reshape(mix.shape)
    grad_gate, grad_up, grad_down = grads(
        position, got, pieces, hidden, gate_cot, up_cot, width, row_part, cot_part
    )
    start = row_rest + cot_rest
    recs = ring_gather(got[: slots // 2, start:], got[slots // 2 :, start:])
    lines = width // sources
    parts = proj(position, gate_cot, up_cot, w_gate, w_up, local_proj, recs, lines)
    other = lax.ppermute(parts[1], "core", [(0, 1), (1, 0)])
    chip = (parts[0].astype(F32) + other.astype(F32)).astype(BF16)
    arrived = lax.all_to_all(
        chip.reshape(4 * chip.shape[1], lines, -1), ("tp", "sq"), 0, 0, tiled=True
    )
    grad_out_proj = arrived.astype(F32).sum(axis=0)
    gate_input_grad, local, pair = scanned(
        back, sel, base, act, b, decay, seg, block, sources
    )
    pairs = lax.all_to_all(pair, sp_axes, 0, 0, tiled=True)
    rec_input_grad = final(position, pairs, local, exp, ca, ci, cs, gate_a_w, gate_i_w)
    return (grad_gate, grad_up, grad_down, grad_out_proj, rec_input_grad, gate_input_grad)


def solution(mesh):
    sp, tp = mesh.devices.shape
    inner = Mesh(mesh.devices.reshape(sp // 2, 2, tp), ("sq", "core", "tp"))
    sp = ("sq", "core")
    in_specs = (
        P(sp, None),
        P(sp, None),
        P(sp, None),
        P(sp, None),
        P(sp, None, "tp"),
        P(sp, None, "tp"),
        P(sp, "tp", None),
        P(None, "tp"),
        P(sp, "tp"),
        P(sp, "tp"),
        P(sp, "tp"),
        P(),
        P("tp", sp),
        P(),
        P(),
    )
    out_specs = (
        P(sp, None, "tp"),
        P(sp, None, "tp"),
        P(sp, "tp", None),
        P(sp, "tp"),
        P(sp, "tp"),
        P(sp, "tp"),
    )
    return jax.shard_map(
        per_device, mesh=inner, in_specs=in_specs, out_specs=out_specs, check_vma=False
    )
```

```python
import functools
import jax
import jax.numpy as jnp
from jax import lax
from jax.experimental import pallas as pl
from jax.experimental.pallas import tpu as pltpu
from jax.sharding import Mesh, PartitionSpec as P


F32 = jnp.float32
BF16 = jnp.bfloat16
gelu_scale = 0.7978845608028654
gelu_cubic = 0.044715
decay_factor = 8.0
ring_steps = (0, 3, 1, 2)


def params(limit_mib=48, **extra):
    return pltpu.CompilerParams(vmem_limit_bytes=limit_mib * 1024 * 1024, **extra)


def cost(flops, moved):
    return pl.CostEstimate(flops=flops, bytes_accessed=moved, transcendentals=0)


def whole(shape):
    return pl.BlockSpec(shape, lambda *_: (0,) * len(shape), pipeline_mode=pl.Buffered(1))


SMEM = pl.BlockSpec(memory_space=pltpu.SMEM)


def made(shape, dtype):
    return pltpu.HBM(shape, dtype)


def kept(arrays):
    return [pltpu.with_memory_space_constraint(a, pltpu.HBM) for a in arrays]


def dot(a, b, dims=((1,), (0,))):
    return lax.dot_general(a, b, (dims, ((), ())), preferred_element_type=F32)


def sigmoid(v):
    return 1.0 / (1.0 + jnp.exp(-v))


def minus_expm1(v):
    series = 1.0 + v / 8.0
    for order in range(7, 1, -1):
        series = 1.0 + v / order * series
    return jnp.where(v > -0.5, -v * series, 1.0 - jnp.exp(v))


def early_kernel(
    where_ref, ids, rec, gate_in, prev, rates, extra, map_a, map_i,
    out_rec, out_act, out_b, out_ca, out_ci, out_cs, out_decay, out_seg, out_exp, out_block, out_sel,
    *, capacity, experts,
):
    tokens, channels = rec.shape
    heads = channels // 128
    first = where_ref[0] * heads

    def block_of_tokens(i, _):
        rows = pl.ds(pl.multiple_of(i * 128, 128), 128)
        for h in range(heads):
            cols = slice(h * 128, (h + 1) * 128)
            values_bf = rec[rows, cols]
            x = values_bf.astype(F32)
            ra = sigmoid(dot(values_bf, map_a[first + h]))
            ig = sigmoid(dot(values_bf, map_i[first + h]))
            rate = rates[pl.ds(first + h, 1), :]
            log_decay = -rate * ra + extra[rows, h : h + 1]
            decay = jnp.exp(log_decay)
            scale = jnp.sqrt(minus_expm1(2.0 * log_decay))
            before = prev[rows, cols]
            state = decay * before + scale * ig * x
            g = gate_in[rows, cols].astype(F32)
            bend = jnp.tanh(gelu_scale * (g + gelu_cubic * g * g * g))
            act = 0.5 * g * (1.0 + bend)
            slope = 0.5 * (1.0 + bend) + 0.5 * g * (1.0 - bend * bend) * gelu_scale * (
                1.0 + 3.0 * gelu_cubic * g * g
            )
            out_rec[rows, cols] = (state * act).astype(BF16)
            out_act[rows, cols] = act
            out_b[rows, cols] = state * slope
            out_ca[rows, cols] = (decay * before - decay * decay / scale * ig * x) * -rate * ra * (1.0 - ra)
            out_ci[rows, cols] = scale * x * ig * (1.0 - ig)
            out_cs[rows, cols] = scale * ig
            out_decay[h, rows, :] = decay
        return 0

    lax.fori_loop(0, tokens // 128, block_of_tokens, 0)
    length = tokens // 8
    for h in range(heads):
        cols = slice(h * 128, (h + 1) * 128)
        product = jnp.ones((8, 128), F32)
        for i in range(length - 1, -1, -1):
            out_seg[h, pl.ds(i, 8, stride=length), :] = product
            product = product * out_decay[h, pl.ds(i, 8, stride=length), :]
        carry = jnp.ones((1, 128), F32)
        for k in range(7, -1, -1):
            rows = slice(k * length, (k + 1) * length)
            out_exp[rows, cols] = out_seg[h, rows, :] * carry
            carry = carry * product[k : k + 1, :]
        out_block[:, cols] = jnp.broadcast_to(carry, (8, 128))
    lane = lax.broadcasted_iota(jnp.int32, (tokens, 128), 1)
    first_id = ids[:, 0:1]
    second_id = ids[:, 1:2]
    one = (lane == first_id).astype(F32)
    two = (lane == second_id).astype(F32)
    lower = lax.broadcasted_iota(jnp.int32, (tokens, tokens), 0) > lax.broadcasted_iota(
        jnp.int32, (tokens, tokens), 1
    )
    rank = dot(lower.astype(F32).astype(BF16), (one + two).astype(BF16))
    place_one = first_id * capacity + jnp.sum(rank * one, axis=1, keepdims=True).astype(jnp.int32)
    place_two = second_id * capacity + jnp.sum(rank * two, axis=1, keepdims=True).astype(jnp.int32)
    slots = experts * capacity

    def block_of_slots(i, _):
        at = pl.multiple_of(i * 256, 256)
        slot = lax.broadcasted_iota(jnp.int32, (tokens, 256), 1) + at
        hit = (slot == place_one) | (slot == place_two)
        out_sel[:, pl.ds(at, 256)] = jnp.where(hit, 1.0, 0.0).astype(BF16)
        return 0

    lax.fori_loop(0, slots // 256, block_of_slots, 0)


def early(position, ids, rec, gate_in, prev, rates, extra, map_a, map_i, capacity, experts):
    tokens, channels = rec.shape
    wide = made((tokens, channels), F32)
    heads = made((channels // 128, tokens, 128), F32)
    outs = (
        made((tokens, channels), BF16),
        wide, wide, wide, wide, wide, heads, heads, wide,
        made((8, channels), F32),
        made((tokens, experts * capacity), BF16),
    )
    args = (position, ids, rec, gate_in, prev, rates, extra, map_a, map_i)
    return pl.pallas_call(
        functools.partial(early_kernel, capacity=capacity, experts=experts),
        out_shape=outs,
        in_specs=[SMEM] + [whole(a.shape) for a in args[1:]],
        out_specs=[whole(o.shape) for o in outs],
        compiler_params=params(14),
        cost_estimate=cost(3 * 10**9, 8 * 2**20),
        name="early",
    )(args[0], *kept(args[1:]))


def build_kernel(where_ref, ids, weight, *refs, capacity, group, weighted):
    sources, out, rank_ref, weight_ref = refs[:-3], refs[-3], refs[-2], refs[-1]
    experts, tokens = rank_ref.shape

    @pl.when(pl.program_id(0) == 0)
    def _():
        name = lax.broadcasted_iota(jnp.int32, (experts, tokens), 0)
        one = jnp.where(name == ids[0:1, :], 1.0, 0.0)
        two = jnp.where(name == ids[1:2, :], 1.0, 0.0)
        both = one + two
        upper = lax.broadcasted_iota(jnp.int32, (tokens, tokens), 0) < lax.broadcasted_iota(
            jnp.int32, (tokens, tokens), 1
        )
        rank = dot(both.astype(BF16), upper.astype(F32).astype(BF16))
        rank_ref[...] = jnp.where(both > 0.0, rank, -1.0)
        weight_ref[...] = one * weight[0:1, :] + two * weight[1:2, :]

    first = pl.program_id(0) * group
    place = lax.broadcasted_iota(jnp.int32, (capacity, tokens), 0).astype(F32)
    picks, weights = [], []
    for e in range(group):
        hit = place == rank_ref[pl.ds(first + e, 1), :]
        picks.append(jnp.where(hit, 1.0, 0.0))
        weights.append(
            jnp.sum(jnp.where(hit, weight_ref[pl.ds(first + e, 1), :], 0.0), axis=1, keepdims=True)
        )
    pick = jnp.concatenate(picks, axis=0).astype(BF16)
    by = jnp.concatenate(weights, axis=0)
    at = 0
    for source, scaled in zip(sources, weighted):
        rows = dot(pick, source[...])
        if scaled:
            rows = rows * by
        out[:, at : at + source.shape[1]] = rows.astype(BF16)
        at += source.shape[1]


def build(position, ids, weight, parts, capacity, experts, group=8):
    tokens = ids.shape[1]
    total = sum(width for _, width, _, _ in parts)
    specs = [pl.BlockSpec(ids.shape, lambda i, where: (0, 0))] * 2
    for _, width, column, _ in parts:
        specs.append(pl.BlockSpec((tokens, width), functools.partial(column_block, column)))
    return pl.pallas_call(
        functools.partial(
            build_kernel, capacity=capacity, group=group, weighted=tuple(p[3] for p in parts)
        ),
        out_shape=made((experts * capacity, total), BF16),
        grid_spec=pltpu.PrefetchScalarGridSpec(
            num_scalar_prefetch=1,
            grid=(experts // group,),
            in_specs=specs,
            out_specs=pl.BlockSpec((group * capacity, total), lambda i, where: (i, 0)),
            scratch_shapes=[pltpu.VMEM((experts, tokens), F32), pltpu.VMEM((experts, tokens), F32)],
        ),
        compiler_params=params(14),
        cost_estimate=cost(1400000 * total, 5000 * total),
    )(position, *kept([ids, weight, *(p[0] for p in parts)]))


def column_block(column, i, where):
    return (0, where[0] if column is None else column)


def weights_kernel(
    where_ref, w_gate, w_up, w_down, whole_own, *refs, row_part, cot_part,
):
    pieces = refs[:8]
    out_gate_up, out_down, out_gate, out_up = refs[8:]
    at, core = where_ref[0], where_ref[1]
    width, units = w_gate.shape
    half = width // 2
    first = ((0,), (0,))
    mine = pl.multiple_of(core * half, half)
    other = pl.multiple_of(half - core * half, half)
    for weights, out in ((w_gate, out_gate), (w_up, out_up)):
        out[at] = dot(weights[...], whole_own[...], first).astype(BF16)
        for step, n in ((3, 0), (1, 1)):
            out[lax.rem(at + step, 4)] = (
                dot(weights[pl.ds(mine, half), :], pieces[n][...], first)
                + dot(weights[pl.ds(other, half), :], pieces[4 + n][...], first)
            ).astype(BF16)
        quarter = half // 2
        out[lax.rem(at + 2, 4)] = sum(
            dot(weights[pl.ds(start + n * quarter, quarter), :], pieces[side + 2 + n][...], first)
            for start, side in ((mine, 0), (other, 4))
            for n in range(2)
        ).astype(BF16)
    rest = width - 4 * row_part
    out_gate_up[:rest, :units] = w_gate[4 * row_part :, :]
    out_gate_up[:rest, units:] = w_up[4 * row_part :, :]
    cot_rest = width - 4 * cot_part
    out_down[:cot_rest, :] = w_down[:, 4 * cot_part :].T
    for n, step in enumerate((2, 0, 3, 1)):
        group = lax.rem(at + step, 4)
        lines = pl.ds(pl.multiple_of(group * row_part, row_part), row_part)
        columns = pl.ds(pl.multiple_of(group * cot_part, 128), cot_part)
        to = slice(rest + n * row_part, rest + (n + 1) * row_part)
        out_gate_up[to, :units] = w_gate[lines, :]
        out_gate_up[to, units:] = w_up[lines, :]
        to = slice(cot_rest + n * cot_part, cot_rest + (n + 1) * cot_part)
        out_down[to, :] = w_down[:, columns].T


def folded_weights(position, w_gate, w_up, w_down, own, pieces, row_part, cot_part):
    width, units = w_gate.shape
    args = (position, w_gate, w_up, w_down, own, *pieces)
    fold = made((4, units, own.shape[1]), BF16)
    outs = (made((width, 2 * units), BF16), made((width, units), BF16), fold, fold)
    return pl.pallas_call(
        functools.partial(weights_kernel, row_part=row_part, cot_part=cot_part),
        out_shape=outs,
        in_specs=[SMEM] + [whole(a.shape) for a in args[1:]],
        out_specs=[whole(o.shape) for o in outs],
        compiler_params=params(24),
        cost_estimate=cost(4 * 10**9, 7 * 2**20),
        name="folded",
    )(position, *kept([w_gate, w_up, w_down, own]), *pieces)


def ahead_kernel(gate_up, down, *refs, row_part, row_from, cot_from):
    pieces, out = refs[:-1], refs[-1]
    half = pieces[0].shape[0]
    wide = gate_up.shape[1]
    for n in range(2):
        lines = slice(n * half, (n + 1) * half)
        rows = jnp.concatenate([p[:, :row_part] for p in pieces[n::2]], axis=1)
        cots = jnp.concatenate([p[:, row_part:] for p in pieces[n::2]], axis=1)
        out[lines, :wide] = dot(rows, gate_up[row_from:, :])
        out[lines, wide:] = dot(cots, down[cot_from:, :])


def ahead(pieces, gate_up, down, row_part, cot_part):
    width = gate_up.shape[0]
    out = made((2 * pieces[0].shape[0], gate_up.shape[1] + down.shape[1]), F32)
    args = (gate_up, down, *pieces)
    return pl.pallas_call(
        functools.partial(
            ahead_kernel,
            row_part=row_part,
            row_from=width - 3 * row_part,
            cot_from=width - 3 * cot_part,
        ),
        out_shape=out,
        in_specs=[whole(a.shape) for a in args],
        out_specs=whole(out.shape),
        compiler_params=params(20),
        cost_estimate=cost(2 * 10**9, 12 * 2**20),
        name="ahead",
    )(*kept([gate_up, down]), *pieces)


def expert_kernel(
    got_rows, got_cot, far_top, far_bottom, before, gate_up, down, fold_gate, fold_up,
    out_hidden, out_gate, out_up, out_mix, *, row_part,
):
    units = down.shape[1]
    upper = pl.program_id(0) < pl.num_programs(0) // 2
    far = jnp.where(upper, far_top[...], far_bottom[...])
    rows = jnp.concatenate([got_rows[...], far[:, :row_part]], axis=1)
    cots = jnp.concatenate([got_cot[...], far[:, row_part:]], axis=1)
    both = dot(rows, gate_up[...]) + before[:, : 2 * units]
    gate_pre, up_pre = both[:, :units], both[:, units:]
    hidden_cot = dot(cots, down[...]) + before[:, 2 * units :]
    sigma = sigmoid(gate_pre)
    swish = gate_pre * sigma
    out_hidden[...] = (swish * up_pre).astype(BF16)
    gate_cot = (hidden_cot * up_pre * sigma * (1.0 + gate_pre * (1.0 - sigma))).astype(BF16)
    up_cot = (hidden_cot * swish).astype(BF16)
    out_gate[...] = gate_cot
    out_up[...] = up_cot
    for c in range(4):
        out_mix[c] = (dot(gate_cot, fold_gate[c]) + dot(up_cot, fold_up[c])).astype(BF16)


def first_rows(array, count):
    return pl.BlockSpec(
        (count, array.shape[1]), lambda i: (0, 0), pipeline_mode=pl.Buffered(1)
    )


def expert(got, far, before, gate_up, down, fold_gate, fold_up, row_part, cot_part, steps=4):
    rows = got.shape[0]
    width, hidden = down.shape
    block = rows // steps
    part = fold_gate.shape[2]
    half = steps // 2
    row_rest, cot_rest = width - 4 * row_part, width - 4 * cot_part
    narrow = made((rows, hidden), BF16)
    mine = pl.BlockSpec((block, hidden), lambda i: (i, 0))
    return pl.pallas_call(
        functools.partial(expert_kernel, row_part=row_part),
        out_shape=(narrow, narrow, narrow, made((4, rows, part), BF16)),
        grid=(steps,),
        in_specs=[
            pl.BlockSpec((block, row_rest), lambda i: (i, 0)),
            pl.BlockSpec((block, cot_rest), lambda i: (i, row_rest // cot_rest)),
            pl.BlockSpec((block, row_part + cot_part), lambda i: (jnp.minimum(i, half - 1), 0)),
            pl.BlockSpec((block, row_part + cot_part), lambda i: (jnp.maximum(i - half, 0), 0)),
            pl.BlockSpec((block, before.shape[1]), lambda i: (i, 0)),
            first_rows(gate_up, row_rest + row_part),
            first_rows(down, cot_rest + cot_part),
            whole(fold_gate.shape),
            whole(fold_up.shape),
        ],
        out_specs=[mine, mine, mine, pl.BlockSpec((4, block, part), lambda i: (0, i, 0))],
        compiler_params=params(26),
        cost_estimate=cost(5 * 10**9, 16 * 2**20),
        name="expert",
    )(*kept([got, got]), *far, *kept([before, gate_up, down, fold_gate, fold_up]))


def grads_kernel(where_ref, got_rows, got_cot, *refs, row_part, cot_part):
    pieces = refs[:8]
    hidden, gate_cot, up_cot, out_gate, out_up, out_down = refs[8:]
    at = where_ref[0]
    first = ((0,), (0,))
    rows = got_rows[...]
    out_gate[0, 4 * row_part :, :] = dot(rows, gate_cot[...], first)
    out_up[0, 4 * row_part :, :] = dot(rows, up_cot[...], first)
    out_down[0, :, 4 * cot_part :] = dot(hidden[...], got_cot[...], first)
    for n, step in enumerate(ring_steps):
        group = lax.rem(at + step, 4)
        top, bottom = pieces[2 * n], pieces[2 * n + 1]
        half = top.shape[0]
        lines = pl.ds(pl.multiple_of(group * row_part, row_part), row_part)
        columns = pl.ds(pl.multiple_of(group * cot_part, 128), cot_part)
        for cot, out in ((gate_cot, out_gate), (up_cot, out_up)):
            out[0, lines, :] = dot(top[:, :row_part], cot[:half, :], first) + dot(
                bottom[:, :row_part], cot[half:, :], first
            )
        out_down[0, :, columns] = dot(hidden[:half, :], top[:, row_part:], first) + dot(
            hidden[half:, :], bottom[:, row_part:], first
        )


def grads(position, got, pieces, hidden, gate_cot, up_cot, width, row_part, cot_part):
    rows, units = hidden.shape
    row_rest, cot_rest = width - 4 * row_part, width - 4 * cot_part
    outs = (
        made((1, width, units), F32),
        made((1, width, units), F32),
        made((1, units, width), F32),
    )
    tail = (*pieces, hidden, gate_cot, up_cot)
    return pl.pallas_call(
        functools.partial(grads_kernel, row_part=row_part, cot_part=cot_part),
        out_shape=outs,
        grid=(1,),
        in_specs=[
            SMEM,
            pl.BlockSpec((rows, row_rest), lambda i: (0, 0), pipeline_mode=pl.Buffered(1)),
            pl.BlockSpec(
                (rows, cot_rest), lambda i: (0, row_rest // cot_rest), pipeline_mode=pl.Buffered(1)
            ),
            *(whole(a.shape) for a in tail),
        ],
        out_specs=[whole(o.shape) for o in outs],
        compiler_params=params(30),
        cost_estimate=cost(4 * 10**9, 17 * 2**20),
        name="grads",
    )(position, *kept([got, got, *tail]))


def proj_kernel(where_ref, gate_cot, up_cot, w_gate, w_up, local, *refs):
    pieces, out = refs[:-1], refs[-1]
    core = where_ref[1]
    first = ((0,), (0,))
    for n, step in enumerate(ring_steps):
        top, bottom = pieces[2 * n], pieces[2 * n + 1]
        half = top.shape[0]
        push_gate, push_up = (
            (dot(cot[:half, :], top[...], first) + dot(cot[half:, :], bottom[...], first)).astype(BF16)
            for cot in (gate_cot, up_cot)
        )
        term = dot(w_gate[...], push_gate) + dot(w_up[...], push_up)
        if step == 0:
            term = term + local[...]
        term = term.astype(BF16)
        lines = out.shape[3]
        for s in range(2 * out.shape[2]):
            slot = lax.rem(s % 2 + core, 2)
            out[slot, n, s // 2] = term[s * lines : (s + 1) * lines, :]


def proj(position, gate_cot, up_cot, w_gate, w_up, local, pieces, lines):
    width, part = w_gate.shape[0], pieces[0].shape[1]
    args = (position, gate_cot, up_cot, w_gate, w_up, local, *pieces)
    out = made((2, 4, width // lines // 2, lines, part), BF16)
    return pl.pallas_call(
        proj_kernel,
        out_shape=out,
        in_specs=[SMEM] + [whole(a.shape) for a in args[1:]],
        out_specs=whole(out.shape),
        compiler_params=params(22),
        cost_estimate=cost(4 * 10**9, 14 * 2**20),
        name="proj",
    )(position, *kept(args[1:6]), *pieces)


def chip_kernel(kept_ref, other, out_own, *outs):
    half = out_own.shape[0] // 2
    out_own[...] = (kept_ref[0, 0].astype(F32) + other[0].astype(F32)).astype(BF16)
    for n in range(6):
        lines = slice((n % 2) * half, (n % 2 + 1) * half)
        at = 1 + n // 2
        outs[n][...] = (
            kept_ref[0, at, lines].astype(F32) + other[at, lines].astype(F32)
        ).astype(BF16)


def chip_sum(parts, other):
    groups, lines, width = other.shape[1:]
    half = made((groups // 2, lines, width), BF16)
    outs = (made((groups, lines, width), BF16),) + (half,) * 6
    return pl.pallas_call(
        chip_kernel,
        out_shape=outs,
        grid=(1,),
        in_specs=[
            pl.BlockSpec(
                (1, *parts.shape[1:]), lambda i: (0, 0, 0, 0, 0), pipeline_mode=pl.Buffered(1)
            ),
            whole(other.shape),
        ],
        out_specs=[whole(o.shape) for o in outs],
        compiler_params=params(16),
        cost_estimate=cost(10**7, 6 * 2**20),
        name="chipsum",
    )(*kept([parts]), other)


def scan_kernel(back, sel, base, act, b, decay, seg, block, out_grad, out_local, out_pair, drive, part):
    tokens, channels = base.shape
    length = tokens // 8
    mix = base[...]
    total = back[0].astype(F32) + back[1].astype(F32) + back[2].astype(F32) + back[3].astype(F32)
    mix = mix + dot(sel[...], total.astype(BF16))
    out_grad[...] = (mix * b[...]).astype(BF16)
    push = mix * act[...]
    for h in range(channels // 128):
        cols = slice(h * 128, (h + 1) * 128)
        drive[h] = push[:, cols]
        value = drive[h, pl.ds(length - 1, 8, stride=length), :]
        part[h, pl.ds(length - 1, 8, stride=length), :] = value
        for i in range(length - 2, -1, -1):
            value = (
                drive[h, pl.ds(i, 8, stride=length), :]
                + decay[h, pl.ds(i + 1, 8, stride=length), :] * value
            )
            part[h, pl.ds(i, 8, stride=length), :] = value
        lead = decay[h, pl.ds(0, 8, stride=length), :]
        inner = seg[h, pl.ds(0, 8, stride=length), :]
        carry = jnp.zeros((1, 128), F32)
        for k in range(7, -1, -1):
            rows = slice(k * length, (k + 1) * length)
            out_local[rows, cols] = part[h, rows, :] + seg[h, rows, :] * carry
            one = slice(k, k + 1)
            carry = lead[one, :] * (value[one, :] + inner[one, :] * carry)
        pair = jnp.concatenate([carry, block[0:1, cols]], axis=0)
        out_pair[:, :, cols] = jnp.broadcast_to(pair[None], (out_pair.shape[0], *pair.shape))


def scanned(back, sel, base, act, b, decay, seg, block, sources):
    tokens, channels = base.shape
    args = (back, sel, base, act, b, decay, seg, block)
    outs = (
        made((tokens, channels), BF16),
        made((tokens, channels), F32),
        made((sources, 2, channels), F32),
    )
    return pl.pallas_call(
        scan_kernel,
        out_shape=outs,
        in_specs=[whole(a.shape) for a in args],
        out_specs=[whole(o.shape) for o in outs],
        scratch_shapes=[pltpu.VMEM(decay.shape, F32), pltpu.VMEM(decay.shape, F32)],
        compiler_params=params(14),
        cost_estimate=cost(4 * 10**8, 8 * 2**20),
        name="scanned",
    )(back, *kept(args[1:]))


def final_kernel(where_ref, pairs, local, exp, ca, ci, cs, map_a, map_i, out):
    channels = local.shape[1]
    heads = channels // 128
    first = where_ref[0] * heads
    total = jnp.zeros((1, channels), F32)
    me = where_ref[2]
    for s in range(pairs.shape[0] - 1, 0, -1):
        total = jnp.where(me < s, pairs[s, 0:1, :] + pairs[s, 1:2, :] * total, total)
    for h in range(heads):
        cols = slice(h * 128, (h + 1) * 128)
        cot = local[:, cols] + exp[:, cols] * total[:, cols]
        a_cot = (cot * ca[:, cols]).astype(BF16)
        i_cot = (cot * ci[:, cols]).astype(BF16)
        result = (
            cot * cs[:, cols]
            + dot(a_cot, map_a[first + h], ((1,), (1,)))
            + dot(i_cot, map_i[first + h], ((1,), (1,)))
        )
        out[:, cols] = result.astype(BF16)


def final(position, pairs, local, exp, ca, ci, cs, map_a, map_i):
    args = (position, pairs, local, exp, ca, ci, cs, map_a, map_i)
    return pl.pallas_call(
        final_kernel,
        out_shape=made(local.shape, BF16),
        in_specs=[SMEM] + [whole(a.shape) for a in args[1:]],
        out_specs=whole(local.shape),
        compiler_params=params(8),
        cost_estimate=cost(10**8, 4 * 2**20),
        name="final",
    )(position, pairs, *kept(args[2:]))


def shifted(piece, by):
    return lax.ppermute(piece, "tp", [(i, (i + by) % 4) for i in range(4)])


def ring_gather(top, bottom):
    left_top, right_bottom = shifted(top, 1), shifted(bottom, -1)
    left_bottom, right_top = shifted(bottom, 1), shifted(top, -1)
    far_top, far_bottom = shifted(left_top, 1), shifted(right_bottom, -1)
    return top, bottom, left_top, left_bottom, right_top, right_bottom, far_top, far_bottom


def shared_ring_gather(own, core):
    half = own.shape[0] // 2
    mine = lax.dynamic_slice_in_dim(own, core * half, half, 0)
    left, right = shifted(mine, 1), shifted(mine, -1)
    quarter = half // 2
    far_top, far_bottom = shifted(left[:quarter], 1), shifted(right[quarter:], -1)
    pieces = (left, right, far_top, far_bottom)
    others = tuple(lax.ppermute(p, "core", [(0, 1), (1, 0)]) for p in pieces)
    return pieces + others


def per_device(
    layer_input, out_cot, expert_ids, route_weight, w_gate, w_up, w_down, out_proj,
    rec_input, gate_input, prev_state, decay_param, extra_decay, gate_a_w, gate_i_w,
):
    sources = lax.axis_size("sq") * lax.axis_size("core")
    tp = lax.axis_index("tp")
    core = lax.axis_index("core")
    sp_axes = ("sq", "core")
    sp = lax.axis_index("sq") * 2 + core
    position = jnp.stack([tp, core, sp]).astype(jnp.int32)
    w_gate, w_up, w_down = w_gate[0], w_up[0], w_down[0]
    tokens, width = layer_input.shape
    capacity = 5 * tokens * expert_ids.shape[1] // (4 * sources)
    slots = sources * capacity
    row_part, cot_part = width // 8, 3 * width // 16
    row_rest, cot_rest = width - 4 * row_part, width - 4 * cot_part
    ids, weight = expert_ids.T, route_weight.T

    def exchanged(rows):
        return lax.all_to_all(
            rows.reshape(sources, capacity, -1), sp_axes, 0, 0, tiled=True
        ).reshape(rows.shape)

    spread = build(
        position, ids, weight,
        [(layer_input, row_part, None, False), (out_cot, cot_part, None, True)],
        capacity, sources,
    )
    spread = exchanged(spread)
    projections = shared_ring_gather(out_proj, core)
    gate_up, down, fold_gate, fold_up = folded_weights(
        position, w_gate, w_up, w_down, out_proj, projections, row_part, cot_part
    )
    rates = (decay_factor * jax.nn.softplus(-decay_param)).reshape(-1, gate_a_w.shape[1])
    rec_output, act, b, ca, ci, cs, decay, seg, exp, block, sel = early(
        position, expert_ids, rec_input, gate_input, prev_state, rates, extra_decay.T,
        gate_a_w, gate_i_w, capacity, sources,
    )
    direct = build(
        position, ids, weight,
        [
            (layer_input, row_rest, 4 * row_part // row_rest, False),
            (out_cot, cot_rest, 4 * cot_part // cot_rest, True),
            (rec_output, rec_output.shape[1], 0, False),
        ],
        capacity, sources,
    )
    got = exchanged(direct)
    pieces = ring_gather(spread[: slots // 2], spread[slots // 2 :])
    base = jnp.dot(out_cot, out_proj, preferred_element_type=F32)
    local_proj = lax.dot_general(
        out_cot, rec_output, (((0,), (0,)), ((), ())), preferred_element_type=F32
    )
    before = ahead(pieces[:6], gate_up, down, row_part, cot_part)
    hidden, gate_cot, up_cot, mix = expert(
        got, pieces[6:], before, gate_up, down, fold_gate, fold_up, row_part, cot_part
    )
    back = lax.all_to_all(
        mix.reshape(4 * sources, capacity, -1), ("tp", *sp_axes), 0, 0, tiled=True
    ).reshape(mix.shape)
    grad_gate, grad_up, grad_down = grads(
        position, got, pieces, hidden, gate_cot, up_cot, width, row_part, cot_part
    )
    start = row_rest + cot_rest
    recs = ring_gather(got[: slots // 2, start:], got[slots // 2 :, start:])
    lines = width // sources
    parts = proj(position, gate_cot, up_cot, w_gate, w_up, local_proj, recs, lines)
    other = lax.ppermute(parts[1], "core", [(0, 1), (1, 0)])
    own, left_top, left_bottom, right_top, right_bottom, far_top, far_bottom = chip_sum(
        parts, other
    )
    through_top, through_bottom = shifted(far_top, 1), shifted(far_bottom, -1)
    from_left, from_right = shifted(right_bottom, 1), shifted(left_top, -1)
    both_top = (right_top.astype(F32) + through_top.astype(F32)).astype(BF16)
    both_bottom = (left_bottom.astype(F32) + through_bottom.astype(F32)).astype(BF16)
    last_top, last_bottom = shifted(both_top, 1), shifted(both_bottom, -1)
    arriving = (
        jnp.concatenate([last_top, last_bottom], axis=0).astype(F32)
        + jnp.concatenate([from_right, from_left], axis=0).astype(F32)
        + own.astype(F32)
    ).astype(BF16)
    arrived = lax.all_to_all(arriving, "sq", 0, 0, tiled=True)
    grad_out_proj = arrived.astype(F32).sum(axis=0)
    gate_input_grad, local, pair = scanned(
        back, sel, base, act, b, decay, seg, block, sources
    )
    pairs = lax.all_to_all(pair, sp_axes, 0, 0, tiled=True)
    rec_input_grad = final(position, pairs, local, exp, ca, ci, cs, gate_a_w, gate_i_w)
    return (grad_gate, grad_up, grad_down, grad_out_proj, rec_input_grad, gate_input_grad)


def solution(mesh):
    sp, tp = mesh.devices.shape
    inner = Mesh(mesh.devices.reshape(sp // 2, 2, tp), ("sq", "core", "tp"))
    sp = ("sq", "core")
    in_specs = (
        P(sp, None),
        P(sp, None),
        P(sp, None),
        P(sp, None),
        P(sp, None, "tp"),
        P(sp, None, "tp"),
        P(sp, "tp", None),
        P(None, "tp"),
        P(sp, "tp"),
        P(sp, "tp"),
        P(sp, "tp"),
        P(),
        P("tp", sp),
        P(),
        P(),
    )
    out_specs = (
        P(sp, None, "tp"),
        P(sp, None, "tp"),
        P(sp, "tp", None),
        P(sp, "tp"),
        P(sp, "tp"),
        P(sp, "tp"),
    )
    return jax.shard_map(
        per_device, mesh=inner, in_specs=in_specs, out_specs=out_specs, check_vma=False
    )
```

```python
import functools
import jax
import jax.numpy as jnp
from jax import lax
from jax.experimental import pallas as pl
from jax.experimental.pallas import tpu as pltpu
from jax.sharding import Mesh, PartitionSpec as P


F32 = jnp.float32
BF16 = jnp.bfloat16
gelu_scale = 0.7978845608028654
gelu_cubic = 0.044715
decay_factor = 8.0
ring_steps = (0, 3, 1, 2)


def params(limit_mib=48, **extra):
    return pltpu.CompilerParams(vmem_limit_bytes=limit_mib * 1024 * 1024, **extra)


def cost(flops, moved):
    return pl.CostEstimate(flops=flops, bytes_accessed=moved, transcendentals=0)


def whole(shape):
    return pl.BlockSpec(shape, lambda *_: (0,) * len(shape), pipeline_mode=pl.Buffered(1))


SMEM = pl.BlockSpec(memory_space=pltpu.SMEM)


def made(shape, dtype):
    return pltpu.HBM(shape, dtype)


def kept(arrays):
    return [pltpu.with_memory_space_constraint(a, pltpu.HBM) for a in arrays]


def dot(a, b, dims=((1,), (0,))):
    return lax.dot_general(a, b, (dims, ((), ())), preferred_element_type=F32)


def sigmoid(v):
    return 1.0 / (1.0 + jnp.exp(-v))


def minus_expm1(v):
    series = 1.0 + v / 8.0
    for order in range(7, 1, -1):
        series = 1.0 + v / order * series
    return jnp.where(v > -0.5, -v * series, 1.0 - jnp.exp(v))


def early_kernel(
    where_ref, ids, rec, gate_in, prev, rates, extra, map_a, map_i,
    out_rec, out_act, out_b, out_ca, out_ci, out_cs, out_decay, out_seg, out_exp, out_block, out_sel,
    *, capacity, experts,
):
    tokens, channels = rec.shape
    heads = channels // 128
    first = where_ref[0] * heads

    def block_of_tokens(i, _):
        rows = pl.ds(pl.multiple_of(i * 128, 128), 128)
        for h in range(heads):
            cols = slice(h * 128, (h + 1) * 128)
            values_bf = rec[rows, cols]
            x = values_bf.astype(F32)
            ra = sigmoid(dot(values_bf, map_a[first + h]))
            ig = sigmoid(dot(values_bf, map_i[first + h]))
            rate = rates[pl.ds(first + h, 1), :]
            log_decay = -rate * ra + extra[rows, h : h + 1]
            decay = jnp.exp(log_decay)
            scale = jnp.sqrt(minus_expm1(2.0 * log_decay))
            before = prev[rows, cols]
            state = decay * before + scale * ig * x
            g = gate_in[rows, cols].astype(F32)
            bend = jnp.tanh(gelu_scale * (g + gelu_cubic * g * g * g))
            act = 0.5 * g * (1.0 + bend)
            slope = 0.5 * (1.0 + bend) + 0.5 * g * (1.0 - bend * bend) * gelu_scale * (
                1.0 + 3.0 * gelu_cubic * g * g
            )
            out_rec[rows, cols] = (state * act).astype(BF16)
            out_act[rows, cols] = act
            out_b[rows, cols] = state * slope
            out_ca[rows, cols] = (decay * before - decay * decay / scale * ig * x) * -rate * ra * (1.0 - ra)
            out_ci[rows, cols] = scale * x * ig * (1.0 - ig)
            out_cs[rows, cols] = scale * ig
            out_decay[h, rows, :] = decay
        return 0

    lax.fori_loop(0, tokens // 128, block_of_tokens, 0)
    length = tokens // 8
    for h in range(heads):
        cols = slice(h * 128, (h + 1) * 128)
        product = jnp.ones((8, 128), F32)
        for i in range(length - 1, -1, -1):
            out_seg[h, pl.ds(i, 8, stride=length), :] = product
            product = product * out_decay[h, pl.ds(i, 8, stride=length), :]
        carry = jnp.ones((1, 128), F32)
        for k in range(7, -1, -1):
            rows = slice(k * length, (k + 1) * length)
            out_exp[rows, cols] = out_seg[h, rows, :] * carry
            carry = carry * product[k : k + 1, :]
        out_block[:, cols] = jnp.broadcast_to(carry, (8, 128))
    lane = lax.broadcasted_iota(jnp.int32, (tokens, 128), 1)
    first_id = ids[:, 0:1]
    second_id = ids[:, 1:2]
    one = (lane == first_id).astype(F32)
    two = (lane == second_id).astype(F32)
    lower = lax.broadcasted_iota(jnp.int32, (tokens, tokens), 0) > lax.broadcasted_iota(
        jnp.int32, (tokens, tokens), 1
    )
    rank = dot(lower.astype(F32).astype(BF16), (one + two).astype(BF16))
    place_one = first_id * capacity + jnp.sum(rank * one, axis=1, keepdims=True).astype(jnp.int32)
    place_two = second_id * capacity + jnp.sum(rank * two, axis=1, keepdims=True).astype(jnp.int32)
    slots = experts * capacity

    def block_of_slots(i, _):
        at = pl.multiple_of(i * 256, 256)
        slot = lax.broadcasted_iota(jnp.int32, (tokens, 256), 1) + at
        hit = (slot == place_one) | (slot == place_two)
        out_sel[:, pl.ds(at, 256)] = jnp.where(hit, 1.0, 0.0).astype(BF16)
        return 0

    lax.fori_loop(0, slots // 256, block_of_slots, 0)


def early(position, ids, rec, gate_in, prev, rates, extra, map_a, map_i, capacity, experts):
    tokens, channels = rec.shape
    wide = made((tokens, channels), F32)
    heads = made((channels // 128, tokens, 128), F32)
    outs = (
        made((tokens, channels), BF16),
        wide, wide, wide, wide, wide, heads, heads, wide,
        made((8, channels), F32),
        made((tokens, experts * capacity), BF16),
    )
    args = (position, ids, rec, gate_in, prev, rates, extra, map_a, map_i)
    return pl.pallas_call(
        functools.partial(early_kernel, capacity=capacity, experts=experts),
        out_shape=outs,
        in_specs=[SMEM] + [whole(a.shape) for a in args[1:]],
        out_specs=[whole(o.shape) for o in outs],
        compiler_params=params(14),
        cost_estimate=cost(3 * 10**9, 8 * 2**20),
        name="early",
    )(args[0], *kept(args[1:]))


def build_kernel(where_ref, ids, weight, *refs, capacity, group, weighted):
    sources, out, rank_ref, weight_ref = refs[:-3], refs[-3], refs[-2], refs[-1]
    experts, tokens = rank_ref.shape

    @pl.when(pl.program_id(0) == 0)
    def _():
        name = lax.broadcasted_iota(jnp.int32, (experts, tokens), 0)
        one = jnp.where(name == ids[0:1, :], 1.0, 0.0)
        two = jnp.where(name == ids[1:2, :], 1.0, 0.0)
        both = one + two
        upper = lax.broadcasted_iota(jnp.int32, (tokens, tokens), 0) < lax.broadcasted_iota(
            jnp.int32, (tokens, tokens), 1
        )
        rank = dot(both.astype(BF16), upper.astype(F32).astype(BF16))
        rank_ref[...] = jnp.where(both > 0.0, rank, -1.0)
        weight_ref[...] = one * weight[0:1, :] + two * weight[1:2, :]

    first = pl.program_id(0) * group
    place = lax.broadcasted_iota(jnp.int32, (capacity, tokens), 0).astype(F32)
    picks, weights = [], []
    for e in range(group):
        hit = place == rank_ref[pl.ds(first + e, 1), :]
        picks.append(jnp.where(hit, 1.0, 0.0))
        weights.append(
            jnp.sum(jnp.where(hit, weight_ref[pl.ds(first + e, 1), :], 0.0), axis=1, keepdims=True)
        )
    pick = jnp.concatenate(picks, axis=0).astype(BF16)
    by = jnp.concatenate(weights, axis=0)
    at = 0
    for source, scaled in zip(sources, weighted):
        rows = dot(pick, source[...])
        if scaled:
            rows = rows * by
        out[:, at : at + source.shape[1]] = rows.astype(BF16)
        at += source.shape[1]


def build(position, ids, weight, parts, capacity, experts, group=8):
    tokens = ids.shape[1]
    total = sum(width for _, width, _, _ in parts)
    specs = [pl.BlockSpec(ids.shape, lambda i, where: (0, 0))] * 2
    for _, width, column, _ in parts:
        specs.append(pl.BlockSpec((tokens, width), functools.partial(column_block, column)))
    return pl.pallas_call(
        functools.partial(
            build_kernel, capacity=capacity, group=group, weighted=tuple(p[3] for p in parts)
        ),
        out_shape=made((experts * capacity, total), BF16),
        grid_spec=pltpu.PrefetchScalarGridSpec(
            num_scalar_prefetch=1,
            grid=(experts // group,),
            in_specs=specs,
            out_specs=pl.BlockSpec((group * capacity, total), lambda i, where: (i, 0)),
            scratch_shapes=[pltpu.VMEM((experts, tokens), F32), pltpu.VMEM((experts, tokens), F32)],
        ),
        compiler_params=params(14),
        cost_estimate=cost(1400000 * total, 5000 * total),
    )(position, *kept([ids, weight, *(p[0] for p in parts)]))


def column_block(column, i, where):
    return (0, where[0] if column is None else column)


def weights_kernel(
    where_ref, w_gate, w_up, w_down, whole_own, *refs, row_part, cot_part,
):
    pieces = refs[:8]
    out_gate_up, out_down, out_gate, out_up = refs[8:]
    at, core = where_ref[0], where_ref[1]
    width, units = w_gate.shape
    half = width // 2
    first = ((0,), (0,))
    mine = pl.multiple_of(core * half, half)
    other = pl.multiple_of(half - core * half, half)
    for weights, out in ((w_gate, out_gate), (w_up, out_up)):
        out[at] = dot(weights[...], whole_own[...], first).astype(BF16)
        for step, n in ((3, 0), (1, 1)):
            out[lax.rem(at + step, 4)] = (
                dot(weights[pl.ds(mine, half), :], pieces[n][...], first)
                + dot(weights[pl.ds(other, half), :], pieces[4 + n][...], first)
            ).astype(BF16)
        quarter = half // 2
        out[lax.rem(at + 2, 4)] = sum(
            dot(weights[pl.ds(start + n * quarter, quarter), :], pieces[side + 2 + n][...], first)
            for start, side in ((mine, 0), (other, 4))
            for n in range(2)
        ).astype(BF16)
    rest = width - 4 * row_part
    out_gate_up[:rest, :units] = w_gate[4 * row_part :, :]
    out_gate_up[:rest, units:] = w_up[4 * row_part :, :]
    cot_rest = width - 4 * cot_part
    out_down[:cot_rest, :] = w_down[:, 4 * cot_part :].T
    for n, step in enumerate((2, 0, 3, 1)):
        group = lax.rem(at + step, 4)
        lines = pl.ds(pl.multiple_of(group * row_part, row_part), row_part)
        columns = pl.ds(pl.multiple_of(group * cot_part, 128), cot_part)
        to = slice(rest + n * row_part, rest + (n + 1) * row_part)
        out_gate_up[to, :units] = w_gate[lines, :]
        out_gate_up[to, units:] = w_up[lines, :]
        to = slice(cot_rest + n * cot_part, cot_rest + (n + 1) * cot_part)
        out_down[to, :] = w_down[:, columns].T


def folded_weights(position, w_gate, w_up, w_down, own, pieces, row_part, cot_part):
    width, units = w_gate.shape
    args = (position, w_gate, w_up, w_down, own, *pieces)
    fold = made((4, units, own.shape[1]), BF16)
    outs = (made((width, 2 * units), BF16), made((width, units), BF16), fold, fold)
    return pl.pallas_call(
        functools.partial(weights_kernel, row_part=row_part, cot_part=cot_part),
        out_shape=outs,
        in_specs=[SMEM] + [whole(a.shape) for a in args[1:]],
        out_specs=[whole(o.shape) for o in outs],
        compiler_params=params(24),
        cost_estimate=cost(4 * 10**9, 7 * 2**20),
        name="folded",
    )(position, *kept([w_gate, w_up, w_down, own]), *pieces)


def ahead_kernel(gate_up, down, *refs, row_part, row_from, cot_from):
    pieces, out = refs[:-1], refs[-1]
    half = pieces[0].shape[0]
    wide = gate_up.shape[1]
    for n in range(2):
        lines = slice(n * half, (n + 1) * half)
        rows = jnp.concatenate([p[:, :row_part] for p in pieces[n::2]], axis=1)
        cots = jnp.concatenate([p[:, row_part:] for p in pieces[n::2]], axis=1)
        out[lines, :wide] = dot(rows, gate_up[row_from:, :])
        out[lines, wide:] = dot(cots, down[cot_from:, :])


def ahead(pieces, gate_up, down, row_part, cot_part):
    width = gate_up.shape[0]
    out = made((2 * pieces[0].shape[0], gate_up.shape[1] + down.shape[1]), F32)
    args = (gate_up, down, *pieces)
    return pl.pallas_call(
        functools.partial(
            ahead_kernel,
            row_part=row_part,
            row_from=width - 3 * row_part,
            cot_from=width - 3 * cot_part,
        ),
        out_shape=out,
        in_specs=[whole(a.shape) for a in args],
        out_specs=whole(out.shape),
        compiler_params=params(20),
        cost_estimate=cost(2 * 10**9, 12 * 2**20),
        name="ahead",
    )(*kept([gate_up, down]), *pieces)


def expert_kernel(
    got_rows, got_cot, far_top, far_bottom, before, gate_up, down, fold_gate, fold_up,
    out_hidden, out_gate, out_up, out_mix, *, row_part,
):
    units = down.shape[1]
    upper = pl.program_id(0) < pl.num_programs(0) // 2
    far = jnp.where(upper, far_top[...], far_bottom[...])
    rows = jnp.concatenate([got_rows[...], far[:, :row_part]], axis=1)
    cots = jnp.concatenate([got_cot[...], far[:, row_part:]], axis=1)
    both = dot(rows, gate_up[...]) + before[:, : 2 * units]
    gate_pre, up_pre = both[:, :units], both[:, units:]
    hidden_cot = dot(cots, down[...]) + before[:, 2 * units :]
    sigma = sigmoid(gate_pre)
    swish = gate_pre * sigma
    out_hidden[...] = (swish * up_pre).astype(BF16)
    gate_cot = (hidden_cot * up_pre * sigma * (1.0 + gate_pre * (1.0 - sigma))).astype(BF16)
    up_cot = (hidden_cot * swish).astype(BF16)
    out_gate[...] = gate_cot
    out_up[...] = up_cot
    for c in range(4):
        out_mix[c] = (dot(gate_cot, fold_gate[c]) + dot(up_cot, fold_up[c])).astype(BF16)


def first_rows(array, count):
    return pl.BlockSpec(
        (count, array.shape[1]), lambda i: (0, 0), pipeline_mode=pl.Buffered(1)
    )


def expert(got, far, before, gate_up, down, fold_gate, fold_up, row_part, cot_part, steps=4):
    rows = got.shape[0]
    width, hidden = down.shape
    block = rows // steps
    part = fold_gate.shape[2]
    half = steps // 2
    row_rest, cot_rest = width - 4 * row_part, width - 4 * cot_part
    narrow = made((rows, hidden), BF16)
    mine = pl.BlockSpec((block, hidden), lambda i: (i, 0))
    return pl.pallas_call(
        functools.partial(expert_kernel, row_part=row_part),
        out_shape=(narrow, narrow, narrow, made((4, rows, part), BF16)),
        grid=(steps,),
        in_specs=[
            pl.BlockSpec((block, row_rest), lambda i: (i, 0)),
            pl.BlockSpec((block, cot_rest), lambda i: (i, row_rest // cot_rest)),
            pl.BlockSpec((block, row_part + cot_part), lambda i: (jnp.minimum(i, half - 1), 0)),
            pl.BlockSpec((block, row_part + cot_part), lambda i: (jnp.maximum(i - half, 0), 0)),
            pl.BlockSpec((block, before.shape[1]), lambda i: (i, 0)),
            first_rows(gate_up, row_rest + row_part),
            first_rows(down, cot_rest + cot_part),
            whole(fold_gate.shape),
            whole(fold_up.shape),
        ],
        out_specs=[mine, mine, mine, pl.BlockSpec((4, block, part), lambda i: (0, i, 0))],
        compiler_params=params(26),
        cost_estimate=cost(5 * 10**9, 16 * 2**20),
        name="expert",
    )(*kept([got, got]), *far, *kept([before, gate_up, down, fold_gate, fold_up]))


def grads_kernel(where_ref, got_rows, got_cot, *refs, row_part, cot_part):
    pieces = refs[:8]
    hidden, gate_cot, up_cot, out_gate, out_up, out_down = refs[8:]
    at = where_ref[0]
    first = ((0,), (0,))
    rows = got_rows[...]
    out_gate[0, 4 * row_part :, :] = dot(rows, gate_cot[...], first)
    out_up[0, 4 * row_part :, :] = dot(rows, up_cot[...], first)
    out_down[0, :, 4 * cot_part :] = dot(hidden[...], got_cot[...], first)
    for n, step in enumerate(ring_steps):
        group = lax.rem(at + step, 4)
        top, bottom = pieces[2 * n], pieces[2 * n + 1]
        half = top.shape[0]
        lines = pl.ds(pl.multiple_of(group * row_part, row_part), row_part)
        columns = pl.ds(pl.multiple_of(group * cot_part, 128), cot_part)
        for cot, out in ((gate_cot, out_gate), (up_cot, out_up)):
            out[0, lines, :] = dot(top[:, :row_part], cot[:half, :], first) + dot(
                bottom[:, :row_part], cot[half:, :], first
            )
        out_down[0, :, columns] = dot(hidden[:half, :], top[:, row_part:], first) + dot(
            hidden[half:, :], bottom[:, row_part:], first
        )


def grads(position, got, pieces, hidden, gate_cot, up_cot, width, row_part, cot_part):
    rows, units = hidden.shape
    row_rest, cot_rest = width - 4 * row_part, width - 4 * cot_part
    outs = (
        made((1, width, units), F32),
        made((1, width, units), F32),
        made((1, units, width), F32),
    )
    tail = (*pieces, hidden, gate_cot, up_cot)
    return pl.pallas_call(
        functools.partial(grads_kernel, row_part=row_part, cot_part=cot_part),
        out_shape=outs,
        grid=(1,),
        in_specs=[
            SMEM,
            pl.BlockSpec((rows, row_rest), lambda i: (0, 0), pipeline_mode=pl.Buffered(1)),
            pl.BlockSpec(
                (rows, cot_rest), lambda i: (0, row_rest // cot_rest), pipeline_mode=pl.Buffered(1)
            ),
            *(whole(a.shape) for a in tail),
        ],
        out_specs=[whole(o.shape) for o in outs],
        compiler_params=params(30),
        cost_estimate=cost(4 * 10**9, 17 * 2**20),
        name="grads",
    )(position, *kept([got, got, *tail]))


def proj_kernel(where_ref, gate_cot, up_cot, w_gate, w_up, local, *refs):
    pieces, out = refs[:-1], refs[-1]
    core = where_ref[1]
    first = ((0,), (0,))
    for n, step in enumerate(ring_steps):
        top, bottom = pieces[2 * n], pieces[2 * n + 1]
        half = top.shape[0]
        push_gate, push_up = (
            (dot(cot[:half, :], top[...], first) + dot(cot[half:, :], bottom[...], first)).astype(BF16)
            for cot in (gate_cot, up_cot)
        )
        term = dot(w_gate[...], push_gate) + dot(w_up[...], push_up)
        if step == 0:
            term = term + local[...]
        term = term.astype(BF16)
        lines = out.shape[3]
        for s in range(2 * out.shape[2]):
            slot = lax.rem(s % 2 + core, 2)
            out[slot, n, s // 2] = term[s * lines : (s + 1) * lines, :]


def proj(position, gate_cot, up_cot, w_gate, w_up, local, pieces, lines):
    width, part = w_gate.shape[0], pieces[0].shape[1]
    args = (position, gate_cot, up_cot, w_gate, w_up, local, *pieces)
    out = made((2, 4, width // lines // 2, lines, part), BF16)
    return pl.pallas_call(
        proj_kernel,
        out_shape=out,
        in_specs=[SMEM] + [whole(a.shape) for a in args[1:]],
        out_specs=whole(out.shape),
        compiler_params=params(22),
        cost_estimate=cost(4 * 10**9, 14 * 2**20),
        name="proj",
    )(position, *kept(args[1:6]), *pieces)


def chip_kernel(kept_ref, other, out_own, *outs):
    half = out_own.shape[0] // 2
    out_own[...] = (kept_ref[0, 0].astype(F32) + other[0].astype(F32)).astype(BF16)
    for n in range(6):
        lines = slice((n % 2) * half, (n % 2 + 1) * half)
        at = 1 + n // 2
        outs[n][...] = (
            kept_ref[0, at, lines].astype(F32) + other[at, lines].astype(F32)
        ).astype(BF16)


def chip_sum(parts, other):
    groups, lines, width = other.shape[1:]
    half = made((groups // 2, lines, width), BF16)
    outs = (made((groups, lines, width), BF16),) + (half,) * 6
    return pl.pallas_call(
        chip_kernel,
        out_shape=outs,
        grid=(1,),
        in_specs=[
            pl.BlockSpec(
                (1, *parts.shape[1:]), lambda i: (0, 0, 0, 0, 0), pipeline_mode=pl.Buffered(1)
            ),
            whole(other.shape),
        ],
        out_specs=[whole(o.shape) for o in outs],
        compiler_params=params(16),
        cost_estimate=cost(10**7, 6 * 2**20),
        name="chipsum",
    )(*kept([parts]), other)


def pair_sum_kernel(one, two, three, four, out_top, out_bottom):
    out_top[...] = (one[...].astype(F32) + two[...].astype(F32)).astype(BF16)
    out_bottom[...] = (three[...].astype(F32) + four[...].astype(F32)).astype(BF16)


def pair_sum(*args):
    out = made(args[0].shape, BF16)
    return pl.pallas_call(
        pair_sum_kernel,
        out_shape=(out, out),
        in_specs=[whole(a.shape) for a in args],
        out_specs=[whole(out.shape)] * 2,
        compiler_params=params(6),
        cost_estimate=cost(10**6, 2**20),
        name="pairsum",
    )(*args)


def arrive_kernel(own, last_top, last_bottom, from_right, from_left, out):
    half = last_top.shape[0]
    for at, far, near in ((0, last_top, from_right), (half, last_bottom, from_left)):
        lines = slice(at, at + half)
        out[lines] = (
            own[lines].astype(F32) + far[...].astype(F32) + near[...].astype(F32)
        ).astype(BF16)


def arrive(*args):
    out = made(args[0].shape, BF16)
    return pl.pallas_call(
        arrive_kernel,
        out_shape=out,
        in_specs=[whole(a.shape) for a in args],
        out_specs=whole(out.shape),
        compiler_params=params(6),
        cost_estimate=cost(10**6, 2**20),
        name="arrive",
    )(*args)


def scan_kernel(back, sel, base, act, b, decay, seg, block, out_grad, out_local, out_pair, drive, part):
    tokens, channels = base.shape
    length = tokens // 8
    mix = base[...]
    total = back[0].astype(F32) + back[1].astype(F32) + back[2].astype(F32) + back[3].astype(F32)
    mix = mix + dot(sel[...], total.astype(BF16))
    out_grad[...] = (mix * b[...]).astype(BF16)
    push = mix * act[...]
    heads = channels // 128
    for h in range(heads):
        drive[h] = push[:, h * 128 : (h + 1) * 128]
    last = pl.ds(length - 1, 8, stride=length)
    values = [drive[h, last, :] for h in range(heads)]
    for h in range(heads):
        part[h, last, :] = values[h]
    for i in range(length - 2, -1, -1):
        here, after = pl.ds(i, 8, stride=length), pl.ds(i + 1, 8, stride=length)
        for h in range(heads):
            values[h] = drive[h, here, :] + decay[h, after, :] * values[h]
            part[h, here, :] = values[h]
    for h in range(heads):
        cols = slice(h * 128, (h + 1) * 128)
        value = values[h]
        lead = decay[h, pl.ds(0, 8, stride=length), :]
        inner = seg[h, pl.ds(0, 8, stride=length), :]
        carry = jnp.zeros((1, 128), F32)
        for k in range(7, -1, -1):
            rows = slice(k * length, (k + 1) * length)
            out_local[rows, cols] = part[h, rows, :] + seg[h, rows, :] * carry
            one = slice(k, k + 1)
            carry = lead[one, :] * (value[one, :] + inner[one, :] * carry)
        pair = jnp.concatenate([carry, block[0:1, cols]], axis=0)
        out_pair[:, :, cols] = jnp.broadcast_to(pair[None], (out_pair.shape[0], *pair.shape))


def scanned(back, sel, base, act, b, decay, seg, block, sources):
    tokens, channels = base.shape
    args = (back, sel, base, act, b, decay, seg, block)
    outs = (
        made((tokens, channels), BF16),
        made((tokens, channels), F32),
        made((sources, 2, channels), F32),
    )
    return pl.pallas_call(
        scan_kernel,
        out_shape=outs,
        in_specs=[whole(a.shape) for a in args],
        out_specs=[whole(o.shape) for o in outs],
        scratch_shapes=[pltpu.VMEM(decay.shape, F32), pltpu.VMEM(decay.shape, F32)],
        compiler_params=params(14),
        cost_estimate=cost(4 * 10**8, 8 * 2**20),
        name="scanned",
    )(back, *kept(args[1:]))


def final_kernel(where_ref, pairs, local, exp, ca, ci, cs, map_a, map_i, out):
    channels = local.shape[1]
    heads = channels // 128
    first = where_ref[0] * heads
    total = jnp.zeros((1, channels), F32)
    me = where_ref[2]
    for s in range(pairs.shape[0] - 1, 0, -1):
        total = jnp.where(me < s, pairs[s, 0:1, :] + pairs[s, 1:2, :] * total, total)
    for h in range(heads):
        cols = slice(h * 128, (h + 1) * 128)
        cot = local[:, cols] + exp[:, cols] * total[:, cols]
        a_cot = (cot * ca[:, cols]).astype(BF16)
        i_cot = (cot * ci[:, cols]).astype(BF16)
        result = (
            cot * cs[:, cols]
            + dot(a_cot, map_a[first + h], ((1,), (1,)))
            + dot(i_cot, map_i[first + h], ((1,), (1,)))
        )
        out[:, cols] = result.astype(BF16)


def final(position, pairs, local, exp, ca, ci, cs, map_a, map_i):
    args = (position, pairs, local, exp, ca, ci, cs, map_a, map_i)
    return pl.pallas_call(
        final_kernel,
        out_shape=made(local.shape, BF16),
        in_specs=[SMEM] + [whole(a.shape) for a in args[1:]],
        out_specs=whole(local.shape),
        compiler_params=params(8),
        cost_estimate=cost(10**8, 4 * 2**20),
        name="final",
    )(position, pairs, *kept(args[2:]))


def shifted(piece, by):
    return lax.ppermute(piece, "tp", [(i, (i + by) % 4) for i in range(4)])


def ring_gather(top, bottom):
    left_top, right_bottom = shifted(top, 1), shifted(bottom, -1)
    left_bottom, right_top = shifted(bottom, 1), shifted(top, -1)
    far_top, far_bottom = shifted(left_top, 1), shifted(right_bottom, -1)
    return top, bottom, left_top, left_bottom, right_top, right_bottom, far_top, far_bottom


def shared_ring_gather(own, core):
    half = own.shape[0] // 2
    mine = lax.dynamic_slice_in_dim(own, core * half, half, 0)
    left, right = shifted(mine, 1), shifted(mine, -1)
    quarter = half // 2
    far_top, far_bottom = shifted(left[:quarter], 1), shifted(right[quarter:], -1)
    pieces = (left, right, far_top, far_bottom)
    others = tuple(lax.ppermute(p, "core", [(0, 1), (1, 0)]) for p in pieces)
    return pieces + others


def per_device(
    layer_input, out_cot, expert_ids, route_weight, w_gate, w_up, w_down, out_proj,
    rec_input, gate_input, prev_state, decay_param, extra_decay, gate_a_w, gate_i_w,
):
    sources = lax.axis_size("sq") * lax.axis_size("core")
    tp = lax.axis_index("tp")
    core = lax.axis_index("core")
    sp_axes = ("sq", "core")
    sp = lax.axis_index("sq") * 2 + core
    position = jnp.stack([tp, core, sp]).astype(jnp.int32)
    w_gate, w_up, w_down = w_gate[0], w_up[0], w_down[0]
    tokens, width = layer_input.shape
    capacity = 5 * tokens * expert_ids.shape[1] // (4 * sources)
    slots = sources * capacity
    row_part, cot_part = width // 8, 3 * width // 16
    row_rest, cot_rest = width - 4 * row_part, width - 4 * cot_part
    ids, weight = expert_ids.T, route_weight.T

    def exchanged(rows):
        return lax.all_to_all(
            rows.reshape(sources, capacity, -1), sp_axes, 0, 0, tiled=True
        ).reshape(rows.shape)

    spread = build(
        position, ids, weight,
        [(layer_input, row_part, None, False), (out_cot, cot_part, None, True)],
        capacity, sources,
    )
    spread = exchanged(spread)
    projections = shared_ring_gather(out_proj, core)
    gate_up, down, fold_gate, fold_up = folded_weights(
        position, w_gate, w_up, w_down, out_proj, projections, row_part, cot_part
    )
    rates = (decay_factor * jax.nn.softplus(-decay_param)).reshape(-1, gate_a_w.shape[1])
    rec_output, act, b, ca, ci, cs, decay, seg, exp, block, sel = early(
        position, expert_ids, rec_input, gate_input, prev_state, rates, extra_decay.T,
        gate_a_w, gate_i_w, capacity, sources,
    )
    direct = build(
        position, ids, weight,
        [
            (layer_input, row_rest, 4 * row_part // row_rest, False),
            (out_cot, cot_rest, 4 * cot_part // cot_rest, True),
            (rec_output, rec_output.shape[1], 0, False),
        ],
        capacity, sources,
    )
    got = exchanged(direct)
    pieces = ring_gather(spread[: slots // 2], spread[slots // 2 :])
    base = jnp.dot(out_cot, out_proj, preferred_element_type=F32)
    local_proj = lax.dot_general(
        out_cot, rec_output, (((0,), (0,)), ((), ())), preferred_element_type=F32
    )
    before = ahead(pieces[:6], gate_up, down, row_part, cot_part)
    hidden, gate_cot, up_cot, mix = expert(
        got, pieces[6:], before, gate_up, down, fold_gate, fold_up, row_part, cot_part
    )
    back = lax.all_to_all(
        mix.reshape(4 * sources, capacity, -1), ("tp", *sp_axes), 0, 0, tiled=True
    ).reshape(mix.shape)
    grad_gate, grad_up, grad_down = grads(
        position, got, pieces, hidden, gate_cot, up_cot, width, row_part, cot_part
    )
    start = row_rest + cot_rest
    recs = ring_gather(got[: slots // 2, start:], got[slots // 2 :, start:])
    lines = width // sources
    parts = proj(position, gate_cot, up_cot, w_gate, w_up, local_proj, recs, lines)
    other = lax.ppermute(parts[1], "core", [(0, 1), (1, 0)])
    own, left_top, left_bottom, right_top, right_bottom, far_top, far_bottom = chip_sum(
        parts, other
    )
    through_top, through_bottom = shifted(far_top, 1), shifted(far_bottom, -1)
    from_left, from_right = shifted(right_bottom, 1), shifted(left_top, -1)
    both_top, both_bottom = pair_sum(right_top, through_top, left_bottom, through_bottom)
    last_top, last_bottom = shifted(both_top, 1), shifted(both_bottom, -1)
    arriving = arrive(own, last_top, last_bottom, from_right, from_left)
    arrived = lax.all_to_all(arriving, "sq", 0, 0, tiled=True)
    grad_out_proj = arrived.astype(F32).sum(axis=0)
    gate_input_grad, local, pair = scanned(
        back, sel, base, act, b, decay, seg, block, sources
    )
    pairs = lax.all_to_all(pair, sp_axes, 0, 0, tiled=True)
    rec_input_grad = final(position, pairs, local, exp, ca, ci, cs, gate_a_w, gate_i_w)
    return (grad_gate, grad_up, grad_down, grad_out_proj, rec_input_grad, gate_input_grad)


def solution(mesh):
    sp, tp = mesh.devices.shape
    inner = Mesh(mesh.devices.reshape(sp // 2, 2, tp), ("sq", "core", "tp"))
    sp = ("sq", "core")
    in_specs = (
        P(sp, None),
        P(sp, None),
        P(sp, None),
        P(sp, None),
        P(sp, None, "tp"),
        P(sp, None, "tp"),
        P(sp, "tp", None),
        P(None, "tp"),
        P(sp, "tp"),
        P(sp, "tp"),
        P(sp, "tp"),
        P(),
        P("tp", sp),
        P(),
        P(),
    )
    out_specs = (
        P(sp, None, "tp"),
        P(sp, None, "tp"),
        P(sp, "tp", None),
        P(sp, "tp"),
        P(sp, "tp"),
        P(sp, "tp"),
    )
    return jax.shard_map(
        per_device, mesh=inner, in_specs=in_specs, out_specs=out_specs, check_vma=False
    )
```

```python
import functools
import jax
import jax.numpy as jnp
from jax import lax
from jax.experimental import pallas as pl
from jax.experimental.pallas import tpu as pltpu
from jax.sharding import Mesh, PartitionSpec as P


F32 = jnp.float32
BF16 = jnp.bfloat16
gelu_scale = 0.7978845608028654
gelu_cubic = 0.044715
decay_factor = 8.0
ring_steps = (0, 3, 1, 2)


def params(limit_mib=48, **extra):
    return pltpu.CompilerParams(vmem_limit_bytes=limit_mib * 1024 * 1024, **extra)


def cost(flops, moved):
    return pl.CostEstimate(flops=flops, bytes_accessed=moved, transcendentals=0)


def whole(shape):
    return pl.BlockSpec(shape, lambda *_: (0,) * len(shape), pipeline_mode=pl.Buffered(1))


SMEM = pl.BlockSpec(memory_space=pltpu.SMEM)


def made(shape, dtype):
    return pltpu.HBM(shape, dtype)


def kept(arrays):
    return [pltpu.with_memory_space_constraint(a, pltpu.HBM) for a in arrays]


def dot(a, b, dims=((1,), (0,))):
    return lax.dot_general(a, b, (dims, ((), ())), preferred_element_type=F32)


def sigmoid(v):
    return 1.0 / (1.0 + jnp.exp(-v))


def minus_expm1(v):
    series = 1.0 + v / 8.0
    for order in range(7, 1, -1):
        series = 1.0 + v / order * series
    return jnp.where(v > -0.5, -v * series, 1.0 - jnp.exp(v))


def early_kernel(
    where_ref, ids, rec, gate_in, prev, rates, extra, map_a, map_i,
    out_rec, out_act, out_b, out_ca, out_ci, out_cs, out_decay, out_seg, out_exp, out_block, out_sel,
    *, capacity, experts,
):
    tokens, channels = rec.shape
    heads = channels // 128
    first = where_ref[0] * heads

    def block_of_tokens(i, _):
        rows = pl.ds(pl.multiple_of(i * 128, 128), 128)
        for h in range(heads):
            cols = slice(h * 128, (h + 1) * 128)
            values_bf = rec[rows, cols]
            x = values_bf.astype(F32)
            ra = sigmoid(dot(values_bf, map_a[first + h]))
            ig = sigmoid(dot(values_bf, map_i[first + h]))
            rate = rates[pl.ds(first + h, 1), :]
            log_decay = -rate * ra + extra[rows, h : h + 1]
            decay = jnp.exp(log_decay)
            scale = jnp.sqrt(minus_expm1(2.0 * log_decay))
            before = prev[rows, cols]
            state = decay * before + scale * ig * x
            g = gate_in[rows, cols].astype(F32)
            bend = jnp.tanh(gelu_scale * (g + gelu_cubic * g * g * g))
            act = 0.5 * g * (1.0 + bend)
            slope = 0.5 * (1.0 + bend) + 0.5 * g * (1.0 - bend * bend) * gelu_scale * (
                1.0 + 3.0 * gelu_cubic * g * g
            )
            out_rec[rows, cols] = (state * act).astype(BF16)
            out_act[rows, cols] = act
            out_b[rows, cols] = state * slope
            out_ca[rows, cols] = (decay * before - decay * decay / scale * ig * x) * -rate * ra * (1.0 - ra)
            out_ci[rows, cols] = scale * x * ig * (1.0 - ig)
            out_cs[rows, cols] = scale * ig
            out_decay[h, rows, :] = decay
        return 0

    lax.fori_loop(0, tokens // 128, block_of_tokens, 0)
    length = tokens // 8
    for h in range(heads):
        cols = slice(h * 128, (h + 1) * 128)
        product = jnp.ones((8, 128), F32)
        for i in range(length - 1, -1, -1):
            out_seg[h, pl.ds(i, 8, stride=length), :] = product
            product = product * out_decay[h, pl.ds(i, 8, stride=length), :]
        carry = jnp.ones((1, 128), F32)
        for k in range(7, -1, -1):
            rows = slice(k * length, (k + 1) * length)
            out_exp[rows, cols] = out_seg[h, rows, :] * carry
            carry = carry * product[k : k + 1, :]
        out_block[:, cols] = jnp.broadcast_to(carry, (8, 128))
    lane = lax.broadcasted_iota(jnp.int32, (tokens, 128), 1)
    first_id = ids[:, 0:1]
    second_id = ids[:, 1:2]
    one = (lane == first_id).astype(F32)
    two = (lane == second_id).astype(F32)
    lower = lax.broadcasted_iota(jnp.int32, (tokens, tokens), 0) > lax.broadcasted_iota(
        jnp.int32, (tokens, tokens), 1
    )
    rank = dot(lower.astype(F32).astype(BF16), (one + two).astype(BF16))
    place_one = first_id * capacity + jnp.sum(rank * one, axis=1, keepdims=True).astype(jnp.int32)
    place_two = second_id * capacity + jnp.sum(rank * two, axis=1, keepdims=True).astype(jnp.int32)
    slots = experts * capacity

    def block_of_slots(i, _):
        at = pl.multiple_of(i * 256, 256)
        slot = lax.broadcasted_iota(jnp.int32, (tokens, 256), 1) + at
        hit = (slot == place_one) | (slot == place_two)
        out_sel[:, pl.ds(at, 256)] = jnp.where(hit, 1.0, 0.0).astype(BF16)
        return 0

    lax.fori_loop(0, slots // 256, block_of_slots, 0)


def early(position, ids, rec, gate_in, prev, rates, extra, map_a, map_i, capacity, experts):
    tokens, channels = rec.shape
    wide = made((tokens, channels), F32)
    heads = made((channels // 128, tokens, 128), F32)
    outs = (
        made((tokens, channels), BF16),
        wide, wide, wide, wide, wide, heads, heads, wide,
        made((8, channels), F32),
        made((tokens, experts * capacity), BF16),
    )
    args = (position, ids, rec, gate_in, prev, rates, extra, map_a, map_i)
    return pl.pallas_call(
        functools.partial(early_kernel, capacity=capacity, experts=experts),
        out_shape=outs,
        in_specs=[SMEM] + [whole(a.shape) for a in args[1:]],
        out_specs=[whole(o.shape) for o in outs],
        compiler_params=params(14),
        cost_estimate=cost(3 * 10**9, 8 * 2**20),
        name="early",
    )(args[0], *kept(args[1:]))


def build_kernel(where_ref, ids, weight, *refs, capacity, group, weighted):
    sources, out, rank_ref, weight_ref = refs[:-3], refs[-3], refs[-2], refs[-1]
    experts, tokens = rank_ref.shape

    @pl.when(pl.program_id(0) == 0)
    def _():
        name = lax.broadcasted_iota(jnp.int32, (experts, tokens), 0)
        one = jnp.where(name == ids[0:1, :], 1.0, 0.0)
        two = jnp.where(name == ids[1:2, :], 1.0, 0.0)
        both = one + two
        upper = lax.broadcasted_iota(jnp.int32, (tokens, tokens), 0) < lax.broadcasted_iota(
            jnp.int32, (tokens, tokens), 1
        )
        rank = dot(both.astype(BF16), upper.astype(F32).astype(BF16))
        rank_ref[...] = jnp.where(both > 0.0, rank, -1.0)
        weight_ref[...] = one * weight[0:1, :] + two * weight[1:2, :]

    first = pl.program_id(0) * group
    place = lax.broadcasted_iota(jnp.int32, (capacity, tokens), 0).astype(F32)
    picks, weights = [], []
    for e in range(group):
        hit = place == rank_ref[pl.ds(first + e, 1), :]
        picks.append(jnp.where(hit, 1.0, 0.0))
        weights.append(
            jnp.sum(jnp.where(hit, weight_ref[pl.ds(first + e, 1), :], 0.0), axis=1, keepdims=True)
        )
    pick = jnp.concatenate(picks, axis=0).astype(BF16)
    by = jnp.concatenate(weights, axis=0)
    at = 0
    for source, scaled in zip(sources, weighted):
        rows = dot(pick, source[...])
        if scaled:
            rows = rows * by
        out[:, at : at + source.shape[1]] = rows.astype(BF16)
        at += source.shape[1]


def build(position, ids, weight, parts, capacity, experts, group=8):
    tokens = ids.shape[1]
    total = sum(width for _, width, _, _ in parts)
    specs = [pl.BlockSpec(ids.shape, lambda i, where: (0, 0))] * 2
    for _, width, column, _ in parts:
        specs.append(pl.BlockSpec((tokens, width), functools.partial(column_block, column)))
    return pl.pallas_call(
        functools.partial(
            build_kernel, capacity=capacity, group=group, weighted=tuple(p[3] for p in parts)
        ),
        out_shape=made((experts * capacity, total), BF16),
        grid_spec=pltpu.PrefetchScalarGridSpec(
            num_scalar_prefetch=1,
            grid=(experts // group,),
            in_specs=specs,
            out_specs=pl.BlockSpec((group * capacity, total), lambda i, where: (i, 0)),
            scratch_shapes=[pltpu.VMEM((experts, tokens), F32), pltpu.VMEM((experts, tokens), F32)],
        ),
        compiler_params=params(14),
        cost_estimate=cost(1400000 * total, 5000 * total),
    )(position, *kept([ids, weight, *(p[0] for p in parts)]))


def column_block(column, i, where):
    return (0, where[0] if column is None else column)


def weights_kernel(
    where_ref, w_gate, w_up, w_down, whole_own, *refs, row_part, cot_part,
):
    pieces = refs[:8]
    out_gate_up, out_down, out_gate, out_up = refs[8:]
    at, core = where_ref[0], where_ref[1]
    width, units = w_gate.shape
    half = width // 2
    first = ((0,), (0,))
    mine = pl.multiple_of(core * half, half)
    other = pl.multiple_of(half - core * half, half)
    for weights, out in ((w_gate, out_gate), (w_up, out_up)):
        out[at] = dot(weights[...], whole_own[...], first).astype(BF16)
        for step, n in ((3, 0), (1, 1)):
            out[lax.rem(at + step, 4)] = (
                dot(weights[pl.ds(mine, half), :], pieces[n][...], first)
                + dot(weights[pl.ds(other, half), :], pieces[4 + n][...], first)
            ).astype(BF16)
        quarter = half // 2
        out[lax.rem(at + 2, 4)] = sum(
            dot(weights[pl.ds(start + n * quarter, quarter), :], pieces[side + 2 + n][...], first)
            for start, side in ((mine, 0), (other, 4))
            for n in range(2)
        ).astype(BF16)
    rest = width - 4 * row_part
    out_gate_up[:rest, :units] = w_gate[4 * row_part :, :]
    out_gate_up[:rest, units:] = w_up[4 * row_part :, :]
    cot_rest = width - 4 * cot_part
    out_down[:cot_rest, :] = w_down[:, 4 * cot_part :].T
    for n, step in enumerate((2, 0, 3, 1)):
        group = lax.rem(at + step, 4)
        lines = pl.ds(pl.multiple_of(group * row_part, row_part), row_part)
        columns = pl.ds(pl.multiple_of(group * cot_part, 128), cot_part)
        to = slice(rest + n * row_part, rest + (n + 1) * row_part)
        out_gate_up[to, :units] = w_gate[lines, :]
        out_gate_up[to, units:] = w_up[lines, :]
        to = slice(cot_rest + n * cot_part, cot_rest + (n + 1) * cot_part)
        out_down[to, :] = w_down[:, columns].T


def folded_weights(position, w_gate, w_up, w_down, own, pieces, row_part, cot_part):
    width, units = w_gate.shape
    args = (position, w_gate, w_up, w_down, own, *pieces)
    fold = made((4, units, own.shape[1]), BF16)
    outs = (made((width, 2 * units), BF16), made((width, units), BF16), fold, fold)
    return pl.pallas_call(
        functools.partial(weights_kernel, row_part=row_part, cot_part=cot_part),
        out_shape=outs,
        in_specs=[SMEM] + [whole(a.shape) for a in args[1:]],
        out_specs=[whole(o.shape) for o in outs],
        compiler_params=params(24),
        cost_estimate=cost(4 * 10**9, 7 * 2**20),
        name="folded",
    )(position, *kept([w_gate, w_up, w_down, own]), *pieces)


def ahead_kernel(gate_up, down, *refs, row_part, row_from, cot_from):
    pieces, out = refs[:-1], refs[-1]
    half = pieces[0].shape[0]
    wide = gate_up.shape[1]
    for n in range(2):
        lines = slice(n * half, (n + 1) * half)
        rows = jnp.concatenate([p[:, :row_part] for p in pieces[n::2]], axis=1)
        cots = jnp.concatenate([p[:, row_part:] for p in pieces[n::2]], axis=1)
        out[lines, :wide] = dot(rows, gate_up[row_from:, :])
        out[lines, wide:] = dot(cots, down[cot_from:, :])


def ahead(pieces, gate_up, down, row_part, cot_part):
    width = gate_up.shape[0]
    out = made((2 * pieces[0].shape[0], gate_up.shape[1] + down.shape[1]), F32)
    args = (gate_up, down, *pieces)
    return pl.pallas_call(
        functools.partial(
            ahead_kernel,
            row_part=row_part,
            row_from=width - 3 * row_part,
            cot_from=width - 3 * cot_part,
        ),
        out_shape=out,
        in_specs=[whole(a.shape) for a in args],
        out_specs=whole(out.shape),
        compiler_params=params(20),
        cost_estimate=cost(2 * 10**9, 12 * 2**20),
        name="ahead",
    )(*kept([gate_up, down]), *pieces)


def expert_kernel(
    got_rows, got_cot, far_top, far_bottom, before, gate_up, down, fold_gate, fold_up,
    out_hidden, out_gate, out_up, out_mix, *, row_part,
):
    units = down.shape[1]
    upper = pl.program_id(0) < pl.num_programs(0) // 2
    far = jnp.where(upper, far_top[...], far_bottom[...])
    rows = jnp.concatenate([got_rows[...], far[:, :row_part]], axis=1)
    cots = jnp.concatenate([got_cot[...], far[:, row_part:]], axis=1)
    both = dot(rows, gate_up[...]) + before[:, : 2 * units]
    gate_pre, up_pre = both[:, :units], both[:, units:]
    hidden_cot = dot(cots, down[...]) + before[:, 2 * units :]
    sigma = sigmoid(gate_pre)
    swish = gate_pre * sigma
    out_hidden[...] = (swish * up_pre).astype(BF16)
    gate_cot = (hidden_cot * up_pre * sigma * (1.0 + gate_pre * (1.0 - sigma))).astype(BF16)
    up_cot = (hidden_cot * swish).astype(BF16)
    out_gate[...] = gate_cot
    out_up[...] = up_cot
    for c in range(4):
        out_mix[c] = (dot(gate_cot, fold_gate[c]) + dot(up_cot, fold_up[c])).astype(BF16)


def first_rows(array, count):
    return pl.BlockSpec(
        (count, array.shape[1]), lambda i: (0, 0), pipeline_mode=pl.Buffered(1)
    )


def expert(got, far, before, gate_up, down, fold_gate, fold_up, row_part, cot_part, steps=4):
    rows = got.shape[0]
    width, hidden = down.shape
    block = rows // steps
    part = fold_gate.shape[2]
    half = steps // 2
    row_rest, cot_rest = width - 4 * row_part, width - 4 * cot_part
    narrow = made((rows, hidden), BF16)
    mine = pl.BlockSpec((block, hidden), lambda i: (i, 0))
    return pl.pallas_call(
        functools.partial(expert_kernel, row_part=row_part),
        out_shape=(narrow, narrow, narrow, made((4, rows, part), BF16)),
        grid=(steps,),
        in_specs=[
            pl.BlockSpec((block, row_rest), lambda i: (i, 0)),
            pl.BlockSpec((block, cot_rest), lambda i: (i, row_rest // cot_rest)),
            pl.BlockSpec((block, row_part + cot_part), lambda i: (jnp.minimum(i, half - 1), 0)),
            pl.BlockSpec((block, row_part + cot_part), lambda i: (jnp.maximum(i - half, 0), 0)),
            pl.BlockSpec((block, before.shape[1]), lambda i: (i, 0)),
            first_rows(gate_up, row_rest + row_part),
            first_rows(down, cot_rest + cot_part),
            whole(fold_gate.shape),
            whole(fold_up.shape),
        ],
        out_specs=[mine, mine, mine, pl.BlockSpec((4, block, part), lambda i: (0, i, 0))],
        compiler_params=params(26),
        cost_estimate=cost(5 * 10**9, 16 * 2**20),
        name="expert",
    )(*kept([got, got]), *far, *kept([before, gate_up, down, fold_gate, fold_up]))


def row_grads_kernel(where_ref, got_rows, *refs, row_part):
    pieces = refs[:8]
    gate_cot, up_cot, out_gate, out_up = refs[8:]
    at = where_ref[0]
    first = ((0,), (0,))
    rows = got_rows[...]
    out_gate[0, 4 * row_part :, :] = dot(rows, gate_cot[...], first)
    out_up[0, 4 * row_part :, :] = dot(rows, up_cot[...], first)
    for n, step in enumerate(ring_steps):
        group = lax.rem(at + step, 4)
        top, bottom = pieces[2 * n], pieces[2 * n + 1]
        half = top.shape[0]
        lines = pl.ds(pl.multiple_of(group * row_part, row_part), row_part)
        for cot, out in ((gate_cot, out_gate), (up_cot, out_up)):
            out[0, lines, :] = dot(top[...], cot[:half, :], first) + dot(
                bottom[...], cot[half:, :], first
            )


def down_grads_kernel(where_ref, got_cot, *refs, row_part, cot_part):
    pieces = refs[:8]
    hidden, out_down = refs[8:]
    at = where_ref[0]
    first = ((0,), (0,))
    out_down[0, :, 4 * cot_part :] = dot(hidden[...], got_cot[...], first)
    for n, step in enumerate(ring_steps):
        group = lax.rem(at + step, 4)
        top, bottom = pieces[2 * n], pieces[2 * n + 1]
        half = top.shape[0]
        columns = pl.ds(pl.multiple_of(group * cot_part, 128), cot_part)
        out_down[0, :, columns] = dot(hidden[:half, :], top[:, row_part:], first) + dot(
            hidden[half:, :], bottom[:, row_part:], first
        )


def columns_of(array, width, index):
    return pl.BlockSpec(
        (array.shape[0], width), lambda i: (0, index), pipeline_mode=pl.Buffered(1)
    )


def row_grads(position, got, pieces, gate_cot, up_cot, width, row_part):
    row_rest = width - 4 * row_part
    out = made((1, width, gate_cot.shape[1]), F32)
    return pl.pallas_call(
        functools.partial(row_grads_kernel, row_part=row_part),
        out_shape=(out, out),
        grid=(1,),
        in_specs=[
            SMEM,
            columns_of(got, row_rest, 0),
            *(columns_of(p, row_part, 0) for p in pieces),
            whole(gate_cot.shape),
            whole(up_cot.shape),
        ],
        out_specs=[whole(out.shape)] * 2,
        compiler_params=params(22),
        cost_estimate=cost(3 * 10**9, 11 * 2**20),
        name="rowgrads",
    )(position, *kept([got, *pieces, gate_cot, up_cot]))


def down_grads(position, got, pieces, hidden, width, row_part, cot_part):
    row_rest, cot_rest = width - 4 * row_part, width - 4 * cot_part
    out = made((1, hidden.shape[1], width), F32)
    return pl.pallas_call(
        functools.partial(down_grads_kernel, row_part=row_part, cot_part=cot_part),
        out_shape=out,
        grid=(1,),
        in_specs=[
            SMEM,
            columns_of(got, cot_rest, row_rest // cot_rest),
            *(whole(p.shape) for p in pieces),
            whole(hidden.shape),
        ],
        out_specs=whole(out.shape),
        compiler_params=params(20),
        cost_estimate=cost(15 * 10**8, 11 * 2**20),
        name="downgrads",
    )(position, *kept([got, *pieces, hidden]))


def proj_kernel(where_ref, gate_cot, up_cot, w_gate, w_up, local, *refs):
    pieces, out = refs[:-1], refs[-1]
    core = where_ref[1]
    first = ((0,), (0,))
    for n, step in enumerate(ring_steps):
        top, bottom = pieces[2 * n], pieces[2 * n + 1]
        half = top.shape[0]
        push_gate, push_up = (
            (dot(cot[:half, :], top[...], first) + dot(cot[half:, :], bottom[...], first)).astype(BF16)
            for cot in (gate_cot, up_cot)
        )
        term = dot(w_gate[...], push_gate) + dot(w_up[...], push_up)
        if step == 0:
            term = term + local[...]
        term = term.astype(BF16)
        lines = out.shape[3]
        for s in range(2 * out.shape[2]):
            slot = lax.rem(s % 2 + core, 2)
            out[slot, n, s // 2] = term[s * lines : (s + 1) * lines, :]


def proj(position, gate_cot, up_cot, w_gate, w_up, local, pieces, lines):
    width, part = w_gate.shape[0], pieces[0].shape[1]
    args = (position, gate_cot, up_cot, w_gate, w_up, local, *pieces)
    out = made((2, 4, width // lines // 2, lines, part), BF16)
    return pl.pallas_call(
        proj_kernel,
        out_shape=out,
        in_specs=[SMEM] + [whole(a.shape) for a in args[1:]],
        out_specs=whole(out.shape),
        compiler_params=params(22),
        cost_estimate=cost(4 * 10**9, 14 * 2**20),
        name="proj",
    )(position, *kept(args[1:6]), *pieces)


def chip_kernel(kept_ref, other, out_own, *outs):
    half = out_own.shape[0] // 2
    out_own[...] = (kept_ref[0, 0].astype(F32) + other[0].astype(F32)).astype(BF16)
    for n in range(6):
        lines = slice((n % 2) * half, (n % 2 + 1) * half)
        at = 1 + n // 2
        outs[n][...] = (
            kept_ref[0, at, lines].astype(F32) + other[at, lines].astype(F32)
        ).astype(BF16)


def chip_sum(parts, other):
    groups, lines, width = other.shape[1:]
    half = made((groups // 2, lines, width), BF16)
    outs = (made((groups, lines, width), BF16),) + (half,) * 6
    return pl.pallas_call(
        chip_kernel,
        out_shape=outs,
        grid=(1,),
        in_specs=[
            pl.BlockSpec(
                (1, *parts.shape[1:]), lambda i: (0, 0, 0, 0, 0), pipeline_mode=pl.Buffered(1)
            ),
            whole(other.shape),
        ],
        out_specs=[whole(o.shape) for o in outs],
        compiler_params=params(16),
        cost_estimate=cost(10**7, 6 * 2**20),
        name="chipsum",
    )(*kept([parts]), other)


def scan_kernel(back, sel, base, act, b, decay, seg, block, out_grad, out_local, out_pair, drive, part):
    tokens, channels = base.shape
    length = tokens // 8
    mix = base[...]
    total = back[0].astype(F32) + back[1].astype(F32) + back[2].astype(F32) + back[3].astype(F32)
    mix = mix + dot(sel[...], total.astype(BF16))
    out_grad[...] = (mix * b[...]).astype(BF16)
    push = mix * act[...]
    for h in range(channels // 128):
        cols = slice(h * 128, (h + 1) * 128)
        drive[h] = push[:, cols]
        value = drive[h, pl.ds(length - 1, 8, stride=length), :]
        part[h, pl.ds(length - 1, 8, stride=length), :] = value
        for i in range(length - 2, -1, -1):
            value = (
                drive[h, pl.ds(i, 8, stride=length), :]
                + decay[h, pl.ds(i + 1, 8, stride=length), :] * value
            )
            part[h, pl.ds(i, 8, stride=length), :] = value
        lead = decay[h, pl.ds(0, 8, stride=length), :]
        inner = seg[h, pl.ds(0, 8, stride=length), :]
        carry = jnp.zeros((1, 128), F32)
        for k in range(7, -1, -1):
            rows = slice(k * length, (k + 1) * length)
            out_local[rows, cols] = part[h, rows, :] + seg[h, rows, :] * carry
            one = slice(k, k + 1)
            carry = lead[one, :] * (value[one, :] + inner[one, :] * carry)
        pair = jnp.concatenate([carry, block[0:1, cols]], axis=0)
        out_pair[:, :, cols] = jnp.broadcast_to(pair[None], (out_pair.shape[0], *pair.shape))


def scanned(back, sel, base, act, b, decay, seg, block, sources):
    tokens, channels = base.shape
    args = (back, sel, base, act, b, decay, seg, block)
    outs = (
        made((tokens, channels), BF16),
        made((tokens, channels), F32),
        made((sources, 2, channels), F32),
    )
    return pl.pallas_call(
        scan_kernel,
        out_shape=outs,
        in_specs=[whole(a.shape) for a in args],
        out_specs=[whole(o.shape) for o in outs],
        scratch_shapes=[pltpu.VMEM(decay.shape, F32), pltpu.VMEM(decay.shape, F32)],
        compiler_params=params(14),
        cost_estimate=cost(4 * 10**8, 8 * 2**20),
        name="scanned",
    )(back, *kept(args[1:]))


def final_kernel(where_ref, pairs, local, exp, ca, ci, cs, map_a, map_i, out):
    channels = local.shape[1]
    heads = channels // 128
    first = where_ref[0] * heads
    total = jnp.zeros((1, channels), F32)
    me = where_ref[2]
    for s in range(pairs.shape[0] - 1, 0, -1):
        total = jnp.where(me < s, pairs[s, 0:1, :] + pairs[s, 1:2, :] * total, total)
    for h in range(heads):
        cols = slice(h * 128, (h + 1) * 128)
        cot = local[:, cols] + exp[:, cols] * total[:, cols]
        a_cot = (cot * ca[:, cols]).astype(BF16)
        i_cot = (cot * ci[:, cols]).astype(BF16)
        result = (
            cot * cs[:, cols]
            + dot(a_cot, map_a[first + h], ((1,), (1,)))
            + dot(i_cot, map_i[first + h], ((1,), (1,)))
        )
        out[:, cols] = result.astype(BF16)


def final(position, pairs, local, exp, ca, ci, cs, map_a, map_i):
    args = (position, pairs, local, exp, ca, ci, cs, map_a, map_i)
    return pl.pallas_call(
        final_kernel,
        out_shape=made(local.shape, BF16),
        in_specs=[SMEM] + [whole(a.shape) for a in args[1:]],
        out_specs=whole(local.shape),
        compiler_params=params(8),
        cost_estimate=cost(10**8, 4 * 2**20),
        name="final",
    )(position, pairs, *kept(args[2:]))


def shifted(piece, by):
    return lax.ppermute(piece, "tp", [(i, (i + by) % 4) for i in range(4)])


def ring_gather(top, bottom):
    left_top, right_bottom = shifted(top, 1), shifted(bottom, -1)
    left_bottom, right_top = shifted(bottom, 1), shifted(top, -1)
    far_top, far_bottom = shifted(left_top, 1), shifted(right_bottom, -1)
    return top, bottom, left_top, left_bottom, right_top, right_bottom, far_top, far_bottom


def shared_ring_gather(own, core):
    half = own.shape[0] // 2
    mine = lax.dynamic_slice_in_dim(own, core * half, half, 0)
    left, right = shifted(mine, 1), shifted(mine, -1)
    quarter = half // 2
    far_top, far_bottom = shifted(left[:quarter], 1), shifted(right[quarter:], -1)
    pieces = (left, right, far_top, far_bottom)
    others = tuple(lax.ppermute(p, "core", [(0, 1), (1, 0)]) for p in pieces)
    return pieces + others


def per_device(
    layer_input, out_cot, expert_ids, route_weight, w_gate, w_up, w_down, out_proj,
    rec_input, gate_input, prev_state, decay_param, extra_decay, gate_a_w, gate_i_w,
):
    sources = lax.axis_size("sq") * lax.axis_size("core")
    tp = lax.axis_index("tp")
    core = lax.axis_index("core")
    sp_axes = ("sq", "core")
    sp = lax.axis_index("sq") * 2 + core
    position = jnp.stack([tp, core, sp]).astype(jnp.int32)
    w_gate, w_up, w_down = w_gate[0], w_up[0], w_down[0]
    tokens, width = layer_input.shape
    capacity = 5 * tokens * expert_ids.shape[1] // (4 * sources)
    slots = sources * capacity
    row_part, cot_part = width // 8, 3 * width // 16
    row_rest, cot_rest = width - 4 * row_part, width - 4 * cot_part
    ids, weight = expert_ids.T, route_weight.T

    def exchanged(rows):
        return lax.all_to_all(
            rows.reshape(sources, capacity, -1), sp_axes, 0, 0, tiled=True
        ).reshape(rows.shape)

    spread = build(
        position, ids, weight,
        [(layer_input, row_part, None, False), (out_cot, cot_part, None, True)],
        capacity, sources,
    )
    spread = exchanged(spread)
    projections = shared_ring_gather(out_proj, core)
    gate_up, down, fold_gate, fold_up = folded_weights(
        position, w_gate, w_up, w_down, out_proj, projections, row_part, cot_part
    )
    rates = (decay_factor * jax.nn.softplus(-decay_param)).reshape(-1, gate_a_w.shape[1])
    rec_output, act, b, ca, ci, cs, decay, seg, exp, block, sel = early(
        position, expert_ids, rec_input, gate_input, prev_state, rates, extra_decay.T,
        gate_a_w, gate_i_w, capacity, sources,
    )
    direct = build(
        position, ids, weight,
        [
            (layer_input, row_rest, 4 * row_part // row_rest, False),
            (out_cot, cot_rest, 4 * cot_part // cot_rest, True),
            (rec_output, rec_output.shape[1], 0, False),
        ],
        capacity, sources,
    )
    got = exchanged(direct)
    pieces = ring_gather(spread[: slots // 2], spread[slots // 2 :])
    base = jnp.dot(out_cot, out_proj, preferred_element_type=F32)
    local_proj = lax.dot_general(
        out_cot, rec_output, (((0,), (0,)), ((), ())), preferred_element_type=F32
    )
    before = ahead(pieces[:6], gate_up, down, row_part, cot_part)
    hidden, gate_cot, up_cot, mix = expert(
        got, pieces[6:], before, gate_up, down, fold_gate, fold_up, row_part, cot_part
    )
    back = lax.all_to_all(
        mix.reshape(4 * sources, capacity, -1), ("tp", *sp_axes), 0, 0, tiled=True
    ).reshape(mix.shape)
    grad_gate, grad_up = row_grads(position, got, pieces, gate_cot, up_cot, width, row_part)
    grad_down = down_grads(position, got, pieces, hidden, width, row_part, cot_part)
    start = row_rest + cot_rest
    recs = ring_gather(got[: slots // 2, start:], got[slots // 2 :, start:])
    lines = width // sources
    parts = proj(position, gate_cot, up_cot, w_gate, w_up, local_proj, recs, lines)
    other = lax.ppermute(parts[1], "core", [(0, 1), (1, 0)])
    own, left_top, left_bottom, right_top, right_bottom, far_top, far_bottom = chip_sum(
        parts, other
    )
    through_top, through_bottom = shifted(far_top, 1), shifted(far_bottom, -1)
    from_left, from_right = shifted(right_bottom, 1), shifted(left_top, -1)
    both_top = (right_top.astype(F32) + through_top.astype(F32)).astype(BF16)
    both_bottom = (left_bottom.astype(F32) + through_bottom.astype(F32)).astype(BF16)
    last_top, last_bottom = shifted(both_top, 1), shifted(both_bottom, -1)
    arriving = (
        jnp.concatenate([last_top, last_bottom], axis=0).astype(F32)
        + jnp.concatenate([from_right, from_left], axis=0).astype(F32)
        + own.astype(F32)
    ).astype(BF16)
    arrived = lax.all_to_all(arriving, "sq", 0, 0, tiled=True)
    grad_out_proj = arrived.astype(F32).sum(axis=0)
    gate_input_grad, local, pair = scanned(
        back, sel, base, act, b, decay, seg, block, sources
    )
    pairs = lax.all_to_all(pair, sp_axes, 0, 0, tiled=True)
    rec_input_grad = final(position, pairs, local, exp, ca, ci, cs, gate_a_w, gate_i_w)
    return (grad_gate, grad_up, grad_down, grad_out_proj, rec_input_grad, gate_input_grad)


def solution(mesh):
    sp, tp = mesh.devices.shape
    inner = Mesh(mesh.devices.reshape(sp // 2, 2, tp), ("sq", "core", "tp"))
    sp = ("sq", "core")
    in_specs = (
        P(sp, None),
        P(sp, None),
        P(sp, None),
        P(sp, None),
        P(sp, None, "tp"),
        P(sp, None, "tp"),
        P(sp, "tp", None),
        P(None, "tp"),
        P(sp, "tp"),
        P(sp, "tp"),
        P(sp, "tp"),
        P(),
        P("tp", sp),
        P(),
        P(),
    )
    out_specs = (
        P(sp, None, "tp"),
        P(sp, None, "tp"),
        P(sp, "tp", None),
        P(sp, "tp"),
        P(sp, "tp"),
        P(sp, "tp"),
    )
    return jax.shard_map(
        per_device, mesh=inner, in_specs=in_specs, out_specs=out_specs, check_vma=False
    )
```

```python
import functools
import jax
import jax.numpy as jnp
from jax import lax
from jax.experimental import pallas as pl
from jax.experimental.pallas import tpu as pltpu
from jax.sharding import Mesh, PartitionSpec as P


F32 = jnp.float32
BF16 = jnp.bfloat16
gelu_scale = 0.7978845608028654
gelu_cubic = 0.044715
decay_factor = 8.0
ring_steps = (0, 3, 1, 2)


def params(limit_mib=48, **extra):
    return pltpu.CompilerParams(vmem_limit_bytes=limit_mib * 1024 * 1024, **extra)


def cost(flops, moved):
    return pl.CostEstimate(flops=flops, bytes_accessed=moved, transcendentals=0)


def whole(shape):
    return pl.BlockSpec(shape, lambda *_: (0,) * len(shape), pipeline_mode=pl.Buffered(1))


SMEM = pl.BlockSpec(memory_space=pltpu.SMEM)


def made(shape, dtype):
    return pltpu.HBM(shape, dtype)


def kept(arrays):
    return [pltpu.with_memory_space_constraint(a, pltpu.HBM) for a in arrays]


def dot(a, b, dims=((1,), (0,))):
    return lax.dot_general(a, b, (dims, ((), ())), preferred_element_type=F32)


def sigmoid(v):
    return 1.0 / (1.0 + jnp.exp(-v))


def minus_expm1(v):
    series = 1.0 + v / 8.0
    for order in range(7, 1, -1):
        series = 1.0 + v / order * series
    return jnp.where(v > -0.5, -v * series, 1.0 - jnp.exp(v))


def early_kernel(
    where_ref, ids, rec, gate_in, prev, rates, extra, map_a, map_i,
    out_rec, out_act, out_b, out_ca, out_ci, out_cs, out_decay, out_seg, out_exp, out_block, out_sel,
    *, capacity, experts,
):
    tokens, channels = rec.shape
    heads = channels // 128
    first = where_ref[0] * heads

    def block_of_tokens(i, _):
        rows = pl.ds(pl.multiple_of(i * 128, 128), 128)
        for h in range(heads):
            cols = slice(h * 128, (h + 1) * 128)
            values_bf = rec[rows, cols]
            x = values_bf.astype(F32)
            ra = sigmoid(dot(values_bf, map_a[first + h]))
            ig = sigmoid(dot(values_bf, map_i[first + h]))
            rate = rates[pl.ds(first + h, 1), :]
            log_decay = -rate * ra + extra[rows, h : h + 1]
            decay = jnp.exp(log_decay)
            scale = jnp.sqrt(minus_expm1(2.0 * log_decay))
            before = prev[rows, cols]
            state = decay * before + scale * ig * x
            g = gate_in[rows, cols].astype(F32)
            bend = jnp.tanh(gelu_scale * (g + gelu_cubic * g * g * g))
            act = 0.5 * g * (1.0 + bend)
            slope = 0.5 * (1.0 + bend) + 0.5 * g * (1.0 - bend * bend) * gelu_scale * (
                1.0 + 3.0 * gelu_cubic * g * g
            )
            out_rec[rows, cols] = (state * act).astype(BF16)
            out_act[rows, cols] = act
            out_b[rows, cols] = state * slope
            out_ca[rows, cols] = (decay * before - decay * decay / scale * ig * x) * -rate * ra * (1.0 - ra)
            out_ci[rows, cols] = scale * x * ig * (1.0 - ig)
            out_cs[rows, cols] = scale * ig
            out_decay[h, rows, :] = decay
        return 0

    lax.fori_loop(0, tokens // 128, block_of_tokens, 0)
    length = tokens // 8
    for h in range(heads):
        cols = slice(h * 128, (h + 1) * 128)
        product = jnp.ones((8, 128), F32)
        for i in range(length - 1, -1, -1):
            out_seg[h, pl.ds(i, 8, stride=length), :] = product
            product = product * out_decay[h, pl.ds(i, 8, stride=length), :]
        carry = jnp.ones((1, 128), F32)
        for k in range(7, -1, -1):
            rows = slice(k * length, (k + 1) * length)
            out_exp[rows, cols] = out_seg[h, rows, :] * carry
            carry = carry * product[k : k + 1, :]
        out_block[:, cols] = jnp.broadcast_to(carry, (8, 128))
    lane = lax.broadcasted_iota(jnp.int32, (tokens, 128), 1)
    first_id = ids[:, 0:1]
    second_id = ids[:, 1:2]
    one = (lane == first_id).astype(F32)
    two = (lane == second_id).astype(F32)
    lower = lax.broadcasted_iota(jnp.int32, (tokens, tokens), 0) > lax.broadcasted_iota(
        jnp.int32, (tokens, tokens), 1
    )
    rank = dot(lower.astype(F32).astype(BF16), (one + two).astype(BF16))
    place_one = first_id * capacity + jnp.sum(rank * one, axis=1, keepdims=True).astype(jnp.int32)
    place_two = second_id * capacity + jnp.sum(rank * two, axis=1, keepdims=True).astype(jnp.int32)
    slots = experts * capacity

    def block_of_slots(i, _):
        at = pl.multiple_of(i * 256, 256)
        slot = lax.broadcasted_iota(jnp.int32, (tokens, 256), 1) + at
        hit = (slot == place_one) | (slot == place_two)
        out_sel[:, pl.ds(at, 256)] = jnp.where(hit, 1.0, 0.0).astype(BF16)
        return 0

    lax.fori_loop(0, slots // 256, block_of_slots, 0)


def early(position, ids, rec, gate_in, prev, rates, extra, map_a, map_i, capacity, experts):
    tokens, channels = rec.shape
    wide = made((tokens, channels), F32)
    heads = made((channels // 128, tokens, 128), F32)
    outs = (
        made((tokens, channels), BF16),
        wide, wide, wide, wide, wide, heads, heads, wide,
        made((8, channels), F32),
        made((tokens, experts * capacity), BF16),
    )
    args = (position, ids, rec, gate_in, prev, rates, extra, map_a, map_i)
    return pl.pallas_call(
        functools.partial(early_kernel, capacity=capacity, experts=experts),
        out_shape=outs,
        in_specs=[SMEM] + [whole(a.shape) for a in args[1:]],
        out_specs=[whole(o.shape) for o in outs],
        compiler_params=params(14),
        cost_estimate=cost(3 * 10**9, 8 * 2**20),
        name="early",
    )(args[0], *kept(args[1:]))


def build_kernel(where_ref, ids, weight, *refs, capacity, group, weighted):
    sources, out, rank_ref, weight_ref = refs[:-3], refs[-3], refs[-2], refs[-1]
    experts, tokens = rank_ref.shape

    @pl.when(pl.program_id(0) == 0)
    def _():
        name = lax.broadcasted_iota(jnp.int32, (experts, tokens), 0)
        one = jnp.where(name == ids[0:1, :], 1.0, 0.0)
        two = jnp.where(name == ids[1:2, :], 1.0, 0.0)
        both = one + two
        upper = lax.broadcasted_iota(jnp.int32, (tokens, tokens), 0) < lax.broadcasted_iota(
            jnp.int32, (tokens, tokens), 1
        )
        rank = dot(both.astype(BF16), upper.astype(F32).astype(BF16))
        rank_ref[...] = jnp.where(both > 0.0, rank, -1.0)
        weight_ref[...] = one * weight[0:1, :] + two * weight[1:2, :]

    first = pl.program_id(0) * group
    place = lax.broadcasted_iota(jnp.int32, (capacity, tokens), 0).astype(F32)
    picks, weights = [], []
    for e in range(group):
        hit = place == rank_ref[pl.ds(first + e, 1), :]
        picks.append(jnp.where(hit, 1.0, 0.0))
        weights.append(
            jnp.sum(jnp.where(hit, weight_ref[pl.ds(first + e, 1), :], 0.0), axis=1, keepdims=True)
        )
    pick = jnp.concatenate(picks, axis=0).astype(BF16)
    by = jnp.concatenate(weights, axis=0)
    at = 0
    for source, scaled in zip(sources, weighted):
        rows = dot(pick, source[...])
        if scaled:
            rows = rows * by
        out[:, at : at + source.shape[1]] = rows.astype(BF16)
        at += source.shape[1]


def build(position, ids, weight, parts, capacity, experts, group=8):
    tokens = ids.shape[1]
    total = sum(width for _, width, _, _ in parts)
    specs = [pl.BlockSpec(ids.shape, lambda i, where: (0, 0))] * 2
    for _, width, column, _ in parts:
        specs.append(pl.BlockSpec((tokens, width), functools.partial(column_block, column)))
    return pl.pallas_call(
        functools.partial(
            build_kernel, capacity=capacity, group=group, weighted=tuple(p[3] for p in parts)
        ),
        out_shape=made((experts * capacity, total), BF16),
        grid_spec=pltpu.PrefetchScalarGridSpec(
            num_scalar_prefetch=1,
            grid=(experts // group,),
            in_specs=specs,
            out_specs=pl.BlockSpec((group * capacity, total), lambda i, where: (i, 0)),
            scratch_shapes=[pltpu.VMEM((experts, tokens), F32), pltpu.VMEM((experts, tokens), F32)],
        ),
        compiler_params=params(14),
        cost_estimate=cost(1400000 * total, 5000 * total),
    )(position, *kept([ids, weight, *(p[0] for p in parts)]))


def column_block(column, i, where):
    return (0, where[0] if column is None else column)


def weights_kernel(
    where_ref, w_gate, w_up, w_down, whole_own, *refs, row_part, cot_part,
):
    pieces = refs[:8]
    out_gate_up, out_down, out_gate, out_up = refs[8:]
    at, core = where_ref[0], where_ref[1]
    width, units = w_gate.shape
    half = width // 2
    first = ((0,), (0,))
    mine = pl.multiple_of(core * half, half)
    other = pl.multiple_of(half - core * half, half)
    for weights, out in ((w_gate, out_gate), (w_up, out_up)):
        out[at] = dot(weights[...], whole_own[...], first).astype(BF16)
        for step, n in ((3, 0), (1, 1)):
            out[lax.rem(at + step, 4)] = (
                dot(weights[pl.ds(mine, half), :], pieces[n][...], first)
                + dot(weights[pl.ds(other, half), :], pieces[4 + n][...], first)
            ).astype(BF16)
        quarter = half // 2
        out[lax.rem(at + 2, 4)] = sum(
            dot(weights[pl.ds(start + n * quarter, quarter), :], pieces[side + 2 + n][...], first)
            for start, side in ((mine, 0), (other, 4))
            for n in range(2)
        ).astype(BF16)
    rest = width - 4 * row_part
    out_gate_up[:rest, :units] = w_gate[4 * row_part :, :]
    out_gate_up[:rest, units:] = w_up[4 * row_part :, :]
    cot_rest = width - 4 * cot_part
    out_down[:cot_rest, :] = w_down[:, 4 * cot_part :].T
    for n, step in enumerate((2, 0, 3, 1)):
        group = lax.rem(at + step, 4)
        lines = pl.ds(pl.multiple_of(group * row_part, row_part), row_part)
        columns = pl.ds(pl.multiple_of(group * cot_part, 128), cot_part)
        to = slice(rest + n * row_part, rest + (n + 1) * row_part)
        out_gate_up[to, :units] = w_gate[lines, :]
        out_gate_up[to, units:] = w_up[lines, :]
        to = slice(cot_rest + n * cot_part, cot_rest + (n + 1) * cot_part)
        out_down[to, :] = w_down[:, columns].T


def folded_weights(position, w_gate, w_up, w_down, own, pieces, row_part, cot_part):
    width, units = w_gate.shape
    args = (position, w_gate, w_up, w_down, own, *pieces)
    fold = made((4, units, own.shape[1]), BF16)
    outs = (made((width, 2 * units), BF16), made((width, units), BF16), fold, fold)
    return pl.pallas_call(
        functools.partial(weights_kernel, row_part=row_part, cot_part=cot_part),
        out_shape=outs,
        in_specs=[SMEM] + [whole(a.shape) for a in args[1:]],
        out_specs=[whole(o.shape) for o in outs],
        compiler_params=params(24),
        cost_estimate=cost(4 * 10**9, 7 * 2**20),
        name="folded",
    )(position, *kept([w_gate, w_up, w_down, own]), *pieces)


def ahead_kernel(gate_up, down, *refs, row_part, row_from, cot_from):
    pieces, out = refs[:-1], refs[-1]
    half = pieces[0].shape[0]
    wide = gate_up.shape[1]
    for n in range(2):
        lines = slice(n * half, (n + 1) * half)
        rows = jnp.concatenate([p[:, :row_part] for p in pieces[n::2]], axis=1)
        cots = jnp.concatenate([p[:, row_part:] for p in pieces[n::2]], axis=1)
        out[lines, :wide] = dot(rows, gate_up[row_from:, :])
        out[lines, wide:] = dot(cots, down[cot_from:, :])


def ahead(pieces, gate_up, down, row_part, cot_part):
    width = gate_up.shape[0]
    out = made((2 * pieces[0].shape[0], gate_up.shape[1] + down.shape[1]), F32)
    args = (gate_up, down, *pieces)
    return pl.pallas_call(
        functools.partial(
            ahead_kernel,
            row_part=row_part,
            row_from=width - 3 * row_part,
            cot_from=width - 3 * cot_part,
        ),
        out_shape=out,
        in_specs=[whole(a.shape) for a in args],
        out_specs=whole(out.shape),
        compiler_params=params(20),
        cost_estimate=cost(2 * 10**9, 12 * 2**20),
        name="ahead",
    )(*kept([gate_up, down]), *pieces)


def expert_kernel(
    got_rows, got_cot, far_top, far_bottom, before, gate_up, down, fold_gate, fold_up,
    out_hidden, out_gate, out_up, out_mix, *, row_part,
):
    units = down.shape[1]
    upper = pl.program_id(0) < pl.num_programs(0) // 2
    far = jnp.where(upper, far_top[...], far_bottom[...])
    rows = jnp.concatenate([got_rows[...], far[:, :row_part]], axis=1)
    cots = jnp.concatenate([got_cot[...], far[:, row_part:]], axis=1)
    both = dot(rows, gate_up[...]) + before[:, : 2 * units]
    gate_pre, up_pre = both[:, :units], both[:, units:]
    hidden_cot = dot(cots, down[...]) + before[:, 2 * units :]
    sigma = sigmoid(gate_pre)
    swish = gate_pre * sigma
    out_hidden[...] = (swish * up_pre).astype(BF16)
    gate_cot = (hidden_cot * up_pre * sigma * (1.0 + gate_pre * (1.0 - sigma))).astype(BF16)
    up_cot = (hidden_cot * swish).astype(BF16)
    out_gate[...] = gate_cot
    out_up[...] = up_cot
    for c in range(4):
        out_mix[c] = (dot(gate_cot, fold_gate[c]) + dot(up_cot, fold_up[c])).astype(BF16)


def first_rows(array, count):
    return pl.BlockSpec(
        (count, array.shape[1]), lambda i: (0, 0), pipeline_mode=pl.Buffered(1)
    )


def expert(got, far, before, gate_up, down, fold_gate, fold_up, row_part, cot_part, steps=4):
    rows = got.shape[0]
    width, hidden = down.shape
    block = rows // steps
    part = fold_gate.shape[2]
    half = steps // 2
    row_rest, cot_rest = width - 4 * row_part, width - 4 * cot_part
    narrow = made((rows, hidden), BF16)
    mine = pl.BlockSpec((block, hidden), lambda i: (i, 0))
    return pl.pallas_call(
        functools.partial(expert_kernel, row_part=row_part),
        out_shape=(narrow, narrow, narrow, made((4, rows, part), BF16)),
        grid=(steps,),
        in_specs=[
            pl.BlockSpec((block, row_rest), lambda i: (i, 0)),
            pl.BlockSpec((block, cot_rest), lambda i: (i, row_rest // cot_rest)),
            pl.BlockSpec((block, row_part + cot_part), lambda i: (jnp.minimum(i, half - 1), 0)),
            pl.BlockSpec((block, row_part + cot_part), lambda i: (jnp.maximum(i - half, 0), 0)),
            pl.BlockSpec((block, before.shape[1]), lambda i: (i, 0)),
            first_rows(gate_up, row_rest + row_part),
            first_rows(down, cot_rest + cot_part),
            whole(fold_gate.shape),
            whole(fold_up.shape),
        ],
        out_specs=[mine, mine, mine, pl.BlockSpec((4, block, part), lambda i: (0, i, 0))],
        compiler_params=params(26),
        cost_estimate=cost(5 * 10**9, 16 * 2**20),
        name="expert",
    )(*kept([got, got]), *far, *kept([before, gate_up, down, fold_gate, fold_up]))


def row_grads_kernel(where_ref, got_rows, *refs, row_part):
    pieces = refs[:8]
    gate_cot, up_cot, out_gate, out_up = refs[8:]
    at = where_ref[0]
    first = ((0,), (0,))
    rows = got_rows[...]
    out_gate[0, 4 * row_part :, :] = dot(rows, gate_cot[...], first)
    out_up[0, 4 * row_part :, :] = dot(rows, up_cot[...], first)
    for n, step in enumerate(ring_steps):
        group = lax.rem(at + step, 4)
        top, bottom = pieces[2 * n], pieces[2 * n + 1]
        half = top.shape[0]
        lines = pl.ds(pl.multiple_of(group * row_part, row_part), row_part)
        for cot, out in ((gate_cot, out_gate), (up_cot, out_up)):
            out[0, lines, :] = dot(top[...], cot[:half, :], first) + dot(
                bottom[...], cot[half:, :], first
            )


def down_grads_kernel(where_ref, got_cot, *refs, row_part, cot_part):
    pieces = refs[:8]
    hidden, out_down = refs[8:]
    at = where_ref[0]
    first = ((0,), (0,))
    out_down[0, :, 4 * cot_part :] = dot(hidden[...], got_cot[...], first)
    for n, step in enumerate(ring_steps):
        group = lax.rem(at + step, 4)
        top, bottom = pieces[2 * n], pieces[2 * n + 1]
        half = top.shape[0]
        columns = pl.ds(pl.multiple_of(group * cot_part, 128), cot_part)
        out_down[0, :, columns] = dot(hidden[:half, :], top[:, row_part:], first) + dot(
            hidden[half:, :], bottom[:, row_part:], first
        )


def columns_of(array, width, index):
    return pl.BlockSpec(
        (array.shape[0], width), lambda i: (0, index), pipeline_mode=pl.Buffered(1)
    )


def row_grads(position, got, pieces, gate_cot, up_cot, width, row_part):
    row_rest = width - 4 * row_part
    out = made((1, width, gate_cot.shape[1]), F32)
    return pl.pallas_call(
        functools.partial(row_grads_kernel, row_part=row_part),
        out_shape=(out, out),
        grid=(1,),
        in_specs=[
            SMEM,
            columns_of(got, row_rest, 0),
            *(columns_of(p, row_part, 0) for p in pieces),
            whole(gate_cot.shape),
            whole(up_cot.shape),
        ],
        out_specs=[whole(out.shape)] * 2,
        compiler_params=params(22),
        cost_estimate=cost(3 * 10**9, 11 * 2**20),
        name="rowgrads",
    )(position, *kept([got, *pieces, gate_cot, up_cot]))


def down_grads(position, got, pieces, hidden, width, row_part, cot_part):
    row_rest, cot_rest = width - 4 * row_part, width - 4 * cot_part
    out = made((1, hidden.shape[1], width), F32)
    return pl.pallas_call(
        functools.partial(down_grads_kernel, row_part=row_part, cot_part=cot_part),
        out_shape=out,
        grid=(1,),
        in_specs=[
            SMEM,
            columns_of(got, cot_rest, row_rest // cot_rest),
            *(whole(p.shape) for p in pieces),
            whole(hidden.shape),
        ],
        out_specs=whole(out.shape),
        compiler_params=params(20),
        cost_estimate=cost(15 * 10**8, 11 * 2**20),
        name="downgrads",
    )(position, *kept([got, *pieces, hidden]))


def proj_kernel(where_ref, gate_cot, up_cot, w_gate, w_up, local, *refs):
    pieces, out = refs[:-1], refs[-1]
    core = where_ref[1]
    first = ((0,), (0,))
    for n, step in enumerate(ring_steps):
        push_gate, push_up = (
            dot(cot[...], pieces[n][...], first).astype(BF16) for cot in (gate_cot, up_cot)
        )
        term = dot(w_gate[...], push_gate) + dot(w_up[...], push_up)
        if step == 0:
            term = term + local[...]
        term = term.astype(BF16)
        lines = out.shape[3]
        for s in range(2 * out.shape[2]):
            slot = lax.rem(s % 2 + core, 2)
            out[slot, n, s // 2] = term[s * lines : (s + 1) * lines, :]


def proj(position, gate_cot, up_cot, w_gate, w_up, local, pieces, lines):
    width, part = w_gate.shape[0], pieces[0].shape[1]
    args = (position, gate_cot, up_cot, w_gate, w_up, local, *pieces)
    out = made((2, 4, width // lines // 2, lines, part), BF16)
    return pl.pallas_call(
        proj_kernel,
        out_shape=out,
        in_specs=[SMEM] + [whole(a.shape) for a in args[1:]],
        out_specs=whole(out.shape),
        compiler_params=params(22),
        cost_estimate=cost(4 * 10**9, 14 * 2**20),
        name="proj",
    )(position, *kept(args[1:6]), *pieces)


def chip_kernel(kept_ref, other, *outs):
    for n, out in enumerate(outs):
        out[...] = (kept_ref[0, n].astype(F32) + other[n].astype(F32)).astype(BF16)


def chip_sum(parts, other):
    out = made(other.shape[1:], BF16)
    return pl.pallas_call(
        chip_kernel,
        out_shape=(out,) * other.shape[0],
        grid=(1,),
        in_specs=[
            pl.BlockSpec(
                (1, *parts.shape[1:]), lambda i: (0, 0, 0, 0, 0), pipeline_mode=pl.Buffered(1)
            ),
            whole(other.shape),
        ],
        out_specs=[whole(out.shape)] * other.shape[0],
        compiler_params=params(16),
        cost_estimate=cost(10**7, 6 * 2**20),
        name="chipsum",
    )(*kept([parts]), other)


def scan_kernel(back, sel, base, act, b, decay, seg, block, out_grad, out_local, out_pair, drive, part):
    tokens, channels = base.shape
    length = tokens // 8
    mix = base[...]
    total = back[0].astype(F32) + back[1].astype(F32) + back[2].astype(F32) + back[3].astype(F32)
    mix = mix + dot(sel[...], total.astype(BF16))
    out_grad[...] = (mix * b[...]).astype(BF16)
    push = mix * act[...]
    for h in range(channels // 128):
        cols = slice(h * 128, (h + 1) * 128)
        drive[h] = push[:, cols]
        value = drive[h, pl.ds(length - 1, 8, stride=length), :]
        part[h, pl.ds(length - 1, 8, stride=length), :] = value
        for i in range(length - 2, -1, -1):
            value = (
                drive[h, pl.ds(i, 8, stride=length), :]
                + decay[h, pl.ds(i + 1, 8, stride=length), :] * value
            )
            part[h, pl.ds(i, 8, stride=length), :] = value
        lead = decay[h, pl.ds(0, 8, stride=length), :]
        inner = seg[h, pl.ds(0, 8, stride=length), :]
        carry = jnp.zeros((1, 128), F32)
        for k in range(7, -1, -1):
            rows = slice(k * length, (k + 1) * length)
            out_local[rows, cols] = part[h, rows, :] + seg[h, rows, :] * carry
            one = slice(k, k + 1)
            carry = lead[one, :] * (value[one, :] + inner[one, :] * carry)
        pair = jnp.concatenate([carry, block[0:1, cols]], axis=0)
        out_pair[:, :, cols] = jnp.broadcast_to(pair[None], (out_pair.shape[0], *pair.shape))


def scanned(back, sel, base, act, b, decay, seg, block, sources):
    tokens, channels = base.shape
    args = (back, sel, base, act, b, decay, seg, block)
    outs = (
        made((tokens, channels), BF16),
        made((tokens, channels), F32),
        made((sources, 2, channels), F32),
    )
    return pl.pallas_call(
        scan_kernel,
        out_shape=outs,
        in_specs=[whole(a.shape) for a in args],
        out_specs=[whole(o.shape) for o in outs],
        scratch_shapes=[pltpu.VMEM(decay.shape, F32), pltpu.VMEM(decay.shape, F32)],
        compiler_params=params(14),
        cost_estimate=cost(4 * 10**8, 8 * 2**20),
        name="scanned",
    )(back, *kept(args[1:]))


def final_kernel(where_ref, pairs, local, exp, ca, ci, cs, map_a, map_i, out):
    channels = local.shape[1]
    heads = channels // 128
    first = where_ref[0] * heads
    total = jnp.zeros((1, channels), F32)
    me = where_ref[2]
    for s in range(pairs.shape[0] - 1, 0, -1):
        total = jnp.where(me < s, pairs[s, 0:1, :] + pairs[s, 1:2, :] * total, total)
    for h in range(heads):
        cols = slice(h * 128, (h + 1) * 128)
        cot = local[:, cols] + exp[:, cols] * total[:, cols]
        a_cot = (cot * ca[:, cols]).astype(BF16)
        i_cot = (cot * ci[:, cols]).astype(BF16)
        result = (
            cot * cs[:, cols]
            + dot(a_cot, map_a[first + h], ((1,), (1,)))
            + dot(i_cot, map_i[first + h], ((1,), (1,)))
        )
        out[:, cols] = result.astype(BF16)


def final(position, pairs, local, exp, ca, ci, cs, map_a, map_i):
    args = (position, pairs, local, exp, ca, ci, cs, map_a, map_i)
    return pl.pallas_call(
        final_kernel,
        out_shape=made(local.shape, BF16),
        in_specs=[SMEM] + [whole(a.shape) for a in args[1:]],
        out_specs=whole(local.shape),
        compiler_params=params(8),
        cost_estimate=cost(10**8, 4 * 2**20),
        name="final",
    )(position, pairs, *kept(args[2:]))


def shifted(piece, by):
    return lax.ppermute(piece, "tp", [(i, (i + by) % 4) for i in range(4)])


def ring_gather(top, bottom):
    left_top, right_bottom = shifted(top, 1), shifted(bottom, -1)
    left_bottom, right_top = shifted(bottom, 1), shifted(top, -1)
    far_top, far_bottom = shifted(left_top, 1), shifted(right_bottom, -1)
    return top, bottom, left_top, left_bottom, right_top, right_bottom, far_top, far_bottom


def across(own):
    return own, shifted(own, 1), shifted(own, -1), shifted(own, 2)


def shared_ring_gather(own, core):
    half = own.shape[0] // 2
    mine = lax.dynamic_slice_in_dim(own, core * half, half, 0)
    left, right = shifted(mine, 1), shifted(mine, -1)
    quarter = half // 2
    far_top, far_bottom = shifted(left[:quarter], 1), shifted(right[quarter:], -1)
    pieces = (left, right, far_top, far_bottom)
    others = tuple(lax.ppermute(p, "core", [(0, 1), (1, 0)]) for p in pieces)
    return pieces + others


def per_device(
    layer_input, out_cot, expert_ids, route_weight, w_gate, w_up, w_down, out_proj,
    rec_input, gate_input, prev_state, decay_param, extra_decay, gate_a_w, gate_i_w,
):
    sources = lax.axis_size("sq") * lax.axis_size("core")
    tp = lax.axis_index("tp")
    core = lax.axis_index("core")
    sp_axes = ("sq", "core")
    sp = lax.axis_index("sq") * 2 + core
    position = jnp.stack([tp, core, sp]).astype(jnp.int32)
    w_gate, w_up, w_down = w_gate[0], w_up[0], w_down[0]
    tokens, width = layer_input.shape
    capacity = 5 * tokens * expert_ids.shape[1] // (4 * sources)
    slots = sources * capacity
    row_part, cot_part = width // 8, 3 * width // 16
    row_rest, cot_rest = width - 4 * row_part, width - 4 * cot_part
    ids, weight = expert_ids.T, route_weight.T

    def exchanged(rows):
        return lax.all_to_all(
            rows.reshape(sources, capacity, -1), sp_axes, 0, 0, tiled=True
        ).reshape(rows.shape)

    spread = build(
        position, ids, weight,
        [(layer_input, row_part, None, False), (out_cot, cot_part, None, True)],
        capacity, sources,
    )
    spread = exchanged(spread)
    projections = shared_ring_gather(out_proj, core)
    gate_up, down, fold_gate, fold_up = folded_weights(
        position, w_gate, w_up, w_down, out_proj, projections, row_part, cot_part
    )
    rates = (decay_factor * jax.nn.softplus(-decay_param)).reshape(-1, gate_a_w.shape[1])
    rec_output, act, b, ca, ci, cs, decay, seg, exp, block, sel = early(
        position, expert_ids, rec_input, gate_input, prev_state, rates, extra_decay.T,
        gate_a_w, gate_i_w, capacity, sources,
    )
    direct = build(
        position, ids, weight,
        [
            (layer_input, row_rest, 4 * row_part // row_rest, False),
            (out_cot, cot_rest, 4 * cot_part // cot_rest, True),
            (rec_output, rec_output.shape[1], 0, False),
        ],
        capacity, sources,
    )
    got = exchanged(direct)
    pieces = ring_gather(spread[: slots // 2], spread[slots // 2 :])
    base = jnp.dot(out_cot, out_proj, preferred_element_type=F32)
    local_proj = lax.dot_general(
        out_cot, rec_output, (((0,), (0,)), ((), ())), preferred_element_type=F32
    )
    before = ahead(pieces[:6], gate_up, down, row_part, cot_part)
    hidden, gate_cot, up_cot, mix = expert(
        got, pieces[6:], before, gate_up, down, fold_gate, fold_up, row_part, cot_part
    )
    back = lax.all_to_all(
        mix.reshape(4 * sources, capacity, -1), ("tp", *sp_axes), 0, 0, tiled=True
    ).reshape(mix.shape)
    grad_gate, grad_up = row_grads(position, got, pieces, gate_cot, up_cot, width, row_part)
    grad_down = down_grads(position, got, pieces, hidden, width, row_part, cot_part)
    start = row_rest + cot_rest
    recs = across(got[:, start:])
    lines = width // sources
    parts = proj(position, gate_cot, up_cot, w_gate, w_up, local_proj, recs, lines)
    other = lax.ppermute(parts[1], "core", [(0, 1), (1, 0)])
    own, left, right, far = chip_sum(parts, other)
    terms = (shifted(right, 1), shifted(left, -1), shifted(far, 2))
    arriving = (sum(t.astype(F32) for t in terms) + own.astype(F32)).astype(BF16)
    arrived = lax.all_to_all(arriving, "sq", 0, 0, tiled=True)
    grad_out_proj = arrived.astype(F32).sum(axis=0)
    gate_input_grad, local, pair = scanned(
        back, sel, base, act, b, decay, seg, block, sources
    )
    pairs = lax.all_to_all(pair, sp_axes, 0, 0, tiled=True)
    rec_input_grad = final(position, pairs, local, exp, ca, ci, cs, gate_a_w, gate_i_w)
    return (grad_gate, grad_up, grad_down, grad_out_proj, rec_input_grad, gate_input_grad)


def solution(mesh):
    sp, tp = mesh.devices.shape
    inner = Mesh(mesh.devices.reshape(sp // 2, 2, tp), ("sq", "core", "tp"))
    sp = ("sq", "core")
    in_specs = (
        P(sp, None),
        P(sp, None),
        P(sp, None),
        P(sp, None),
        P(sp, None, "tp"),
        P(sp, None, "tp"),
        P(sp, "tp", None),
        P(None, "tp"),
        P(sp, "tp"),
        P(sp, "tp"),
        P(sp, "tp"),
        P(),
        P("tp", sp),
        P(),
        P(),
    )
    out_specs = (
        P(sp, None, "tp"),
        P(sp, None, "tp"),
        P(sp, "tp", None),
        P(sp, "tp"),
        P(sp, "tp"),
        P(sp, "tp"),
    )
    return jax.shard_map(
        per_device, mesh=inner, in_specs=in_specs, out_specs=out_specs, check_vma=False
    )
```
